512 devices in a mesh: grp: 2 (over y), sp: 32 (over z), tp: 8 (over x, core).
Axes of the slice: x: 4, y: 2, z: 32, core: 2. Of those that a mesh axis runs over, the one named last changes fastest.
The devices are a block of a 4x8x32 slice.
Arguments:
- input_wide: bfloat16 [8192, 512], P(('grp', 'sp'), 'tp'), parts along dimension 0, may hold values from -6 to 6
- input_narrow: bfloat16 [8192, 512], P(('grp', 'sp'), 'tp'), parts along dimension 0, may hold values from -6 to 6
- spacing: float32 [8192], P(('grp', 'sp')), parts along dimension 0, may hold values from 0.2 to 1642
- rate_wide: float32 [2, 32, 64], P(None, 'tp'), may hold values from 0.00012207031 to 0.035
- turn_wide: float32 [2, 32, 64], P(None, 'tp'), may hold values from 0.1 to 1.5
- drive_wide: float32 [2, 32, 16, 128], P(None, 'tp'), may hold values from -0.2 to 0.2
- read_wide: float32 [2, 32, 16, 128], P(None, 'tp'), may hold values from -0.5 to 0.5
- narrow_decay_rate: float32 [2, 32, 32], P(None, 'tp'), may hold values from 0.00012207031 to 0.035
- turn_narrow: float32 [2, 32, 32], P(None, 'tp'), may hold values from 0.1 to 1.5
- drive_narrow: float32 [2, 32, 16, 64], P(None, 'tp'), may hold values from -0.2 to 0.2
- read_narrow: float32 [2, 32, 16, 64], P(None, 'tp'), may hold values from -0.75 to 0.75
- skip_gain: float32 [2, 512], P(None, 'tp'), may hold values from -4 to 4
- out_value: bfloat16 [1024, 1024], P(None, 'tp'), may hold values from -0.1875 to 0.1875
- out_gate: bfloat16 [1024, 1024], P(None, 'tp'), may hold values from -0.1875 to 0.1875
- stream: bfloat16 [8192, 1024], P(('grp', 'sp'), 'tp'), parts along dimension 0, may hold values from -20 to 20
- norm_gain: float32 [1024], P('tp'), may hold values from 0.1 to 1.9
- up_value: bfloat16 [1024, 5632], P('sp', 'tp'), may hold values from -0.1875 to 0.1875
- up_gate: bfloat16 [1024, 5632], P('sp', 'tp'), may hold values from -0.1875 to 0.1875
- conv_taps: float32 [2, 3, 5632], P(None, None, 'tp'), may hold values from -3.5 to 3.5
- down_weight: bfloat16 [5632, 1024], P('tp', 'sp'), may hold values from -0.078125 to 0.078125
Outputs:
- mixed: bfloat16 [8192, 1024], P(('grp', 'sp'), 'tp'), parts along dimension 0
The draws below stay inside these ranges and needn't reach their ends.
There are 2 independent parts, one for each index of `grp`. The reference program is written for one: setup_inputs(seed, part) draws one part's arguments, and reference() takes and returns one part's arrays. A program takes and returns all parts, laid end to end along the dimension named above; an argument that names none is the same for every part. Nothing has to cross between parts.
All inputs are finite; a program needn't handle non-finite values.
Results may differ from the reference program's by a relative error of at most 0.017.
Values may be sent and summed in bfloat16 or wider, within the bound.
No kernel may reach another device: no remote copies, remote signals or barrier semaphores. Data moves between devices by JAX's collectives and lax.ppermute only.
A program may use at most 128 MiB of HBM per device.

```python
import math
import jax
import jax.numpy as jnp
from jax import lax

DA = 512
DB = 512
GROUP = 16
PA = 64
PB = 32
FF = 5632
TOK_DEV = 128
D = 1024
SEQUENCE_SLOTS = 4096
N_TP = 8


def rates_and_drive(key, groups, states):
    keys = jax.random.split(key, 4)
    share = 0.5
    quick = jax.random.bernoulli(keys[0], share, (2, groups, 1))
    slow_floor = 0.5 / SEQUENCE_SLOTS
    slow = slow_floor * jnp.exp(jax.random.uniform(keys[1], (2, groups, states), jnp.float32, 0.0, math.log(2.0)))
    fast = 0.01 * jnp.exp(jax.random.uniform(keys[2], (2, groups, states), jnp.float32, 0.0, math.log(3.5)))
    rate = jnp.where(quick, fast, slow)
    scale = jnp.sqrt(2.0 * rate / (2.0 * GROUP))
    scale = jnp.concatenate([scale, scale], axis=-1)[:, :, None, :]
    drive = jnp.clip(jax.random.normal(keys[3], (2, groups, GROUP, 2 * states), jnp.float32), -4.0, 4.0) * scale
    return (rate, drive)


def draw_rate_wide(key, part):
    return rates_and_drive(jax.random.fold_in(key, 11), DA // GROUP, PA)[0]


def draw_drive_wide(key, part):
    return rates_and_drive(jax.random.fold_in(key, 11), DA // GROUP, PA)[1]


def draw_narrow_decay_rate(key, part):
    return rates_and_drive(jax.random.fold_in(key, 23), DB // GROUP, PB)[0]


def draw_drive_narrow(key, part):
    return rates_and_drive(jax.random.fold_in(key, 23), DB // GROUP, PB)[1]


def draw_spacing(key, part):
    keys = jax.random.split(key, 3)
    blocks = SEQUENCE_SLOTS // TOK_DEV
    level = jnp.exp(jax.random.uniform(keys[0], (blocks,), jnp.float32, -0.69, 0.69))
    rough = jax.random.uniform(keys[1], (SEQUENCE_SLOTS,), jnp.float32, 0.5, 1.5)
    starting_shift = jnp.repeat(level, TOK_DEV) * rough
    slot_number = jax.random.randint(keys[2], (3,), 0, SEQUENCE_SLOTS)
    pulse_source = jnp.zeros((SEQUENCE_SLOTS,), jnp.float32).at[slot_number].set(0.4 * SEQUENCE_SLOTS)
    return starting_shift + pulse_source


def draw_stream(key, part):
    keys = jax.random.split(key, 2)
    values = jnp.clip(jax.random.normal(keys[0], (SEQUENCE_SLOTS, D), jnp.float32), -4.0, 4.0)
    rows = 10.0 ** jax.random.uniform(keys[1], (SEQUENCE_SLOTS, 1), jnp.float32, -0.5, 0.5)
    columns = 10.0 ** jnp.linspace(-0.5, 0.5, D, dtype=jnp.float32)
    return (values * rows * columns[None, :] * 0.5).astype(jnp.bfloat16)


def shard_levels(stream_key, shape, cuts, least, largest):
    loudness = 1.0
    for position, parts in cuts:
        heights = jax.random.uniform(jax.random.fold_in(jax.random.fold_in(stream_key, 6), position), (parts,), jnp.float32, least / len(cuts), largest / len(cuts))
        loudness = loudness * jnp.repeat(jnp.exp(heights), shape[position] // parts).reshape((-1,) + (1,) * (len(shape) - 1 - position))
    return loudness


def normal_values(stream_key, shape, deviation, limit, cuts=(), held_as=jnp.bfloat16):
    level = shard_levels(stream_key, shape, cuts, -0.22, 0.18) if cuts else 1.0
    values = jax.random.normal(stream_key, shape, jnp.float32) * deviation * level
    return jnp.minimum(jnp.maximum(values, -limit), limit).astype(held_as)


def setup_inputs(seed: int = 0, part: int = 0) -> dict:
    key_list = jax.random.split(jax.random.key(seed), 21)
    own_keys = jax.random.split(jax.random.fold_in(key_list[20], part), 21)
    input_wide = normal_values(own_keys[0], (SEQUENCE_SLOTS, DA), 1.0, 6.0, ((0, 32), (1, 8)))
    input_narrow = normal_values(own_keys[1], (SEQUENCE_SLOTS, DB), 1.0, 6.0, ((0, 32), (1, 8)))
    spacing = draw_spacing(jax.random.fold_in(jax.random.fold_in(key_list[20], part), 71), part)
    rate_wide = draw_rate_wide(jax.random.fold_in(key_list[20], 71), part)
    turn_wide = jnp.clip(0.1 + 1.4 * jax.random.uniform(key_list[4], (2, DA // GROUP, PA), jnp.float32) ** shard_levels(key_list[4], (2, DA // GROUP, PA), ((1, 8),), -0.2, 0.2), 0.1, 1.5)
    drive_wide = draw_drive_wide(jax.random.fold_in(key_list[20], 71), part)
    read_wide = normal_values(key_list[6], (2, DA // GROUP, GROUP, 2 * PA), (2 * PA) ** -0.5, 0.5, ((1, 8),), jnp.float32)
    narrow_decay_rate = draw_narrow_decay_rate(jax.random.fold_in(key_list[20], 71), part)
    turn_narrow = jnp.clip(0.1 + 1.4 * jax.random.uniform(key_list[8], (2, DB // GROUP, PB), jnp.float32) ** shard_levels(key_list[8], (2, DB // GROUP, PB), ((1, 8),), -0.2, 0.2), 0.1, 1.5)
    drive_narrow = draw_drive_narrow(jax.random.fold_in(key_list[20], 71), part)
    read_narrow = normal_values(key_list[10], (2, DB // GROUP, GROUP, 2 * PB), (2 * PB) ** -0.5, 0.75, ((1, 8),), jnp.float32)
    skip_gain = normal_values(key_list[11], (2, DA), 1.0, 4.0, ((1, 8),), jnp.float32)
    out_value = normal_values(key_list[12], (D, D), D ** -0.5, 0.1875, ((1, 8),))
    out_gate = normal_values(key_list[13], (D, D), D ** -0.5, 0.1875, ((1, 8),))
    stream = draw_stream(jax.random.fold_in(jax.random.fold_in(key_list[20], part), 71), part)
    norm_gain = jnp.clip(1.0 + 0.18 * jax.random.normal(key_list[15], (D,), jnp.float32), 0.1, 1.9)
    up_value = normal_values(key_list[16], (D, FF), D ** -0.5, 0.1875, ((0, 32), (1, 8)))
    up_gate = normal_values(key_list[17], (D, FF), D ** -0.5, 0.1875, ((0, 32), (1, 8)))
    conv_taps = normal_values(key_list[18], (2, 3, FF), 3 ** -0.5, 3.5, ((2, 8),), jnp.float32)
    down_weight = normal_values(key_list[19], (FF, D), FF ** -0.5, 0.078125, ((0, 8), (1, 32)))
    return {"input_wide": input_wide, "input_narrow": input_narrow, "spacing": spacing, "rate_wide": rate_wide, "turn_wide": turn_wide, "drive_wide": drive_wide, "read_wide": read_wide, "narrow_decay_rate": narrow_decay_rate, "turn_narrow": turn_narrow, "drive_narrow": drive_narrow, "read_narrow": read_narrow, "skip_gain": skip_gain, "out_value": out_value, "out_gate": out_gate, "stream": stream, "norm_gain": norm_gain, "up_value": up_value, "up_gate": up_gate, "conv_taps": conv_taps, "down_weight": down_weight}


precise = lax.Precision.HIGHEST
epsilon = 1e-06

def complex_times(left_real, left_quad, right_real, right_quad):
    return (left_real * right_real - left_quad * right_quad, left_real * right_quad + left_quad * right_real)

def step_factors(rate, turn, spacing):
    shrink = jnp.exp(-rate * spacing)
    angle = turn * spacing
    decay_real = shrink * jnp.cos(angle)
    decay_quad = shrink * jnp.sin(angle)
    square = rate * rate + turn * turn
    coef_real, coef_quad = complex_times(decay_real - 1.0, decay_quad, -rate / square, -turn / square)
    return (decay_real, decay_quad, coef_real, coef_quad)

def state_pass(inputs, spacing, rate, turn, drive, read, reverse):
    extent = inputs.shape[0]
    groups = rate.shape[0]
    states = rate.shape[1]
    clustered = inputs.astype(jnp.float32).reshape(extent, groups, GROUP)

    def advance(carry, item):
        state_real, state_quad = carry
        values, spot = item
        decay_real, decay_quad, coef_real, coef_quad = step_factors(rate, turn, spot)
        pushed = jnp.einsum('gc,gcq->gq', values, drive, precision=precise)
        kick_real, impulse_quadrature = complex_times(coef_real, coef_quad, pushed[:, :states], pushed[:, states:])
        kept_real, kept_quad = complex_times(decay_real, decay_quad, state_real, state_quad)
        state_real = kept_real + kick_real
        state_quad = kept_quad + impulse_quadrature
        joined = jnp.concatenate([state_real, state_quad], axis=1)
        reading = jnp.einsum('gq,gcq->gc', joined, read, precision=precise)
        return ((state_real, state_quad), reading)
    start = (jnp.zeros((groups, states), jnp.float32), jnp.zeros((groups, states), jnp.float32))
    _, readings = lax.scan(advance, start, (clustered, spacing), reverse=reverse)
    return readings.reshape(extent, groups * GROUP)

def mixer_half(inputs, spacing, rate, turn, drive, read, skip):
    reading = state_pass(inputs, spacing, rate[0], turn[0], drive[0], read[0], False)
    reading = reading + state_pass(inputs, spacing, rate[1], turn[1], drive[1], read[1], True)
    return jax.nn.gelu(reading + skip * inputs.astype(jnp.float32)).astype(jnp.bfloat16)

def reference(input_wide, input_narrow, spacing, rate_wide, turn_wide, drive_wide, read_wide, narrow_decay_rate, turn_narrow, drive_narrow, read_narrow, skip_gain, out_value, out_gate, stream, norm_gain, up_value, up_gate, conv_taps, down_weight):
    mixer_in = jnp.concatenate([mixer_half(input_wide, spacing, rate_wide, turn_wide, drive_wide, read_wide, skip_gain[0]), mixer_half(input_narrow, spacing, narrow_decay_rate, turn_narrow, drive_narrow, read_narrow, skip_gain[1])], axis=1)
    value = jnp.dot(mixer_in, out_value, preferred_element_type=jnp.float32)
    gate = jnp.dot(mixer_in, out_gate, preferred_element_type=jnp.float32)
    middle = (stream.astype(jnp.float32) + value * jax.nn.sigmoid(gate)).astype(jnp.bfloat16)
    expanded_width = middle.astype(jnp.float32)
    scale = lax.rsqrt(lax.optimization_barrier(jnp.mean(expanded_width * expanded_width, axis=1, keepdims=True)) + epsilon)
    normed = (expanded_width * scale * norm_gain).astype(jnp.bfloat16)
    pre = jnp.concatenate([jnp.dot(normed, up_value, preferred_element_type=jnp.float32), jnp.dot(normed, up_gate, preferred_element_type=jnp.float32)], axis=1).astype(jnp.bfloat16)
    padded = jnp.pad(pre, ((1, 1), (0, 0)))
    taps = jnp.concatenate([conv_taps[0], conv_taps[1]], axis=1)
    conv = taps[0] * padded[:-2] + taps[1] * padded[1:-1] + taps[2] * padded[2:]
    hidden = (jax.nn.silu(conv[:, FF:]) * conv[:, :FF]).astype(jnp.bfloat16)
    block = FF // N_TP
    ffn = jnp.zeros((hidden.shape[0], down_weight.shape[1]), jnp.float32)
    for index in range(N_TP):
        partial_value = jnp.dot(hidden[:, index * block:(index + 1) * block], down_weight[index * block:(index + 1) * block], preferred_element_type=jnp.float32)
        ffn = ffn + lax.optimization_barrier(partial_value.astype(jnp.bfloat16)).astype(jnp.float32)
    return (middle.astype(jnp.float32) + ffn).astype(jnp.bfloat16)
```

```python
import jax
import jax.numpy as jnp
from jax import lax
from jax.sharding import Mesh
from jax.sharding import PartitionSpec as P

GROUP = 16
SHARE = 2
LANES = 128

precise = lax.Precision.HIGHEST
epsilon = 1e-06
SP = ("zp", "zi")
MEMBERS = ("zi", "tp")


def complex_times(left_real, left_quad, right_real, right_quad):
    return (
        left_real * right_real - left_quad * right_quad,
        left_real * right_quad + left_quad * right_real,
    )


def powers(rate, turn, span):
    shrink = jnp.exp(-rate * span)
    angle = turn * span
    return shrink * jnp.cos(angle), shrink * jnp.sin(angle)


def pair_combine(early, later):
    decay_real, decay_quad = complex_times(early[0], early[1], later[0], later[1])
    shifted_real, moved_quad = complex_times(later[0], later[1], early[2], early[3])
    return (decay_real, decay_quad, shifted_real + later[2], moved_quad + later[3])


def lanes_up(count):
    return -(-count // LANES) * LANES


def padded_last(array, width):
    return jnp.pad(array, [(0, 0)] * (array.ndim - 1) + [(0, width - array.shape[-1])])


def sent_to_all(array, axes):
    copies = jnp.broadcast_to(array, (lax.axis_size(axes), *array.shape))
    return lax.all_to_all(copies, axes, split_axis=0, concat_axis=0, tiled=True)


def weight_block(up_value, up_gate, down_weight):
    share = lax.axis_size("zi")
    part = up_value.shape[1] // share
    width = lanes_up(part)
    block = [
        jnp.concatenate(
            [
                padded_last(w[:, k * part : (k + 1) * part], width)
                for w in (up_value, up_gate, down_weight.T)
            ],
            axis=1,
        )
        for k in range(share)
    ]
    if share > 1:
        block = lax.all_to_all(jnp.concatenate(block), "zi", 0, 0, tiled=True)
    else:
        block = block[0]
    return block, width


def mixer(input_wide, input_narrow, spacing, wide, narrow, skip_gain):
    extent = input_wide.shape[0]
    rates, turns = [], []
    pushes = [[], []]
    both_spacing = jnp.stack([spacing, spacing[::-1]])
    for inputs, (rate, turn, drive, _) in ((input_wide, wide), (input_narrow, narrow)):
        states = rate.shape[2]
        rates.append(rate.reshape(2, -1))
        turns.append(turn.reshape(2, -1))
        clustered = inputs.astype(jnp.float32).reshape(extent, -1, GROUP)
        clustered = jnp.stack([clustered, clustered[::-1]])
        pushed = jnp.einsum("dtgc,dgcq->dtgq", clustered, drive, precision=precise)
        pushes[0].append(pushed[..., :states].reshape(2, extent, -1))
        pushes[1].append(pushed[..., states:].reshape(2, extent, -1))
    rate, turn = jnp.concatenate(rates, axis=1), jnp.concatenate(turns, axis=1)
    push_real, push_quad = (jnp.concatenate(p, axis=2) for p in pushes)
    decay_real, decay_quad = powers(rate[:, None], turn[:, None], both_spacing[:, :, None])
    square = rate * rate + turn * turn
    coef_real, coef_quad = complex_times(
        decay_real - 1.0, decay_quad, (-rate / square)[:, None], (-turn / square)[:, None]
    )
    kick_real, kick_quad = complex_times(coef_real, coef_quad, push_real, push_quad)
    _, _, local_real, local_quad = lax.associative_scan(
        pair_combine, (decay_real, decay_quad, kick_real, kick_quad), axis=1
    )
    count, mine = lax.axis_size(SP), lax.axis_index(SP)
    place = jnp.arange(count)
    ends = jnp.concatenate([local_real[:, -1], local_quad[:, -1]], axis=1)
    ends = jnp.concatenate([ends, jnp.full((2, LANES), jnp.sum(spacing))], axis=1)
    ends = ends.reshape(2, -1, LANES)
    outgoing = jnp.where((place > mine)[:, None, None], ends[0], ends[1])
    arrived = lax.all_to_all(outgoing, SP, split_axis=0, concat_axis=0, tiled=True)
    spans = arrived[:, -1, 0]
    between = ((place[:, None] < place) & (place < mine)) | ((place[:, None] > place) & (place > mine))
    gap = jnp.sum(jnp.where(between, spans, 0.0), axis=1)[:, None]
    ahead = (place < mine)[:, None]
    arrived = arrived[:, :-1].reshape(count, 2, -1)
    weight_real, weight_quad = powers(
        jnp.where(ahead, rate[0], rate[1]), jnp.where(ahead, turn[0], turn[1]), gap
    )
    term_real, term_quad = complex_times(weight_real, weight_quad, arrived[:, 0], arrived[:, 1])
    masks = (ahead, (place > mine)[:, None])
    carry_real = jnp.stack([jnp.sum(jnp.where(m, term_real, 0.0), axis=0) for m in masks])
    carry_quad = jnp.stack([jnp.sum(jnp.where(m, term_quad, 0.0), axis=0) for m in masks])
    span = jnp.cumsum(both_spacing, axis=1)[:, :, None]
    power_real, power_quad = powers(rate[:, None], turn[:, None], span)
    extra_real, extra_quad = complex_times(
        power_real, power_quad, carry_real[:, None], carry_quad[:, None]
    )
    state_real, state_quad = local_real + extra_real, local_quad + extra_quad
    parts, at = [], 0
    for which, (inputs, (own_rate, _, _, read)) in enumerate(
        ((input_wide, wide), (input_narrow, narrow))
    ):
        groups, states = own_rate.shape[1:]
        upto = at + groups * states
        joined = jnp.concatenate(
            [
                state[:, :, at:upto].reshape(2, extent, groups, states)
                for state in (state_real, state_quad)
            ],
            axis=3,
        )
        at = upto
        reading = jnp.einsum("dtgq,dgcq->dtgc", joined, read, precision=precise)
        reading = (reading[0] + reading[1][::-1]).reshape(extent, -1)
        parts.append(jax.nn.gelu(reading + skip_gain[which] * inputs.astype(jnp.float32)))
    return jnp.concatenate(parts, axis=1).astype(jnp.bfloat16)


def on_device(
    input_wide,
    input_narrow,
    spacing,
    rate_wide,
    turn_wide,
    drive_wide,
    read_wide,
    narrow_decay_rate,
    turn_narrow,
    drive_narrow,
    read_narrow,
    skip_gain,
    out_value,
    out_gate,
    stream,
    norm_gain,
    up_value,
    up_gate,
    conv_taps,
    down_weight,
):
    share = lax.axis_size("zi")
    extent = input_wide.shape[0]
    block, width = weight_block(up_value, up_gate, down_weight)
    block, input_wide, input_narrow, spacing = lax.optimization_barrier(
        (block, input_wide, input_narrow, spacing)
    )
    weights = lax.all_gather(block, "zp", axis=0, tiled=True)
    mixer_in = mixer(
        input_wide,
        input_narrow,
        spacing,
        (rate_wide, turn_wide, drive_wide, read_wide),
        (narrow_decay_rate, turn_narrow, drive_narrow, read_narrow),
        skip_gain,
    )
    channels = input_wide.shape[1]
    slots = sent_to_all(mixer_in, "tp")
    peers = slots.shape[0]
    rows = jnp.moveaxis(slots, 0, 1).reshape(extent, -1)

    def by_slot(weight):
        turned = jnp.moveaxis(weight.reshape(2, peers, channels, -1), 0, 1)
        return turned.reshape(weight.shape)

    value = jnp.dot(rows, by_slot(out_value), preferred_element_type=jnp.float32)
    gate = jnp.dot(rows, by_slot(out_gate), preferred_element_type=jnp.float32)
    middle = (stream.astype(jnp.float32) + value * jax.nn.sigmoid(gate)).astype(jnp.bfloat16)
    count = lax.axis_size(SP)
    up, down = [(i, i + 1) for i in range(count - 1)], [(i + 1, i) for i in range(count - 1)]
    low = lax.ppermute(middle[-1:], SP, up)
    high = lax.ppermute(middle[:1], SP, down)
    gain_a = lax.reduce_precision(norm_gain, 8, 7)
    gain_b = lax.reduce_precision(norm_gain - gain_a, 8, 7)
    gain_c = norm_gain - gain_a - gain_b
    gains = jnp.stack([gain_a, gain_b, gain_c]).astype(jnp.bfloat16)
    sent = jnp.concatenate([middle, low, high, gains], axis=0)
    slots = sent_to_all(sent, MEMBERS)
    slots = slots.reshape(share, -1, *sent.shape)
    picked = [slots[0, :, extent : extent + 1]]
    picked += [slots[k, :, :extent] for k in range(share)]
    picked += [slots[share - 1, :, extent + 1 : extent + 2]]
    whole = jnp.moveaxis(jnp.concatenate(picked, axis=1), 0, 1)
    whole = whole.reshape(whole.shape[0], -1).astype(jnp.float32)
    gain = jnp.sum(slots[0, :, extent + 2 :].astype(jnp.float32), axis=1).reshape(-1)
    mean = jnp.mean(whole * whole, axis=1, keepdims=True)
    normed = (whole * lax.rsqrt(mean + epsilon) * gain).astype(jnp.bfloat16)
    pre = jnp.dot(normed, weights[:, : 2 * width], preferred_element_type=jnp.float32)
    pre = pre.astype(jnp.bfloat16)
    taps = conv_taps.reshape(2, 3, share, -1)
    taps = lax.dynamic_index_in_dim(taps, lax.axis_index("zi"), 2, keepdims=False)
    taps = jnp.moveaxis(padded_last(taps, width), 0, 1).reshape(3, -1)
    conv = taps[0] * pre[:-2] + taps[1] * pre[1:-1] + taps[2] * pre[2:]
    hidden = (jax.nn.silu(conv[:, width:]) * conv[:, :width]).astype(jnp.bfloat16)
    terms = lax.dot_general(
        hidden,
        weights[:, 2 * width :],
        (((1,), (1,)), ((), ())),
        preferred_element_type=jnp.float32,
    ).astype(jnp.bfloat16)
    terms = terms.reshape(share, extent, peers, -1)
    terms = jnp.moveaxis(terms, 2, 1).reshape(share * peers, extent, -1)
    arrived = lax.all_to_all(terms, MEMBERS, split_axis=0, concat_axis=0, tiled=True)
    ffn = jnp.sum(arrived.astype(jnp.float32), axis=0)
    return (middle.astype(jnp.float32) + ffn).astype(jnp.bfloat16)


def solution(mesh):
    grp, sp, tp = mesh.axis_names
    sizes = mesh.devices.shape
    parted = Mesh(
        mesh.devices.reshape(sizes[0], sizes[1] // SHARE, SHARE, sizes[2]), ("grp", *SP, "tp")
    )
    spot = ("grp", *SP)
    placed = (
        P(spot, "tp"),
        P(spot, "tp"),
        P(spot),
        P(None, "tp", None),
        P(None, "tp", None),
        P(None, "tp", None, None),
        P(None, "tp", None, None),
        P(None, "tp", None),
        P(None, "tp", None),
        P(None, "tp", None, None),
        P(None, "tp", None, None),
        P(None, "tp"),
        P(None, "tp"),
        P(None, "tp"),
        P(spot, "tp"),
        P("tp"),
        P(SP, "tp"),
        P(SP, "tp"),
        P(None, None, "tp"),
        P("tp", SP),
    )
    return jax.shard_map(
        on_device, mesh=parted, in_specs=placed, out_specs=P(spot, "tp"), check_vma=False
    )
```

```python
import functools
import math

import jax
import jax.numpy as jnp
from jax import lax
from jax.experimental import pallas as pl
from jax.experimental.pallas import tpu as pltpu
from jax.sharding import Mesh
from jax.sharding import PartitionSpec as P

SHARE = 2
LANES = 128
SUB = 8

epsilon = 1e-06
SP = ("zp", "zi")
MEMBERS = ("zi", "tp")


def complex_times(left_real, left_quad, right_real, right_quad):
    return (
        left_real * right_real - left_quad * right_quad,
        left_real * right_quad + left_quad * right_real,
    )


def lanes_up(count):
    return -(-count // LANES) * LANES


def padded_last(array, width):
    return jnp.pad(array, [(0, 0)] * (array.ndim - 1) + [(0, width - array.shape[-1])])


def sent_to_all(array, axes):
    copies = jnp.broadcast_to(array, (lax.axis_size(axes), *array.shape))
    return lax.all_to_all(copies, axes, split_axis=0, concat_axis=0, tiled=True)


def weight_block(up_value, up_gate, down_weight):
    share = lax.axis_size("zi")
    part = up_value.shape[1] // share
    width = lanes_up(part)
    block = [
        jnp.concatenate(
            [
                padded_last(w[:, k * part : (k + 1) * part], width)
                for w in (up_value, up_gate, down_weight.T)
            ],
            axis=1,
        )
        for k in range(share)
    ]
    if share > 1:
        block = lax.all_to_all(jnp.concatenate(block), "zi", 0, 0, tiled=True)
    else:
        block = block[0]
    return block, width


def cos_sin(turn, span):
    turns = (turn * (0.5 / math.pi)) * span
    half = (turns - jnp.floor(turns + 0.5)) * math.pi
    square = half * half
    sine, cosine = 1.0 / math.factorial(13), 1.0 / math.factorial(12)
    for k in range(11, 0, -2):
        sine = sine * square + (-1.0) ** (k // 2) / math.factorial(k)
    for k in range(10, -1, -2):
        cosine = cosine * square + (-1.0) ** (k // 2) / math.factorial(k)
    sine = sine * half
    return 1.0 - 2.0 * sine * sine, 2.0 * sine * cosine


def powers(rate, turn, span):
    shrink = jnp.exp(-rate * span)
    cosine, sine = cos_sin(turn, span)
    return shrink * cosine, shrink * sine


def in_lanes(wide, narrow, d):
    rows = [ref[d, k : k + 1, :] for ref in (wide, narrow) for k in range(ref.shape[1])]
    return jnp.concatenate(rows, axis=1)


def two_terms(x):
    high = x.astype(jnp.bfloat16)
    return high, (x - high.astype(jnp.float32)).astype(jnp.bfloat16)


def spread(ref, d, part, groups):
    states = ref.shape[2] // 2
    own = ref[d][:, part * states : (part + 1) * states]
    wide = jnp.concatenate([own] * groups, axis=1)
    row = lax.broadcasted_iota(jnp.int32, wide.shape, 0) // (wide.shape[0] // groups)
    lane = lax.broadcasted_iota(jnp.int32, wide.shape, 1) // states
    return two_terms(jnp.where(row == lane, wide, 0.0))


def shuffled(shape, row_axis):
    row = lax.broadcasted_iota(jnp.int32, shape, row_axis)
    position = lax.broadcasted_iota(jnp.int32, shape, 1 - row_axis)
    return position == (row % SUB) * (shape[0] // SUB) + row // SUB


def local_kernel(
    mine, wide_in, narrow_in, spacing, rw, tw, dw, rn, tn, dn, out, inputs, sr, si, pr, pi
):
    extent = spacing.shape[1]
    steps = extent // SUB
    place = shuffled((extent, extent), 0)
    span = jnp.sum(jnp.where(place, spacing[...], 0.0), axis=1, keepdims=True)
    both = jnp.concatenate([wide_in[...], narrow_in[...]], axis=0)
    rows = lax.dot_general(
        place.astype(jnp.float32).astype(jnp.bfloat16),
        both,
        (((1,), (1,)), ((), ())),
        preferred_element_type=jnp.float32,
    ).astype(jnp.bfloat16)
    inputs[...] = rows
    channels = wide_in.shape[0]
    halves = ((rows[:, :channels], dw, rw.shape[1]), (rows[:, channels:], dn, rn.shape[1]))
    tiles = []
    for d in range(2):
        rate, turn = in_lanes(rw, rn, d), in_lanes(tw, tn, d)
        push = []
        for part in range(2):
            pieces = []
            for x, drive, groups in halves:
                high, low = spread(drive, d, part, groups)
                pieces.append(
                    jnp.dot(x, high, preferred_element_type=jnp.float32)
                    + jnp.dot(x, low, preferred_element_type=jnp.float32)
                )
            push.append(jnp.concatenate(pieces, axis=1))
        square = rate * rate + turn * turn
        back_real, back_quad = -rate / square, -turn / square
        decay_real, decay_quad = powers(rate, turn, span)
        coef_real, coef_quad = complex_times(decay_real - 1.0, decay_quad, back_real, back_quad)
        kick_real, kick_quad = complex_times(coef_real, coef_quad, push[0], push[1])
        order = range(steps) if d == 0 else range(steps - 1, -1, -1)
        state = None
        for i in order:
            at = slice(i * SUB, (i + 1) * SUB)
            decay = (decay_real[at], decay_quad[at])
            if state is None:
                state, power = (kick_real[at], kick_quad[at]), decay
            else:
                kept = complex_times(*decay, *state)
                state = (kept[0] + kick_real[at], kept[1] + kick_quad[at])
                power = complex_times(*decay, *power)
            sr[d, at, :] = state[0]
            si[d, at, :] = state[1]
            pr[d, at, :] = power[0]
            pi[d, at, :] = power[1]
        end = None
        for c in range(SUB) if d == 0 else range(SUB - 1, -1, -1):
            own = (state[0][c : c + 1], state[1][c : c + 1])
            if end is None:
                end = own
            else:
                kept = complex_times(power[0][c : c + 1], power[1][c : c + 1], *end)
                end = (kept[0] + own[0], kept[1] + own[1])
        count = end[0].shape[1] // LANES
        pieces = [e[:, k * LANES : (k + 1) * LANES] for e in end for k in range(count)]
        total = jnp.sum(spacing[...], axis=1, keepdims=True)
        pieces.append(jnp.broadcast_to(total, (1, LANES)))
        pieces.append(jnp.zeros((SUB - len(pieces), LANES), jnp.float32))
        tiles.append(jnp.concatenate(pieces, axis=0))
    for j in range(out.shape[0]):
        out[j] = jnp.where(j > mine[0], tiles[0], tiles[1])


def carried(mine, arrived, rates, turns, count):
    peers = arrived.shape[0]
    quads = 2 * count

    def tile(row):
        pieces = [row[:, k * LANES : (k + 1) * LANES] for k in range(count)] * 2
        pieces.append(jnp.zeros((SUB - quads, LANES), jnp.float32))
        return jnp.concatenate(pieces, axis=0)

    rates, turns = [tile(r) for r in rates], [tile(t) for t in turns]
    spans = [arrived[j, quads : quads + 1, :] for j in range(peers)]
    zero = jnp.zeros((1, LANES), jnp.float32)
    before, after = [zero] * peers, [zero] * peers
    for j in range(peers - 2, -1, -1):
        before[j] = jnp.where(j + 1 < mine, before[j + 1] + spans[j + 1], zero)
    for j in range(1, peers):
        after[j] = jnp.where(j - 1 > mine, after[j - 1] + spans[j - 1], zero)
    sums = [jnp.zeros((SUB, LANES), jnp.float32)] * 2
    for j in range(peers):
        early, late = j < mine, j > mine
        gap = jnp.where(early, before[j], after[j])
        weight = powers(
            jnp.where(early, rates[0], rates[1]), jnp.where(early, turns[0], turns[1]), gap
        )
        end = arrived[j]
        crossed = jnp.concatenate([-end[count:quads], end[:count], end[quads:]], axis=0)
        term = weight[0] * end + weight[1] * crossed
        sums[0] = sums[0] + jnp.where(early, term, 0.0)
        sums[1] = sums[1] + jnp.where(late, term, 0.0)
    out = []
    for s in sums:
        row = [s[k : k + 1] for k in range(quads)]
        out.append((jnp.concatenate(row[:count], axis=1), jnp.concatenate(row[count:], axis=1)))
    return out


def reading_kernel(
    mine, arrived, rw, tw, dw, rn, tn, dn, skip, inputs, sr, si, pr, pi, out
):
    extent = inputs.shape[0]
    steps = extent // SUB
    count = sr.shape[2] // LANES
    rates = [in_lanes(rw, rn, d) for d in range(2)]
    turns = [in_lanes(tw, tn, d) for d in range(2)]
    carries = carried(mine[0], arrived, rates, turns, count)
    channels = dw.shape[1]
    reading = [jnp.zeros((extent, channels), jnp.float32) for _ in range(2)]
    for d in range(2):
        last = slice((steps - 1) * SUB, extent) if d == 0 else slice(0, SUB)
        state, power = (sr[d, last, :], si[d, last, :]), (pr[d, last, :], pi[d, last, :])
        carry, starts = carries[d], [None] * SUB
        for c in range(SUB) if d == 0 else range(SUB - 1, -1, -1):
            starts[c] = carry
            at = slice(c, c + 1)
            kept = complex_times(power[0][at], power[1][at], *carry)
            carry = (kept[0] + state[0][at], kept[1] + state[1][at])
        start = [jnp.concatenate([s[k] for s in starts], axis=0) for k in range(2)]
        start = [jnp.concatenate([s] * steps, axis=0) for s in start]
        extra = complex_times(pr[d], pi[d], *start)
        at = 0
        for which, (read, groups) in enumerate(((dw, rw.shape[1]), (dn, rn.shape[1]))):
            upto = at + groups * read.shape[2] // 2
            for part, local in enumerate((sr, si)):
                value = local[d, :, at:upto] + extra[part][:, at:upto]
                high, low = two_terms(value)
                read_high, read_low = spread(read, d, part, groups)
                for x, y in ((high, read_high), (low, read_high), (high, read_low)):
                    reading[which] = reading[which] + lax.dot_general(
                        x, y, (((1,), (1,)), ((), ())), preferred_element_type=jnp.float32
                    )
            at = upto
    total = jnp.concatenate(reading, axis=1) + skip[...] * inputs[...].astype(jnp.float32)
    mixed = jax.nn.gelu(total).astype(jnp.bfloat16)
    back = shuffled((extent, extent), 1).astype(jnp.float32).astype(jnp.bfloat16)
    rows = jnp.dot(back, mixed, preferred_element_type=jnp.float32).astype(jnp.bfloat16)
    for k in range(out.shape[0]):
        out[k] = rows


def in_memory(count):
    vmem = pl.BlockSpec(memory_space=pltpu.VMEM)
    return [pl.BlockSpec(memory_space=pltpu.SMEM)] + [vmem] * count


def mixer(input_wide, input_narrow, spacing, wide, narrow, skip_gain):
    extent, channels = input_wide.shape
    rw, tw, dw, cw = wide
    rn, tn, dn, cn = narrow
    dw, cw, dn, cn = (m.reshape(2, channels, m.shape[3]) for m in (dw, cw, dn, cn))
    states = rw.shape[1] * rw.shape[2] + rn.shape[1] * rn.shape[2]
    mine = lax.axis_index(SP).astype(jnp.int32).reshape(1)
    f32 = functools.partial(jax.ShapeDtypeStruct, dtype=jnp.float32)
    table = f32((2, extent, states))
    cost = pl.CostEstimate(flops=20_000_000, bytes_accessed=2_000_000, transcendentals=100_000)
    out, inputs, *tables = pl.pallas_call(
        local_kernel,
        name="local_states",
        out_shape=(
            f32((lax.axis_size(SP), SUB, LANES)),
            jax.ShapeDtypeStruct((extent, 2 * channels), jnp.bfloat16),
            table,
            table,
            table,
            table,
        ),
        in_specs=in_memory(9),
        out_specs=tuple(in_memory(6)[1:]),
        cost_estimate=cost,
    )(mine, input_wide.T, input_narrow.T, spacing.reshape(1, -1), rw, tw, dw, rn, tn, dn)
    arrived = lax.all_to_all(out, SP, split_axis=0, concat_axis=0, tiled=True)
    return pl.pallas_call(
        reading_kernel,
        name="readings",
        out_shape=jax.ShapeDtypeStruct(
            (lax.axis_size("tp"), extent, 2 * channels), jnp.bfloat16
        ),
        in_specs=in_memory(13),
        out_specs=in_memory(1)[1],
        cost_estimate=cost,
    )(mine, arrived, rw, tw, cw, rn, tn, cn, skip_gain.reshape(1, -1), inputs, *tables)


def on_device(
    input_wide,
    input_narrow,
    spacing,
    rate_wide,
    turn_wide,
    drive_wide,
    read_wide,
    narrow_decay_rate,
    turn_narrow,
    drive_narrow,
    read_narrow,
    skip_gain,
    out_value,
    out_gate,
    stream,
    norm_gain,
    up_value,
    up_gate,
    conv_taps,
    down_weight,
):
    share = lax.axis_size("zi")
    extent = input_wide.shape[0]
    block, width = weight_block(up_value, up_gate, down_weight)
    block, input_wide, input_narrow, spacing = lax.optimization_barrier(
        (block, input_wide, input_narrow, spacing)
    )
    weights = lax.all_gather(block, "zp", axis=0, tiled=True)
    mixer_in = mixer(
        input_wide,
        input_narrow,
        spacing,
        (rate_wide, turn_wide, drive_wide, read_wide),
        (narrow_decay_rate, turn_narrow, drive_narrow, read_narrow),
        skip_gain,
    )
    channels = input_wide.shape[1]
    slots = lax.all_to_all(mixer_in, "tp", split_axis=0, concat_axis=0, tiled=True)
    peers = slots.shape[0]
    rows = jnp.moveaxis(slots, 0, 1).reshape(extent, -1)

    def by_slot(weight):
        turned = jnp.moveaxis(weight.reshape(2, peers, channels, -1), 0, 1)
        return turned.reshape(weight.shape)

    value = jnp.dot(rows, by_slot(out_value), preferred_element_type=jnp.float32)
    gate = jnp.dot(rows, by_slot(out_gate), preferred_element_type=jnp.float32)
    middle = (stream.astype(jnp.float32) + value * jax.nn.sigmoid(gate)).astype(jnp.bfloat16)
    count = lax.axis_size(SP)
    up, down = [(i, i + 1) for i in range(count - 1)], [(i + 1, i) for i in range(count - 1)]
    low = lax.ppermute(middle[-1:], SP, up)
    high = lax.ppermute(middle[:1], SP, down)
    gain_a = lax.reduce_precision(norm_gain, 8, 7)
    gain_b = lax.reduce_precision(norm_gain - gain_a, 8, 7)
    gain_c = norm_gain - gain_a - gain_b
    gains = jnp.stack([gain_a, gain_b, gain_c]).astype(jnp.bfloat16)
    sent = jnp.concatenate([middle, low, high, gains], axis=0)
    slots = sent_to_all(sent, MEMBERS)
    slots = slots.reshape(share, -1, *sent.shape)
    picked = [slots[0, :, extent : extent + 1]]
    picked += [slots[k, :, :extent] for k in range(share)]
    picked += [slots[share - 1, :, extent + 1 : extent + 2]]
    whole = jnp.moveaxis(jnp.concatenate(picked, axis=1), 0, 1)
    whole = whole.reshape(whole.shape[0], -1).astype(jnp.float32)
    gain = jnp.sum(slots[0, :, extent + 2 :].astype(jnp.float32), axis=1).reshape(-1)
    mean = jnp.mean(whole * whole, axis=1, keepdims=True)
    normed = (whole * lax.rsqrt(mean + epsilon) * gain).astype(jnp.bfloat16)
    pre = jnp.dot(normed, weights[:, : 2 * width], preferred_element_type=jnp.float32)
    pre = pre.astype(jnp.bfloat16)
    taps = conv_taps.reshape(2, 3, share, -1)
    taps = lax.dynamic_index_in_dim(taps, lax.axis_index("zi"), 2, keepdims=False)
    taps = jnp.moveaxis(padded_last(taps, width), 0, 1).reshape(3, -1)
    conv = taps[0] * pre[:-2] + taps[1] * pre[1:-1] + taps[2] * pre[2:]
    hidden = (jax.nn.silu(conv[:, width:]) * conv[:, :width]).astype(jnp.bfloat16)
    terms = lax.dot_general(
        hidden,
        weights[:, 2 * width :],
        (((1,), (1,)), ((), ())),
        preferred_element_type=jnp.float32,
    ).astype(jnp.bfloat16)
    terms = terms.reshape(share, extent, peers, -1)
    terms = jnp.moveaxis(terms, 2, 1).reshape(share * peers, extent, -1)
    arrived = lax.all_to_all(terms, MEMBERS, split_axis=0, concat_axis=0, tiled=True)
    ffn = jnp.sum(arrived.astype(jnp.float32), axis=0)
    return (middle.astype(jnp.float32) + ffn).astype(jnp.bfloat16)


def solution(mesh):
    grp, sp, tp = mesh.axis_names
    sizes = mesh.devices.shape
    parted = Mesh(
        mesh.devices.reshape(sizes[0], sizes[1] // SHARE, SHARE, sizes[2]), ("grp", *SP, "tp")
    )
    spot = ("grp", *SP)
    placed = (
        P(spot, "tp"),
        P(spot, "tp"),
        P(spot),
        P(None, "tp", None),
        P(None, "tp", None),
        P(None, "tp", None, None),
        P(None, "tp", None, None),
        P(None, "tp", None),
        P(None, "tp", None),
        P(None, "tp", None, None),
        P(None, "tp", None, None),
        P(None, "tp"),
        P(None, "tp"),
        P(None, "tp"),
        P(spot, "tp"),
        P("tp"),
        P(SP, "tp"),
        P(SP, "tp"),
        P(None, None, "tp"),
        P("tp", SP),
    )
    return jax.shard_map(
        on_device, mesh=parted, in_specs=placed, out_specs=P(spot, "tp"), check_vma=False
    )
```

```python
import functools
import math

import jax
import jax.numpy as jnp
from jax import lax
from jax.experimental import pallas as pl
from jax.experimental.pallas import tpu as pltpu
from jax.sharding import Mesh
from jax.sharding import PartitionSpec as P

SHARE = 2
LANES = 128
SUB = 8

epsilon = 1e-06
SP = ("zp", "zi")
MEMBERS = ("gi", "zi", "tp")


def complex_times(left_real, left_quad, right_real, right_quad):
    return (
        left_real * right_real - left_quad * right_quad,
        left_real * right_quad + left_quad * right_real,
    )


def lanes_up(count):
    return -(-count // LANES) * LANES


def padded_last(array, width):
    return jnp.pad(array, [(0, 0)] * (array.ndim - 1) + [(0, width - array.shape[-1])])


def sent_to_all(array, axes):
    copies = jnp.broadcast_to(array, (lax.axis_size(axes), *array.shape))
    return lax.all_to_all(copies, axes, split_axis=0, concat_axis=0, tiled=True)


def pack_kernel(quads, which, value, gate, down, out):
    pair, rows, width = out.shape
    part = value.shape[1] // (pair * quads)
    for k in range(pair):
        pieces = []
        for w in (value, gate, down):
            own = None
            for q in range(quads):
                at = (q * pair + k) * part
                piece = w[:, at : at + part].astype(jnp.float32)
                own = piece if own is None else jnp.where(which[0] == q, piece, own)
            pieces.append(own)
        if width > 3 * part:
            pieces.append(jnp.zeros((rows, width - 3 * part), jnp.float32))
        out[k] = jnp.concatenate(pieces, axis=1).astype(out.dtype)


def weight_block(up_value, up_gate, down_weight):
    pair, quads = lax.axis_size("zi"), lax.axis_size("gi")
    rows, columns = up_value.shape
    part = columns // (pair * quads)
    which = lax.axis_index("gi").astype(jnp.int32).reshape(1)
    block = pl.pallas_call(
        functools.partial(pack_kernel, quads),
        name="pack",
        out_shape=jax.ShapeDtypeStruct((pair, rows, lanes_up(3 * part)), jnp.bfloat16),
        in_specs=in_memory(3),
        out_specs=in_memory(1)[1],
    )(which, up_value, up_gate, down_weight.T)
    block = lax.all_to_all(block, "zi", 0, 0, tiled=True)
    return block.reshape(pair * rows, -1), part


def cos_sin(turn, span):
    turns = (turn * (0.5 / math.pi)) * span
    half = (turns - jnp.floor(turns + 0.5)) * math.pi
    square = half * half
    sine, cosine = 1.0 / math.factorial(13), 1.0 / math.factorial(12)
    for k in range(11, 0, -2):
        sine = sine * square + (-1.0) ** (k // 2) / math.factorial(k)
    for k in range(10, -1, -2):
        cosine = cosine * square + (-1.0) ** (k // 2) / math.factorial(k)
    sine = sine * half
    return 1.0 - 2.0 * sine * sine, 2.0 * sine * cosine


def powers(rate, turn, span):
    shrink = jnp.exp(-rate * span)
    cosine, sine = cos_sin(turn, span)
    return shrink * cosine, shrink * sine


def in_lanes(wide, narrow, d):
    rows = [ref[d, k : k + 1, :] for ref in (wide, narrow) for k in range(ref.shape[1])]
    return jnp.concatenate(rows, axis=1)


def two_terms(x):
    high = x.astype(jnp.bfloat16)
    return high, (x - high.astype(jnp.float32)).astype(jnp.bfloat16)


def spread(ref, d, part, groups):
    states = ref.shape[2] // 2
    own = ref[d][:, part * states : (part + 1) * states]
    wide = jnp.concatenate([own] * groups, axis=1)
    row = lax.broadcasted_iota(jnp.int32, wide.shape, 0) // (wide.shape[0] // groups)
    lane = lax.broadcasted_iota(jnp.int32, wide.shape, 1) // states
    return two_terms(jnp.where(row == lane, wide, 0.0))


def shuffled(shape, row_axis):
    row = lax.broadcasted_iota(jnp.int32, shape, row_axis)
    position = lax.broadcasted_iota(jnp.int32, shape, 1 - row_axis)
    return position == (row % SUB) * (shape[0] // SUB) + row // SUB


def local_kernel(
    mine, wide_in, narrow_in, spacing, rw, tw, dw, rn, tn, dn, out, inputs, sr, si, pr, pi
):
    extent = spacing.shape[1]
    steps = extent // SUB
    place = shuffled((extent, extent), 0)
    span = jnp.sum(jnp.where(place, spacing[...], 0.0), axis=1, keepdims=True)
    both = jnp.concatenate([wide_in[...], narrow_in[...]], axis=0)
    rows = lax.dot_general(
        place.astype(jnp.float32).astype(jnp.bfloat16),
        both,
        (((1,), (1,)), ((), ())),
        preferred_element_type=jnp.float32,
    ).astype(jnp.bfloat16)
    inputs[...] = rows
    channels = wide_in.shape[0]
    halves = ((rows[:, :channels], dw, rw.shape[1]), (rows[:, channels:], dn, rn.shape[1]))
    tiles = []
    for d in range(2):
        rate, turn = in_lanes(rw, rn, d), in_lanes(tw, tn, d)
        push = []
        for part in range(2):
            pieces = []
            for x, drive, groups in halves:
                high, low = spread(drive, d, part, groups)
                pieces.append(
                    jnp.dot(x, high, preferred_element_type=jnp.float32)
                    + jnp.dot(x, low, preferred_element_type=jnp.float32)
                )
            push.append(jnp.concatenate(pieces, axis=1))
        square = rate * rate + turn * turn
        back_real, back_quad = -rate / square, -turn / square
        decay_real, decay_quad = powers(rate, turn, span)
        coef_real, coef_quad = complex_times(decay_real - 1.0, decay_quad, back_real, back_quad)
        kick_real, kick_quad = complex_times(coef_real, coef_quad, push[0], push[1])
        order = range(steps) if d == 0 else range(steps - 1, -1, -1)
        state = None
        for i in order:
            at = slice(i * SUB, (i + 1) * SUB)
            decay = (decay_real[at], decay_quad[at])
            if state is None:
                state, power = (kick_real[at], kick_quad[at]), decay
            else:
                kept = complex_times(*decay, *state)
                state = (kept[0] + kick_real[at], kept[1] + kick_quad[at])
                power = complex_times(*decay, *power)
            sr[d, at, :] = state[0]
            si[d, at, :] = state[1]
            pr[d, at, :] = power[0]
            pi[d, at, :] = power[1]
        end = None
        for c in range(SUB) if d == 0 else range(SUB - 1, -1, -1):
            own = (state[0][c : c + 1], state[1][c : c + 1])
            if end is None:
                end = own
            else:
                kept = complex_times(power[0][c : c + 1], power[1][c : c + 1], *end)
                end = (kept[0] + own[0], kept[1] + own[1])
        count = end[0].shape[1] // LANES
        pieces = [e[:, k * LANES : (k + 1) * LANES] for e in end for k in range(count)]
        total = jnp.broadcast_to(jnp.sum(spacing[...], axis=1, keepdims=True), (1, LANES))
        lane = lax.broadcasted_iota(jnp.int32, (1, LANES), 1)
        length = jnp.zeros((1, LANES), jnp.float32)
        for k in range(3):
            addend = total.astype(jnp.bfloat16).astype(jnp.float32)
            length = jnp.where(lane == k, addend, length)
            total = total - addend
        pieces.append(length)
        pieces.append(jnp.zeros((SUB - len(pieces), LANES), jnp.float32))
        tiles.append(jnp.concatenate(pieces, axis=0))
    for j in range(out.shape[0]):
        out[j] = jnp.where(j > mine[0], tiles[0], tiles[1]).astype(out.dtype)


def carried(mine, arrived, rates, turns, count):
    peers = arrived.shape[0]
    quads = 2 * count

    def tile(row):
        pieces = [row[:, k * LANES : (k + 1) * LANES] for k in range(count)] * 2
        pieces.append(jnp.zeros((SUB - quads, LANES), jnp.float32))
        return jnp.concatenate(pieces, axis=0)

    rates, turns = [tile(r) for r in rates], [tile(t) for t in turns]
    ends = [arrived[j].astype(jnp.float32) for j in range(peers)]
    spans = [jnp.sum(e[quads : quads + 1], axis=1, keepdims=True) for e in ends]
    spans = [jnp.broadcast_to(x, (1, LANES)) for x in spans]
    zero = jnp.zeros((1, LANES), jnp.float32)
    before, after = [zero] * peers, [zero] * peers
    for j in range(peers - 2, -1, -1):
        before[j] = jnp.where(j + 1 < mine, before[j + 1] + spans[j + 1], zero)
    for j in range(1, peers):
        after[j] = jnp.where(j - 1 > mine, after[j - 1] + spans[j - 1], zero)
    sums = [jnp.zeros((SUB, LANES), jnp.float32)] * 2
    for j in range(peers):
        early, late = j < mine, j > mine
        gap = jnp.where(early, before[j], after[j])
        weight = powers(
            jnp.where(early, rates[0], rates[1]), jnp.where(early, turns[0], turns[1]), gap
        )
        end = ends[j]
        crossed = jnp.concatenate([-end[count:quads], end[:count], end[quads:]], axis=0)
        term = weight[0] * end + weight[1] * crossed
        sums[0] = sums[0] + jnp.where(early, term, 0.0)
        sums[1] = sums[1] + jnp.where(late, term, 0.0)
    out = []
    for s in sums:
        row = [s[k : k + 1] for k in range(quads)]
        out.append((jnp.concatenate(row[:count], axis=1), jnp.concatenate(row[count:], axis=1)))
    return out


def reading_kernel(
    mine, arrived, rw, tw, dw, rn, tn, dn, skip, inputs, sr, si, pr, pi, out
):
    extent = inputs.shape[0]
    steps = extent // SUB
    count = sr.shape[2] // LANES
    rates = [in_lanes(rw, rn, d) for d in range(2)]
    turns = [in_lanes(tw, tn, d) for d in range(2)]
    carries = carried(mine[0], arrived, rates, turns, count)
    channels = dw.shape[1]
    reading = [jnp.zeros((extent, channels), jnp.float32) for _ in range(2)]
    for d in range(2):
        last = slice((steps - 1) * SUB, extent) if d == 0 else slice(0, SUB)
        state, power = (sr[d, last, :], si[d, last, :]), (pr[d, last, :], pi[d, last, :])
        carry, starts = carries[d], [None] * SUB
        for c in range(SUB) if d == 0 else range(SUB - 1, -1, -1):
            starts[c] = carry
            at = slice(c, c + 1)
            kept = complex_times(power[0][at], power[1][at], *carry)
            carry = (kept[0] + state[0][at], kept[1] + state[1][at])
        start = [jnp.concatenate([s[k] for s in starts], axis=0) for k in range(2)]
        start = [jnp.concatenate([s] * steps, axis=0) for s in start]
        extra = complex_times(pr[d], pi[d], *start)
        at = 0
        for which, (read, groups) in enumerate(((dw, rw.shape[1]), (dn, rn.shape[1]))):
            upto = at + groups * read.shape[2] // 2
            for part, local in enumerate((sr, si)):
                value = local[d, :, at:upto] + extra[part][:, at:upto]
                high, low = two_terms(value)
                read_high, read_low = spread(read, d, part, groups)
                for x, y in ((high, read_high), (low, read_high), (high, read_low)):
                    reading[which] = reading[which] + lax.dot_general(
                        x, y, (((1,), (1,)), ((), ())), preferred_element_type=jnp.float32
                    )
            at = upto
    total = jnp.concatenate(reading, axis=1) + skip[...] * inputs[...].astype(jnp.float32)
    mixed = jax.nn.gelu(total).astype(jnp.bfloat16)
    back = shuffled((extent, extent), 1).astype(jnp.float32).astype(jnp.bfloat16)
    rows = jnp.dot(back, mixed, preferred_element_type=jnp.float32).astype(jnp.bfloat16)
    for k in range(out.shape[0]):
        out[k] = rows


def in_memory(count):
    vmem = pl.BlockSpec(memory_space=pltpu.VMEM)
    return [pl.BlockSpec(memory_space=pltpu.SMEM)] + [vmem] * count


def mixer(input_wide, input_narrow, spacing, wide, narrow, skip_gain):
    extent, channels = input_wide.shape
    rw, tw, dw, cw = wide
    rn, tn, dn, cn = narrow
    dw, cw, dn, cn = (m.reshape(2, channels, m.shape[3]) for m in (dw, cw, dn, cn))
    states = rw.shape[1] * rw.shape[2] + rn.shape[1] * rn.shape[2]
    mine = lax.axis_index(SP).astype(jnp.int32).reshape(1)
    f32 = functools.partial(jax.ShapeDtypeStruct, dtype=jnp.float32)
    table = f32((2, extent, states))
    cost = pl.CostEstimate(flops=20_000_000, bytes_accessed=2_000_000, transcendentals=100_000)
    out, inputs, *tables = pl.pallas_call(
        local_kernel,
        name="local_states",
        out_shape=(
            jax.ShapeDtypeStruct((lax.axis_size(SP), SUB, LANES), jnp.bfloat16),
            jax.ShapeDtypeStruct((extent, 2 * channels), jnp.bfloat16),
            table,
            table,
            table,
            table,
        ),
        in_specs=in_memory(9),
        out_specs=tuple(in_memory(6)[1:]),
        cost_estimate=cost,
    )(mine, input_wide.T, input_narrow.T, spacing.reshape(1, -1), rw, tw, dw, rn, tn, dn)
    arrived = lax.all_to_all(out, SP, split_axis=0, concat_axis=0, tiled=True)
    return pl.pallas_call(
        reading_kernel,
        name="readings",
        out_shape=jax.ShapeDtypeStruct(
            (lax.axis_size("tp"), extent, 2 * channels), jnp.bfloat16
        ),
        in_specs=in_memory(13),
        out_specs=in_memory(1)[1],
        cost_estimate=cost,
    )(mine, arrived, rw, tw, cw, rn, tn, cn, skip_gain.reshape(1, -1), inputs, *tables)


def on_device(
    input_wide,
    input_narrow,
    spacing,
    rate_wide,
    turn_wide,
    drive_wide,
    read_wide,
    narrow_decay_rate,
    turn_narrow,
    drive_narrow,
    read_narrow,
    skip_gain,
    out_value,
    out_gate,
    stream,
    norm_gain,
    up_value,
    up_gate,
    conv_taps,
    down_weight,
):
    pair, quads = lax.axis_size("zi"), lax.axis_size("gi")
    share = pair * quads
    extent = input_wide.shape[0]
    block, part = weight_block(up_value, up_gate, down_weight)
    block, input_wide, input_narrow, spacing = lax.optimization_barrier(
        (block, input_wide, input_narrow, spacing)
    )
    weights = lax.all_gather(block, "zp", axis=0, tiled=True)
    mixer_in = mixer(
        input_wide,
        input_narrow,
        spacing,
        (rate_wide, turn_wide, drive_wide, read_wide),
        (narrow_decay_rate, turn_narrow, drive_narrow, read_narrow),
        skip_gain,
    )
    channels = input_wide.shape[1]
    slots = lax.all_to_all(mixer_in, "tp", split_axis=0, concat_axis=0, tiled=True)
    peers = slots.shape[0]
    rows = jnp.moveaxis(slots, 0, 1).reshape(extent, -1)

    def by_slot(weight):
        turned = jnp.moveaxis(weight.reshape(2, peers, channels, -1), 0, 1)
        return turned.reshape(weight.shape)

    value = jnp.dot(rows, by_slot(out_value), preferred_element_type=jnp.float32)
    gate = jnp.dot(rows, by_slot(out_gate), preferred_element_type=jnp.float32)
    middle = (stream.astype(jnp.float32) + value * jax.nn.sigmoid(gate)).astype(jnp.bfloat16)
    count = lax.axis_size(SP)
    up, down = [(i, i + 1) for i in range(count - 1)], [(i + 1, i) for i in range(count - 1)]
    low = lax.ppermute(middle[-1:], SP, up)
    high = lax.ppermute(middle[:1], SP, down)
    gain_a = lax.reduce_precision(norm_gain, 8, 7)
    gain_b = lax.reduce_precision(norm_gain - gain_a, 8, 7)
    gain_c = norm_gain - gain_a - gain_b
    gains = jnp.stack([gain_a, gain_b, gain_c]).astype(jnp.bfloat16)
    sent = jnp.concatenate([middle, low, high, gains], axis=0)
    slots = sent_to_all(sent, MEMBERS)
    slots = slots.reshape(quads, pair, -1, *sent.shape)
    picked = [slots[:, 0, :, extent : extent + 1]]
    picked += [slots[:, k, :, :extent] for k in range(pair)]
    picked += [slots[:, pair - 1, :, extent + 1 : extent + 2]]
    whole = jnp.moveaxis(jnp.concatenate(picked, axis=2), 1, 2)
    whole = whole.reshape(quads * (pair * extent + 2), -1).astype(jnp.float32)
    gain = jnp.sum(slots[0, 0, :, extent + 2 :].astype(jnp.float32), axis=1).reshape(-1)
    mean = jnp.mean(whole * whole, axis=1, keepdims=True)
    normed = (whole * lax.rsqrt(mean + epsilon) * gain).astype(jnp.bfloat16)
    width = lanes_up(2 * part)
    pre = jnp.dot(normed, weights[:, :width], preferred_element_type=jnp.float32)
    pre = pre.astype(jnp.bfloat16).reshape(quads, -1, width)
    taps = conv_taps.reshape(2, 3, share, -1)
    mine = lax.axis_index("gi") * pair + lax.axis_index("zi")
    taps = lax.dynamic_index_in_dim(taps, mine, 2, keepdims=False)
    taps = padded_last(jnp.moveaxis(taps, 0, 1).reshape(3, -1), width)
    conv = taps[0] * pre[:, :-2] + taps[1] * pre[:, 1:-1] + taps[2] * pre[:, 2:]
    conv = conv.reshape(share * extent, width)
    hidden = (jax.nn.silu(conv[:, part : 2 * part]) * conv[:, :part]).astype(jnp.bfloat16)
    terms = lax.dot_general(
        hidden,
        weights[:, 2 * part : 3 * part],
        (((1,), (1,)), ((), ())),
        preferred_element_type=jnp.float32,
    ).astype(jnp.bfloat16)
    terms = terms.reshape(share, extent, peers, -1)
    terms = jnp.moveaxis(terms, 2, 1).reshape(share * peers, extent, -1)
    arrived = lax.all_to_all(terms, MEMBERS, split_axis=0, concat_axis=0, tiled=True)
    ffn = jnp.sum(arrived.astype(jnp.float32), axis=0)
    return (middle.astype(jnp.float32) + ffn).astype(jnp.bfloat16)


def solution(mesh):
    grp, sp, tp = mesh.devices.shape
    quads = SHARE if grp % SHARE == 0 else 1
    parted = Mesh(
        mesh.devices.reshape(grp // quads, quads, sp // SHARE, SHARE, tp),
        ("gp", "gi", *SP, "tp"),
    )
    spot = ("gp", "gi", *SP)
    placed = (
        P(spot, "tp"),
        P(spot, "tp"),
        P(spot),
        P(None, "tp", None),
        P(None, "tp", None),
        P(None, "tp", None, None),
        P(None, "tp", None, None),
        P(None, "tp", None),
        P(None, "tp", None),
        P(None, "tp", None, None),
        P(None, "tp", None, None),
        P(None, "tp"),
        P(None, "tp"),
        P(None, "tp"),
        P(spot, "tp"),
        P("tp"),
        P(SP, "tp"),
        P(SP, "tp"),
        P(None, None, "tp"),
        P("tp", SP),
    )
    return jax.shard_map(
        on_device, mesh=parted, in_specs=placed, out_specs=P(spot, "tp"), check_vma=False
    )
```

```python
import functools
import math

import jax
import jax.numpy as jnp
from jax import lax
from jax.experimental import pallas as pl
from jax.experimental.pallas import tpu as pltpu
from jax.sharding import Mesh
from jax.sharding import PartitionSpec as P

SHARE = 2
LANES = 128
SUB = 8
EXTRA = 16

epsilon = 1e-06
SP = ("zp", "zi")
MEMBERS = ("gi", "zi", "tp")


def complex_times(left_real, left_quad, right_real, right_quad):
    return (
        left_real * right_real - left_quad * right_quad,
        left_real * right_quad + left_quad * right_real,
    )


def lanes_up(count):
    return -(-count // LANES) * LANES


def padded_last(array, width):
    return jnp.pad(array, [(0, 0)] * (array.ndim - 1) + [(0, width - array.shape[-1])])


def sent_to_all(array, axes):
    copies = jnp.broadcast_to(array, (lax.axis_size(axes), *array.shape))
    return lax.all_to_all(copies, axes, split_axis=0, concat_axis=0, tiled=True)


def pack_kernel(quads, which, value, gate, down, out):
    pair, rows, width = out.shape
    part = value.shape[1] // (pair * quads)
    for k in range(pair):
        pieces = []
        for w in (value, gate, down):
            own = None
            for q in range(quads):
                at = (q * pair + k) * part
                piece = w[:, at : at + part].astype(jnp.float32)
                own = piece if own is None else jnp.where(which[0] == q, piece, own)
            pieces.append(own)
        if width > 3 * part:
            pieces.append(jnp.zeros((rows, width - 3 * part), jnp.float32))
        out[k] = jnp.concatenate(pieces, axis=1).astype(out.dtype)


def weight_block(up_value, up_gate, down_weight):
    pair, quads = lax.axis_size("zi"), lax.axis_size("gi")
    rows, columns = up_value.shape
    part = columns // (pair * quads)
    which = lax.axis_index("gi").astype(jnp.int32).reshape(1)
    block = pl.pallas_call(
        functools.partial(pack_kernel, quads),
        name="pack",
        out_shape=jax.ShapeDtypeStruct((pair, rows, lanes_up(3 * part)), jnp.bfloat16),
        in_specs=in_memory(3),
        out_specs=in_memory(1)[1],
    )(which, up_value, up_gate, down_weight.T)
    block = lax.all_to_all(block, "zi", 0, 0, tiled=True)
    return block.reshape(pair * rows, -1), part


def cos_sin(turn, span):
    turns = (turn * (0.5 / math.pi)) * span
    half = (turns - jnp.floor(turns + 0.5)) * math.pi
    square = half * half
    sine, cosine = 1.0 / math.factorial(13), 1.0 / math.factorial(12)
    for k in range(11, 0, -2):
        sine = sine * square + (-1.0) ** (k // 2) / math.factorial(k)
    for k in range(10, -1, -2):
        cosine = cosine * square + (-1.0) ** (k // 2) / math.factorial(k)
    sine = sine * half
    return 1.0 - 2.0 * sine * sine, 2.0 * sine * cosine


def powers(rate, turn, span):
    shrink = jnp.exp(-rate * span)
    cosine, sine = cos_sin(turn, span)
    return shrink * cosine, shrink * sine


def in_lanes(wide, narrow, d):
    rows = [ref[d, k : k + 1, :] for ref in (wide, narrow) for k in range(ref.shape[1])]
    return jnp.concatenate(rows, axis=1)


def two_terms(x):
    high = x.astype(jnp.bfloat16)
    return high, (x - high.astype(jnp.float32)).astype(jnp.bfloat16)


def spread(ref, d, part, groups):
    states = ref.shape[2] // 2
    own = ref[d][:, part * states : (part + 1) * states]
    wide = jnp.concatenate([own] * groups, axis=1)
    row = lax.broadcasted_iota(jnp.int32, wide.shape, 0) // (wide.shape[0] // groups)
    lane = lax.broadcasted_iota(jnp.int32, wide.shape, 1) // states
    return two_terms(jnp.where(row == lane, wide, 0.0))


def shuffled(size, extent, row_axis):
    row = lax.broadcasted_iota(jnp.int32, (size, size), row_axis)
    position = lax.broadcasted_iota(jnp.int32, (size, size), 1 - row_axis)
    moved = (row % SUB) * (extent // SUB) + row // SUB
    return position == jnp.where(row < extent, moved, row)


def local_kernel(
    mine, wide_in, narrow_in, spacing, rw, tw, dw, rn, tn, dn, out, inputs, sr, si, pr, pi
):
    extent = spacing.shape[1]
    steps = extent // SUB
    place = shuffled(extent, extent, 0)
    span = jnp.sum(jnp.where(place, spacing[...], 0.0), axis=1, keepdims=True)
    both = jnp.concatenate([wide_in[...], narrow_in[...]], axis=0)
    rows = lax.dot_general(
        place.astype(jnp.float32).astype(jnp.bfloat16),
        both,
        (((1,), (1,)), ((), ())),
        preferred_element_type=jnp.float32,
    ).astype(jnp.bfloat16)
    inputs[...] = rows
    channels = wide_in.shape[0]
    halves = ((rows[:, :channels], dw, rw.shape[1]), (rows[:, channels:], dn, rn.shape[1]))
    tiles = []
    for d in range(2):
        rate, turn = in_lanes(rw, rn, d), in_lanes(tw, tn, d)
        push = []
        for part in range(2):
            pieces = []
            for x, drive, groups in halves:
                high, low = spread(drive, d, part, groups)
                pieces.append(
                    jnp.dot(x, high, preferred_element_type=jnp.float32)
                    + jnp.dot(x, low, preferred_element_type=jnp.float32)
                )
            push.append(jnp.concatenate(pieces, axis=1))
        square = rate * rate + turn * turn
        back_real, back_quad = -rate / square, -turn / square
        decay_real, decay_quad = powers(rate, turn, span)
        coef_real, coef_quad = complex_times(decay_real - 1.0, decay_quad, back_real, back_quad)
        kick_real, kick_quad = complex_times(coef_real, coef_quad, push[0], push[1])
        order = range(steps) if d == 0 else range(steps - 1, -1, -1)
        state = None
        for i in order:
            at = slice(i * SUB, (i + 1) * SUB)
            decay = (decay_real[at], decay_quad[at])
            if state is None:
                state, power = (kick_real[at], kick_quad[at]), decay
            else:
                kept = complex_times(*decay, *state)
                state = (kept[0] + kick_real[at], kept[1] + kick_quad[at])
                power = complex_times(*decay, *power)
            sr[d, at, :] = state[0]
            si[d, at, :] = state[1]
            pr[d, at, :] = power[0]
            pi[d, at, :] = power[1]
        end = None
        for c in range(SUB) if d == 0 else range(SUB - 1, -1, -1):
            own = (state[0][c : c + 1], state[1][c : c + 1])
            if end is None:
                end = own
            else:
                kept = complex_times(power[0][c : c + 1], power[1][c : c + 1], *end)
                end = (kept[0] + own[0], kept[1] + own[1])
        count = end[0].shape[1] // LANES
        pieces = [e[:, k * LANES : (k + 1) * LANES] for e in end for k in range(count)]
        total = jnp.broadcast_to(jnp.sum(spacing[...], axis=1, keepdims=True), (1, LANES))
        lane = lax.broadcasted_iota(jnp.int32, (1, LANES), 1)
        length = jnp.zeros((1, LANES), jnp.float32)
        for k in range(3):
            addend = total.astype(jnp.bfloat16).astype(jnp.float32)
            length = jnp.where(lane == k, addend, length)
            total = total - addend
        pieces.append(length)
        pieces.append(jnp.zeros((SUB - len(pieces), LANES), jnp.float32))
        tiles.append(jnp.concatenate(pieces, axis=0))
    for j in range(out.shape[0]):
        out[j] = jnp.where(j > mine[0], tiles[0], tiles[1]).astype(out.dtype)


def addends(x):
    first = lax.reduce_precision(x, 8, 7)
    second = lax.reduce_precision(x - first, 8, 7)
    return jnp.stack([first, second, x - first - second]).astype(jnp.bfloat16)


def beside_kernel(low, high, rw, tw, dw, rn, tn, dn, steps_out, rows_out):
    rows = jnp.concatenate([low[0:1], high[0:1]], axis=0).astype(jnp.float32)
    rows = jnp.concatenate([rows, jnp.zeros((EXTRA - 2, rows.shape[1]), jnp.float32)], axis=0)
    rows = rows.astype(jnp.bfloat16)
    rows_out[...] = rows
    channels = dw.shape[1]
    halves = ((rows[:, :channels], dw, rw.shape[1]), (rows[:, channels:], dn, rn.shape[1]))
    out = []
    for row, (d, side) in enumerate(((1, low), (0, high))):
        rate, turn = in_lanes(rw, rn, d), in_lanes(tw, tn, d)
        span = jnp.sum(side[2:3].astype(jnp.float32), axis=1, keepdims=True)
        push = []
        for part in range(2):
            pieces = []
            for x, drive, groups in halves:
                first, second = spread(drive, d, part, groups)
                pieces.append(
                    jnp.dot(x, first, preferred_element_type=jnp.float32)
                    + jnp.dot(x, second, preferred_element_type=jnp.float32)
                )
            push.append(jnp.concatenate(pieces, axis=1)[row : row + 1])
        square = rate * rate + turn * turn
        decay = powers(rate, turn, jnp.broadcast_to(span, rate.shape))
        coef = complex_times(decay[0] - 1.0, decay[1], -rate / square, -turn / square)
        out += [*decay, *complex_times(*coef, *push)]
    steps_out[...] = jnp.concatenate(out, axis=0)


def carried(mine, arrived, rates, turns, count):
    peers = arrived.shape[0]
    quads = 2 * count

    def tile(row):
        pieces = [row[:, k * LANES : (k + 1) * LANES] for k in range(count)] * 2
        pieces.append(jnp.zeros((SUB - quads, LANES), jnp.float32))
        return jnp.concatenate(pieces, axis=0)

    rates, turns = [tile(r) for r in rates], [tile(t) for t in turns]
    ends = [arrived[j].astype(jnp.float32) for j in range(peers)]
    spans = [jnp.sum(e[quads : quads + 1], axis=1, keepdims=True) for e in ends]
    spans = [jnp.broadcast_to(x, (1, LANES)) for x in spans]
    zero = jnp.zeros((1, LANES), jnp.float32)
    before, after = [zero] * peers, [zero] * peers
    for j in range(peers - 2, -1, -1):
        before[j] = jnp.where(j + 1 < mine, before[j + 1] + spans[j + 1], zero)
    for j in range(1, peers):
        after[j] = jnp.where(j - 1 > mine, after[j - 1] + spans[j - 1], zero)
    sums = [jnp.zeros((SUB, LANES), jnp.float32)] * 2
    for j in range(peers):
        early, late = j < mine, j > mine
        gap = jnp.where(early, before[j], after[j])
        weight = powers(
            jnp.where(early, rates[0], rates[1]), jnp.where(early, turns[0], turns[1]), gap
        )
        end = ends[j]
        crossed = jnp.concatenate([-end[count:quads], end[:count], end[quads:]], axis=0)
        term = weight[0] * end + weight[1] * crossed
        sums[0] = sums[0] + jnp.where(early, term, 0.0)
        sums[1] = sums[1] + jnp.where(late, term, 0.0)
    out = []
    for s in sums:
        row = [s[k : k + 1] for k in range(quads)]
        out.append((jnp.concatenate(row[:count], axis=1), jnp.concatenate(row[count:], axis=1)))
    return out


def reading_kernel(
    mine, arrived, rw, tw, dw, rn, tn, dn, skip, inputs, beside, more, sr, si, pr, pi, out
):
    extent = inputs.shape[0]
    steps = extent // SUB
    count = sr.shape[2] // LANES
    rates = [in_lanes(rw, rn, d) for d in range(2)]
    turns = [in_lanes(tw, tn, d) for d in range(2)]
    carries = carried(mine[0], arrived, rates, turns, count)
    channels = dw.shape[1]
    size = extent + EXTRA
    reading = [jnp.zeros((size, channels), jnp.float32) for _ in range(2)]
    for d in range(2):
        last = slice((steps - 1) * SUB, extent) if d == 0 else slice(0, SUB)
        state, power = (sr[d, last, :], si[d, last, :]), (pr[d, last, :], pi[d, last, :])
        carry, starts = carries[d], [None] * SUB
        for c in range(SUB) if d == 0 else range(SUB - 1, -1, -1):
            starts[c] = carry
            at = slice(c, c + 1)
            kept = complex_times(power[0][at], power[1][at], *carry)
            carry = (kept[0] + state[0][at], kept[1] + state[1][at])
        start = [jnp.concatenate([s[k] for s in starts], axis=0) for k in range(2)]
        start = [jnp.concatenate([s] * steps, axis=0) for s in start]
        extra = complex_times(pr[d], pi[d], *start)
        step = [more[k : k + 1, :] for k in range(4 * (1 - d), 4 * (1 - d) + 4)]
        beyond = complex_times(*step[:2], *carry)
        beyond = [beyond[k] + step[2 + k] for k in range(2)]
        pairs = zip(carries[d], beyond) if d == 0 else zip(beyond, carries[d])
        spare = jnp.zeros((EXTRA - 2, carry[0].shape[1]), jnp.float32)
        tail = [jnp.concatenate([*pair, spare], axis=0) for pair in pairs]
        at = 0
        for which, (read, groups) in enumerate(((dw, rw.shape[1]), (dn, rn.shape[1]))):
            upto = at + groups * read.shape[2] // 2
            for part, local in enumerate((sr, si)):
                value = local[d, :, at:upto] + extra[part][:, at:upto]
                value = jnp.concatenate([value, tail[part][:, at:upto]], axis=0)
                high, low = two_terms(value)
                read_high, read_low = spread(read, d, part, groups)
                for x, y in ((high, read_high), (low, read_high), (high, read_low)):
                    reading[which] = reading[which] + lax.dot_general(
                        x, y, (((1,), (1,)), ((), ())), preferred_element_type=jnp.float32
                    )
            at = upto
    rows = jnp.concatenate([inputs[...], beside[...]], axis=0).astype(jnp.float32)
    total = jnp.concatenate(reading, axis=1) + skip[...] * rows
    mixed = jax.nn.gelu(total).astype(jnp.bfloat16)
    back = shuffled(size, extent, 1).astype(jnp.float32).astype(jnp.bfloat16)
    rows = jnp.dot(back, mixed, preferred_element_type=jnp.float32).astype(jnp.bfloat16)
    for k in range(out.shape[0]):
        out[k] = rows


def in_memory(count):
    vmem = pl.BlockSpec(memory_space=pltpu.VMEM)
    return [pl.BlockSpec(memory_space=pltpu.SMEM)] + [vmem] * count


def mixer(input_wide, input_narrow, spacing, stream, wide, narrow, skip_gain):
    extent, channels = input_wide.shape
    rw, tw, dw, cw = wide
    rn, tn, dn, cn = narrow
    dw, cw, dn, cn = (m.reshape(2, channels, m.shape[3]) for m in (dw, cw, dn, cn))
    states = rw.shape[1] * rw.shape[2] + rn.shape[1] * rn.shape[2]
    mine = lax.axis_index(SP).astype(jnp.int32).reshape(1)
    f32 = functools.partial(jax.ShapeDtypeStruct, dtype=jnp.float32)
    table = f32((2, extent, states))
    cost = pl.CostEstimate(flops=20_000_000, bytes_accessed=2_000_000, transcendentals=100_000)
    out, inputs, *tables = pl.pallas_call(
        local_kernel,
        name="local_states",
        out_shape=(
            jax.ShapeDtypeStruct((lax.axis_size(SP), SUB, LANES), jnp.bfloat16),
            jax.ShapeDtypeStruct((extent, 2 * channels), jnp.bfloat16),
            table,
            table,
            table,
            table,
        ),
        in_specs=in_memory(9),
        out_specs=tuple(in_memory(6)[1:]),
        cost_estimate=cost,
    )(mine, input_wide.T, input_narrow.T, spacing.reshape(1, -1), rw, tw, dw, rn, tn, dn)
    both = jnp.concatenate([input_wide, input_narrow], axis=1)

    def edge(at):
        length = addends(spacing[at : at + 1])[:, 0]
        length = padded_last(length.reshape(1, -1), both.shape[1])
        return jnp.concatenate([both[at : at + 1], stream[at : at + 1], length], axis=0)

    out, last, first = lax.optimization_barrier((out, edge(extent - 1), edge(0)))
    with jax.named_scope("exchange"):
        arrived = lax.all_to_all(out, SP, split_axis=0, concat_axis=0, tiled=True)
    count = lax.axis_size(SP)
    with jax.named_scope("low"):
        low = lax.ppermute(last, SP, [(i, i + 1) for i in range(count - 1)])
    with jax.named_scope("high"):
        high = lax.ppermute(first, SP, [(i + 1, i) for i in range(count - 1)])
    more, beside = pl.pallas_call(
        beside_kernel,
        name="beside",
        out_shape=(f32((8, states)), jax.ShapeDtypeStruct((EXTRA, 2 * channels), jnp.bfloat16)),
        in_specs=in_memory(8)[1:],
        out_specs=tuple(in_memory(2)[1:]),
        cost_estimate=cost,
    )(low, high, rw, tw, dw, rn, tn, dn)
    slots = pl.pallas_call(
        reading_kernel,
        name="readings",
        out_shape=jax.ShapeDtypeStruct(
            (lax.axis_size("tp"), extent + EXTRA, 2 * channels), jnp.bfloat16
        ),
        in_specs=in_memory(15),
        out_specs=in_memory(1)[1],
        cost_estimate=cost,
    )(mine, arrived, rw, tw, cw, rn, tn, cn, skip_gain.reshape(1, -1), inputs, beside, more, *tables)
    return slots, low[1:2], high[1:2]


def on_device(
    input_wide,
    input_narrow,
    spacing,
    rate_wide,
    turn_wide,
    drive_wide,
    read_wide,
    narrow_decay_rate,
    turn_narrow,
    drive_narrow,
    read_narrow,
    skip_gain,
    out_value,
    out_gate,
    stream,
    norm_gain,
    up_value,
    up_gate,
    conv_taps,
    down_weight,
):
    pair, quads = lax.axis_size("zi"), lax.axis_size("gi")
    share = pair * quads
    extent = input_wide.shape[0]
    block, part = weight_block(up_value, up_gate, down_weight)
    block, input_wide, input_narrow, spacing = lax.optimization_barrier(
        (block, input_wide, input_narrow, spacing)
    )
    weights = lax.all_gather(block, "zp", axis=0, tiled=True)
    mixer_in, low, high = mixer(
        input_wide,
        input_narrow,
        spacing,
        stream,
        (rate_wide, turn_wide, drive_wide, read_wide),
        (narrow_decay_rate, turn_narrow, drive_narrow, read_narrow),
        skip_gain,
    )
    channels = input_wide.shape[1]
    slots = lax.all_to_all(mixer_in, "tp", split_axis=0, concat_axis=0, tiled=True)
    peers = slots.shape[0]
    rows = jnp.moveaxis(slots, 0, 1).reshape(extent + EXTRA, -1)

    def by_slot(weight):
        turned = jnp.moveaxis(weight.reshape(2, peers, channels, -1), 0, 1)
        return turned.reshape(weight.shape)

    value = jnp.dot(rows, by_slot(out_value), preferred_element_type=jnp.float32)
    gate = jnp.dot(rows, by_slot(out_gate), preferred_element_type=jnp.float32)
    mine, count = lax.axis_index(SP), lax.axis_size(SP)
    row = jnp.arange(extent + 2)[:, None]
    inside = ((row != extent) | (mine > 0)) & ((row != extent + 1) | (mine < count - 1))
    branch = (value * jax.nn.sigmoid(gate))[: extent + 2]
    middle = jnp.concatenate([stream, low, high], axis=0).astype(jnp.float32) + branch
    middle = jnp.where(inside, middle, 0.0).astype(jnp.bfloat16)
    sent = jnp.concatenate([middle, addends(norm_gain)], axis=0)
    middle = middle[:extent]
    slots = sent_to_all(sent, MEMBERS)
    slots = slots.reshape(quads, pair, -1, *sent.shape)
    picked = [slots[:, 0, :, extent : extent + 1]]
    picked += [slots[:, k, :, :extent] for k in range(pair)]
    picked += [slots[:, pair - 1, :, extent + 1 : extent + 2]]
    whole = jnp.moveaxis(jnp.concatenate(picked, axis=2), 1, 2)
    whole = whole.reshape(quads * (pair * extent + 2), -1).astype(jnp.float32)
    gain = jnp.sum(slots[0, 0, :, extent + 2 :].astype(jnp.float32), axis=1).reshape(-1)
    mean = jnp.mean(whole * whole, axis=1, keepdims=True)
    normed = (whole * lax.rsqrt(mean + epsilon) * gain).astype(jnp.bfloat16)
    width = lanes_up(2 * part)
    pre = jnp.dot(normed, weights[:, :width], preferred_element_type=jnp.float32)
    pre = pre.astype(jnp.bfloat16).reshape(quads, -1, width)
    taps = conv_taps.reshape(2, 3, share, -1)
    mine = lax.axis_index("gi") * pair + lax.axis_index("zi")
    taps = lax.dynamic_index_in_dim(taps, mine, 2, keepdims=False)
    taps = padded_last(jnp.moveaxis(taps, 0, 1).reshape(3, -1), width)
    conv = taps[0] * pre[:, :-2] + taps[1] * pre[:, 1:-1] + taps[2] * pre[:, 2:]
    conv = conv.reshape(share * extent, width)
    hidden = (jax.nn.silu(conv[:, part : 2 * part]) * conv[:, :part]).astype(jnp.bfloat16)
    terms = lax.dot_general(
        hidden,
        weights[:, 2 * part : 3 * part],
        (((1,), (1,)), ((), ())),
        preferred_element_type=jnp.float32,
    ).astype(jnp.bfloat16)
    terms = terms.reshape(share, extent, peers, -1)
    terms = jnp.moveaxis(terms, 2, 1).reshape(share * peers, extent, -1)
    arrived = lax.all_to_all(terms, MEMBERS, split_axis=0, concat_axis=0, tiled=True)
    ffn = jnp.sum(arrived.astype(jnp.float32), axis=0)
    return (middle.astype(jnp.float32) + ffn).astype(jnp.bfloat16)


def solution(mesh):
    grp, sp, tp = mesh.devices.shape
    quads = SHARE if grp % SHARE == 0 else 1
    parted = Mesh(
        mesh.devices.reshape(grp // quads, quads, sp // SHARE, SHARE, tp),
        ("gp", "gi", *SP, "tp"),
    )
    spot = ("gp", "gi", *SP)
    placed = (
        P(spot, "tp"),
        P(spot, "tp"),
        P(spot),
        P(None, "tp", None),
        P(None, "tp", None),
        P(None, "tp", None, None),
        P(None, "tp", None, None),
        P(None, "tp", None),
        P(None, "tp", None),
        P(None, "tp", None, None),
        P(None, "tp", None, None),
        P(None, "tp"),
        P(None, "tp"),
        P(None, "tp"),
        P(spot, "tp"),
        P("tp"),
        P(SP, "tp"),
        P(SP, "tp"),
        P(None, None, "tp"),
        P("tp", SP),
    )
    return jax.shard_map(
        on_device, mesh=parted, in_specs=placed, out_specs=P(spot, "tp"), check_vma=False
    )
```

```python
import functools
import math

import jax
import jax.numpy as jnp
from jax import lax
from jax.experimental import pallas as pl
from jax.experimental.pallas import tpu as pltpu
from jax.sharding import Mesh
from jax.sharding import PartitionSpec as P

SHARE = 2
LANES = 128
SUB = 8
EXTRA = 16

epsilon = 1e-06
SP = ("zp", "zi")
MEMBERS = ("gi", "zi", "tp")


def complex_times(left_real, left_quad, right_real, right_quad):
    return (
        left_real * right_real - left_quad * right_quad,
        left_real * right_quad + left_quad * right_real,
    )


def lanes_up(count):
    return -(-count // LANES) * LANES


def padded_last(array, width):
    return jnp.pad(array, [(0, 0)] * (array.ndim - 1) + [(0, width - array.shape[-1])])


def sent_to_all(array, axes):
    copies = jnp.broadcast_to(array, (lax.axis_size(axes), *array.shape))
    return lax.all_to_all(copies, axes, split_axis=0, concat_axis=0, tiled=True)


def pack_kernel(quads, which, value, gate, down, out):
    pair, rows, width = out.shape
    part = value.shape[1] // (pair * quads)
    for k in range(pair):
        pieces = []
        for w in (value, gate, down):
            own = None
            for q in range(quads):
                at = (q * pair + k) * part
                piece = w[:, at : at + part].astype(jnp.float32)
                own = piece if own is None else jnp.where(which[0] == q, piece, own)
            pieces.append(own)
        if width > 3 * part:
            pieces.append(jnp.zeros((rows, width - 3 * part), jnp.float32))
        out[k] = jnp.concatenate(pieces, axis=1).astype(out.dtype)


def weight_block(up_value, up_gate, down_weight):
    pair, quads = lax.axis_size("zi"), lax.axis_size("gi")
    rows, columns = up_value.shape
    part = columns // (pair * quads)
    which = lax.axis_index("gi").astype(jnp.int32).reshape(1)
    block = pl.pallas_call(
        functools.partial(pack_kernel, quads),
        name="pack",
        out_shape=jax.ShapeDtypeStruct((pair, rows, lanes_up(3 * part)), jnp.bfloat16),
        in_specs=in_memory(3),
        out_specs=in_memory(1)[1],
    )(which, up_value, up_gate, down_weight.T)
    block = lax.all_to_all(block, "zi", 0, 0, tiled=True)
    return block.reshape(pair * rows, -1), part


def cos_sin(turn, span):
    turns = (turn * (0.5 / math.pi)) * span
    half = (turns - jnp.floor(turns + 0.5)) * math.pi
    square = half * half
    sine, cosine = 1.0 / math.factorial(13), 1.0 / math.factorial(12)
    for k in range(11, 0, -2):
        sine = sine * square + (-1.0) ** (k // 2) / math.factorial(k)
    for k in range(10, -1, -2):
        cosine = cosine * square + (-1.0) ** (k // 2) / math.factorial(k)
    sine = sine * half
    return 1.0 - 2.0 * sine * sine, 2.0 * sine * cosine


def powers(rate, turn, span):
    shrink = jnp.exp(-rate * span)
    cosine, sine = cos_sin(turn, span)
    return shrink * cosine, shrink * sine


def in_lanes(wide, narrow, d):
    rows = [ref[d, k : k + 1, :] for ref in (wide, narrow) for k in range(ref.shape[1])]
    return jnp.concatenate(rows, axis=1)


def two_terms(x):
    high = x.astype(jnp.bfloat16)
    return high, (x - high.astype(jnp.float32)).astype(jnp.bfloat16)


def spread(ref, d, part, groups):
    states = ref.shape[2] // 2
    own = ref[d][:, part * states : (part + 1) * states]
    wide = jnp.concatenate([own] * groups, axis=1)
    row = lax.broadcasted_iota(jnp.int32, wide.shape, 0) // (wide.shape[0] // groups)
    lane = lax.broadcasted_iota(jnp.int32, wide.shape, 1) // states
    return two_terms(jnp.where(row == lane, wide, 0.0))


def shuffled(size, extent, row_axis):
    row = lax.broadcasted_iota(jnp.int32, (size, size), row_axis)
    position = lax.broadcasted_iota(jnp.int32, (size, size), 1 - row_axis)
    moved = (row % SUB) * (extent // SUB) + row // SUB
    return position == jnp.where(row < extent, moved, row)


def length_row(value):
    lane = lax.broadcasted_iota(jnp.int32, value.shape, 1)
    out = jnp.zeros(value.shape, jnp.float32)
    for k in range(3):
        addend = value.astype(jnp.bfloat16).astype(jnp.float32)
        out = jnp.where(lane == k, addend, out)
        value = value - addend
    return out


def local_kernel(
    mine, wide_in, narrow_in, spacing, stream, rw, tw, dw, rn, tn, dn,
    out, inputs, last, first, sr, si, pr, pi
):
    extent = spacing.shape[1]
    steps = extent // SUB
    place = shuffled(extent, extent, 0)
    span = jnp.sum(jnp.where(place, spacing[...], 0.0), axis=1, keepdims=True)
    both = jnp.concatenate([wide_in[...], narrow_in[...]], axis=0)
    rows = lax.dot_general(
        place.astype(jnp.float32).astype(jnp.bfloat16),
        both,
        (((1,), (1,)), ((), ())),
        preferred_element_type=jnp.float32,
    ).astype(jnp.bfloat16)
    inputs[...] = rows
    for edge, at in ((first, 0), (last, extent - 1)):
        near = at // (2 * SUB) * (2 * SUB)
        pieces = [
            x[near : near + 2 * SUB].astype(jnp.float32)[at - near : at - near + 1]
            for x in (rows, stream[...])
        ]
        pieces.append(length_row(jnp.broadcast_to(span[at : at + 1], (1, LANES))))
        pieces.append(jnp.zeros((SUB - 3, LANES), jnp.float32))
        edge[...] = jnp.concatenate(pieces, axis=0).astype(edge.dtype)
    channels = wide_in.shape[0]
    halves = ((rows[:, :channels], dw, rw.shape[1]), (rows[:, channels:], dn, rn.shape[1]))
    tiles = []
    for d in range(2):
        rate, turn = in_lanes(rw, rn, d), in_lanes(tw, tn, d)
        push = []
        for part in range(2):
            pieces = []
            for x, drive, groups in halves:
                high, low = spread(drive, d, part, groups)
                pieces.append(
                    jnp.dot(x, high, preferred_element_type=jnp.float32)
                    + jnp.dot(x, low, preferred_element_type=jnp.float32)
                )
            push.append(jnp.concatenate(pieces, axis=1))
        square = rate * rate + turn * turn
        back_real, back_quad = -rate / square, -turn / square
        decay_real, decay_quad = powers(rate, turn, span)
        coef_real, coef_quad = complex_times(decay_real - 1.0, decay_quad, back_real, back_quad)
        kick_real, kick_quad = complex_times(coef_real, coef_quad, push[0], push[1])
        order = range(steps) if d == 0 else range(steps - 1, -1, -1)
        state = None
        for i in order:
            at = slice(i * SUB, (i + 1) * SUB)
            decay = (decay_real[at], decay_quad[at])
            if state is None:
                state, power = (kick_real[at], kick_quad[at]), decay
            else:
                kept = complex_times(*decay, *state)
                state = (kept[0] + kick_real[at], kept[1] + kick_quad[at])
                power = complex_times(*decay, *power)
            sr[d, at, :] = state[0]
            si[d, at, :] = state[1]
            pr[d, at, :] = power[0]
            pi[d, at, :] = power[1]
        end = None
        for c in range(SUB) if d == 0 else range(SUB - 1, -1, -1):
            own = (state[0][c : c + 1], state[1][c : c + 1])
            if end is None:
                end = own
            else:
                kept = complex_times(power[0][c : c + 1], power[1][c : c + 1], *end)
                end = (kept[0] + own[0], kept[1] + own[1])
        count = end[0].shape[1] // LANES
        pieces = [e[:, k * LANES : (k + 1) * LANES] for e in end for k in range(count)]
        total = jnp.sum(spacing[...], axis=1, keepdims=True)
        pieces.append(length_row(jnp.broadcast_to(total, (1, LANES))))
        pieces.append(jnp.zeros((SUB - len(pieces), LANES), jnp.float32))
        tiles.append(jnp.concatenate(pieces, axis=0))
    for j in range(out.shape[0]):
        out[j] = jnp.where(j > mine[0], tiles[0], tiles[1]).astype(out.dtype)


def addends(x):
    first = lax.reduce_precision(x, 8, 7)
    second = lax.reduce_precision(x - first, 8, 7)
    return jnp.stack([first, second, x - first - second]).astype(jnp.bfloat16)


def beside_kernel(low, high, rw, tw, dw, rn, tn, dn, steps_out, rows_out):
    rows = jnp.concatenate([low[0:1], high[0:1]], axis=0).astype(jnp.float32)
    rows = jnp.concatenate([rows, jnp.zeros((EXTRA - 2, rows.shape[1]), jnp.float32)], axis=0)
    rows = rows.astype(jnp.bfloat16)
    rows_out[...] = rows
    channels = dw.shape[1]
    halves = ((rows[:, :channels], dw, rw.shape[1]), (rows[:, channels:], dn, rn.shape[1]))
    out = []
    for row, (d, side) in enumerate(((1, low), (0, high))):
        rate, turn = in_lanes(rw, rn, d), in_lanes(tw, tn, d)
        span = jnp.sum(side[2:3].astype(jnp.float32), axis=1, keepdims=True)
        push = []
        for part in range(2):
            pieces = []
            for x, drive, groups in halves:
                first, second = spread(drive, d, part, groups)
                pieces.append(
                    jnp.dot(x, first, preferred_element_type=jnp.float32)
                    + jnp.dot(x, second, preferred_element_type=jnp.float32)
                )
            push.append(jnp.concatenate(pieces, axis=1)[row : row + 1])
        square = rate * rate + turn * turn
        decay = powers(rate, turn, jnp.broadcast_to(span, rate.shape))
        coef = complex_times(decay[0] - 1.0, decay[1], -rate / square, -turn / square)
        out += [*decay, *complex_times(*coef, *push)]
    steps_out[...] = jnp.concatenate(out, axis=0)


def carried(mine, arrived, rates, turns, count):
    peers = arrived.shape[0]
    quads = 2 * count

    def tile(row):
        pieces = [row[:, k * LANES : (k + 1) * LANES] for k in range(count)] * 2
        pieces.append(jnp.zeros((SUB - quads, LANES), jnp.float32))
        return jnp.concatenate(pieces, axis=0)

    rates, turns = [tile(r) for r in rates], [tile(t) for t in turns]
    ends = [arrived[j].astype(jnp.float32) for j in range(peers)]
    spans = [jnp.sum(e[quads : quads + 1], axis=1, keepdims=True) for e in ends]
    spans = [jnp.broadcast_to(x, (1, LANES)) for x in spans]
    zero = jnp.zeros((1, LANES), jnp.float32)
    before, after = [zero] * peers, [zero] * peers
    for j in range(peers - 2, -1, -1):
        before[j] = jnp.where(j + 1 < mine, before[j + 1] + spans[j + 1], zero)
    for j in range(1, peers):
        after[j] = jnp.where(j - 1 > mine, after[j - 1] + spans[j - 1], zero)
    sums = [jnp.zeros((SUB, LANES), jnp.float32)] * 2
    for j in range(peers):
        early, late = j < mine, j > mine
        gap = jnp.where(early, before[j], after[j])
        weight = powers(
            jnp.where(early, rates[0], rates[1]), jnp.where(early, turns[0], turns[1]), gap
        )
        end = ends[j]
        crossed = jnp.concatenate([-end[count:quads], end[:count], end[quads:]], axis=0)
        term = weight[0] * end + weight[1] * crossed
        sums[0] = sums[0] + jnp.where(early, term, 0.0)
        sums[1] = sums[1] + jnp.where(late, term, 0.0)
    out = []
    for s in sums:
        row = [s[k : k + 1] for k in range(quads)]
        out.append((jnp.concatenate(row[:count], axis=1), jnp.concatenate(row[count:], axis=1)))
    return out


def reading_kernel(
    mine, arrived, rw, tw, dw, rn, tn, dn, skip, inputs, beside, more, sr, si, pr, pi, out
):
    extent = inputs.shape[0]
    steps = extent // SUB
    count = sr.shape[2] // LANES
    rates = [in_lanes(rw, rn, d) for d in range(2)]
    turns = [in_lanes(tw, tn, d) for d in range(2)]
    carries = carried(mine[0], arrived, rates, turns, count)
    channels = dw.shape[1]
    size = extent + EXTRA
    reading = [jnp.zeros((size, channels), jnp.float32) for _ in range(2)]
    for d in range(2):
        last = slice((steps - 1) * SUB, extent) if d == 0 else slice(0, SUB)
        state, power = (sr[d, last, :], si[d, last, :]), (pr[d, last, :], pi[d, last, :])
        carry, starts = carries[d], [None] * SUB
        for c in range(SUB) if d == 0 else range(SUB - 1, -1, -1):
            starts[c] = carry
            at = slice(c, c + 1)
            kept = complex_times(power[0][at], power[1][at], *carry)
            carry = (kept[0] + state[0][at], kept[1] + state[1][at])
        start = [jnp.concatenate([s[k] for s in starts], axis=0) for k in range(2)]
        start = [jnp.concatenate([s] * steps, axis=0) for s in start]
        extra = complex_times(pr[d], pi[d], *start)
        step = [more[k : k + 1, :] for k in range(4 * (1 - d), 4 * (1 - d) + 4)]
        beyond = complex_times(*step[:2], *carry)
        beyond = [beyond[k] + step[2 + k] for k in range(2)]
        pairs = zip(carries[d], beyond) if d == 0 else zip(beyond, carries[d])
        spare = jnp.zeros((EXTRA - 2, carry[0].shape[1]), jnp.float32)
        tail = [jnp.concatenate([*pair, spare], axis=0) for pair in pairs]
        at = 0
        for which, (read, groups) in enumerate(((dw, rw.shape[1]), (dn, rn.shape[1]))):
            upto = at + groups * read.shape[2] // 2
            for part, local in enumerate((sr, si)):
                value = local[d, :, at:upto] + extra[part][:, at:upto]
                value = jnp.concatenate([value, tail[part][:, at:upto]], axis=0)
                high, low = two_terms(value)
                read_high, read_low = spread(read, d, part, groups)
                for x, y in ((high, read_high), (low, read_high), (high, read_low)):
                    reading[which] = reading[which] + lax.dot_general(
                        x, y, (((1,), (1,)), ((), ())), preferred_element_type=jnp.float32
                    )
            at = upto
    rows = jnp.concatenate([inputs[...], beside[...]], axis=0).astype(jnp.float32)
    total = jnp.concatenate(reading, axis=1) + skip[...] * rows
    mixed = jax.nn.gelu(total).astype(jnp.bfloat16)
    back = shuffled(size, extent, 1).astype(jnp.float32).astype(jnp.bfloat16)
    rows = jnp.dot(back, mixed, preferred_element_type=jnp.float32).astype(jnp.bfloat16)
    for k in range(out.shape[0]):
        out[k] = rows


def norm_kernel(extent, slots, out):
    quads, pair, peers = slots.shape[:3]
    gains = [
        jnp.sum(slots[0, 0, k, extent + 2 : extent + 5, :].astype(jnp.float32), axis=0, keepdims=True)
        for k in range(peers)
    ]

    def scaled(pieces, q, rows):
        square = sum(jnp.sum(x * x, axis=1, keepdims=True) for x in pieces)
        scale = lax.rsqrt(square / (peers * LANES) + epsilon)
        for k in range(peers):
            value = pieces[k] * scale * gains[k]
            out[q, rows, k * LANES : (k + 1) * LANES] = value.astype(out.dtype)

    for q in range(quads):
        for m in range(pair):
            pieces = [slots[q, m, k, 0:extent, :].astype(jnp.float32) for k in range(peers)]
            scaled(pieces, q, slice(m * extent, (m + 1) * extent))
        pieces = []
        spare = jnp.zeros((EXTRA - 2, LANES), jnp.float32)
        for k in range(peers):
            low = slots[q, 0, k, extent : extent + 2, :].astype(jnp.float32)[0:1]
            high = slots[q, pair - 1, k, extent : extent + 2, :].astype(jnp.float32)[1:2]
            pieces.append(jnp.concatenate([low, high, spare], axis=0))
        scaled(pieces, q, slice(pair * extent, pair * extent + EXTRA))


def ffn_kernel(part, normed, weights, taps, out):
    quads, size, _ = normed.shape
    size = size - EXTRA
    width = taps.shape[1]
    peers = weights.shape[0] // LANES
    extent = out.shape[1]
    at = 2 * part // LANES * LANES
    row = lax.broadcasted_iota(jnp.int32, (size, width), 0)
    lane = lax.broadcasted_iota(jnp.int32, (size, width), 1)
    room = weights.shape[1] - at
    for q in range(quads):
        pre = jnp.dot(normed[q], weights[:, :width], preferred_element_type=jnp.float32)
        pre = pre.astype(jnp.bfloat16).astype(jnp.float32)
        main, low, high = pre[:size], pre[size : size + 1], pre[size + 1 : size + 2]
        before = jnp.where(row == 0, low, pltpu.roll(main, 1, 0))
        after = jnp.where(row == size - 1, high, pltpu.roll(main, size - 1, 0))
        conv = taps[0:1, :] * before + taps[1:2, :] * main + taps[2:3, :] * after
        gate = pltpu.roll(conv, width - part, 1)
        hidden = jnp.where(lane < part, jax.nn.silu(gate) * conv, 0.0)
        if room != width:
            spare = jnp.zeros((size, abs(room - width)), jnp.float32)
            hidden = jnp.concatenate([hidden, spare], axis=1) if room > width else hidden[:, :room]
        hidden = pltpu.roll(hidden, 2 * part - at, 1).astype(jnp.bfloat16)
        for k in range(peers):
            terms = lax.dot_general(
                hidden,
                weights[k * LANES : (k + 1) * LANES, at:],
                (((1,), (1,)), ((), ())),
                preferred_element_type=jnp.float32,
            ).astype(out.dtype)
            for m in range(size // extent):
                out[(q * (size // extent) + m) * peers + k] = terms[m * extent : (m + 1) * extent]


def in_memory(count):
    vmem = pl.BlockSpec(memory_space=pltpu.VMEM)
    return [pl.BlockSpec(memory_space=pltpu.SMEM)] + [vmem] * count


def mixer(input_wide, input_narrow, spacing, stream, wide, narrow, skip_gain):
    extent, channels = input_wide.shape
    rw, tw, dw, cw = wide
    rn, tn, dn, cn = narrow
    dw, cw, dn, cn = (m.reshape(2, channels, m.shape[3]) for m in (dw, cw, dn, cn))
    states = rw.shape[1] * rw.shape[2] + rn.shape[1] * rn.shape[2]
    mine = lax.axis_index(SP).astype(jnp.int32).reshape(1)
    f32 = functools.partial(jax.ShapeDtypeStruct, dtype=jnp.float32)
    table = f32((2, extent, states))
    cost = pl.CostEstimate(flops=20_000_000, bytes_accessed=2_000_000, transcendentals=100_000)
    edge = jax.ShapeDtypeStruct((SUB, LANES), jnp.bfloat16)
    out, inputs, last, first, *tables = pl.pallas_call(
        local_kernel,
        name="local_states",
        out_shape=(
            jax.ShapeDtypeStruct((lax.axis_size(SP), SUB, LANES), jnp.bfloat16),
            jax.ShapeDtypeStruct((extent, 2 * channels), jnp.bfloat16),
            edge,
            edge,
            table,
            table,
            table,
            table,
        ),
        in_specs=in_memory(10),
        out_specs=tuple(in_memory(8)[1:]),
        cost_estimate=cost,
    )(mine, input_wide.T, input_narrow.T, spacing.reshape(1, -1), stream, rw, tw, dw, rn, tn, dn)
    with jax.named_scope("exchange"):
        arrived = lax.all_to_all(out, SP, split_axis=0, concat_axis=0, tiled=True)
    count = lax.axis_size(SP)
    with jax.named_scope("low"):
        low = lax.ppermute(last, SP, [(i, i + 1) for i in range(count - 1)])
    with jax.named_scope("high"):
        high = lax.ppermute(first, SP, [(i + 1, i) for i in range(count - 1)])
    more, beside = pl.pallas_call(
        beside_kernel,
        name="beside",
        out_shape=(f32((8, states)), jax.ShapeDtypeStruct((EXTRA, 2 * channels), jnp.bfloat16)),
        in_specs=in_memory(8)[1:],
        out_specs=tuple(in_memory(2)[1:]),
        cost_estimate=cost,
    )(low, high, rw, tw, dw, rn, tn, dn)
    slots = pl.pallas_call(
        reading_kernel,
        name="readings",
        out_shape=jax.ShapeDtypeStruct(
            (lax.axis_size("tp"), extent + EXTRA, 2 * channels), jnp.bfloat16
        ),
        in_specs=in_memory(15),
        out_specs=in_memory(1)[1],
        cost_estimate=cost,
    )(mine, arrived, rw, tw, cw, rn, tn, cn, skip_gain.reshape(1, -1), inputs, beside, more, *tables)
    return slots, low[1:2], high[1:2]


def on_device(
    input_wide,
    input_narrow,
    spacing,
    rate_wide,
    turn_wide,
    drive_wide,
    read_wide,
    narrow_decay_rate,
    turn_narrow,
    drive_narrow,
    read_narrow,
    skip_gain,
    out_value,
    out_gate,
    stream,
    norm_gain,
    up_value,
    up_gate,
    conv_taps,
    down_weight,
):
    pair, quads = lax.axis_size("zi"), lax.axis_size("gi")
    share = pair * quads
    extent = input_wide.shape[0]
    block, part = weight_block(up_value, up_gate, down_weight)
    block, input_wide, input_narrow, spacing = lax.optimization_barrier(
        (block, input_wide, input_narrow, spacing)
    )
    weights = lax.all_gather(block, "zp", axis=0, tiled=True)
    mixer_in, low, high = mixer(
        input_wide,
        input_narrow,
        spacing,
        stream,
        (rate_wide, turn_wide, drive_wide, read_wide),
        (narrow_decay_rate, turn_narrow, drive_narrow, read_narrow),
        skip_gain,
    )
    channels = input_wide.shape[1]
    slots = lax.all_to_all(mixer_in, "tp", split_axis=0, concat_axis=0, tiled=True)
    peers = slots.shape[0]
    rows = jnp.moveaxis(slots, 0, 1).reshape(extent + EXTRA, -1)

    def by_slot(weight):
        turned = jnp.moveaxis(weight.reshape(2, peers, channels, -1), 0, 1)
        return turned.reshape(weight.shape)

    value = jnp.dot(rows, by_slot(out_value), preferred_element_type=jnp.float32)
    gate = jnp.dot(rows, by_slot(out_gate), preferred_element_type=jnp.float32)
    mine, count = lax.axis_index(SP), lax.axis_size(SP)
    row = jnp.arange(extent + 2)[:, None]
    inside = ((row != extent) | (mine > 0)) & ((row != extent + 1) | (mine < count - 1))
    branch = (value * jax.nn.sigmoid(gate))[: extent + 2]
    middle = jnp.concatenate([stream, low, high], axis=0).astype(jnp.float32) + branch
    middle = jnp.where(inside, middle, 0.0).astype(jnp.bfloat16)
    sent = jnp.concatenate([middle, addends(norm_gain)], axis=0)
    middle = middle[:extent]
    slots = sent_to_all(sent, MEMBERS)
    slots = slots.reshape(quads, pair, -1, *sent.shape)
    size = pair * extent
    normed = pl.pallas_call(
        functools.partial(norm_kernel, extent),
        name="norm",
        out_shape=jax.ShapeDtypeStruct((quads, size + EXTRA, peers * LANES), jnp.bfloat16),
        in_specs=in_memory(1)[1:],
        out_specs=in_memory(1)[1],
        cost_estimate=pl.CostEstimate(
            flops=3_000_000, bytes_accessed=2_000_000, transcendentals=1000
        ),
    )(slots)
    width = lanes_up(2 * part)
    taps = conv_taps.reshape(2, 3, share, -1)
    mine = lax.axis_index("gi") * pair + lax.axis_index("zi")
    taps = lax.dynamic_index_in_dim(taps, mine, 2, keepdims=False)
    taps = padded_last(jnp.moveaxis(taps, 0, 1).reshape(3, -1), width)
    terms = pl.pallas_call(
        functools.partial(ffn_kernel, part),
        name="ffn",
        out_shape=jax.ShapeDtypeStruct((share * peers, extent, LANES), jnp.bfloat16),
        in_specs=in_memory(3)[1:],
        out_specs=in_memory(1)[1],
        cost_estimate=pl.CostEstimate(
            flops=600_000_000, bytes_accessed=4_000_000, transcendentals=100_000
        ),
    )(normed, weights, taps)
    arrived = lax.all_to_all(terms, MEMBERS, split_axis=0, concat_axis=0, tiled=True)
    ffn = jnp.sum(arrived.astype(jnp.float32), axis=0)
    return (middle.astype(jnp.float32) + ffn).astype(jnp.bfloat16)


def solution(mesh):
    grp, sp, tp = mesh.devices.shape
    quads = SHARE if grp % SHARE == 0 else 1
    parted = Mesh(
        mesh.devices.reshape(grp // quads, quads, sp // SHARE, SHARE, tp),
        ("gp", "gi", *SP, "tp"),
    )
    spot = ("gp", "gi", *SP)
    placed = (
        P(spot, "tp"),
        P(spot, "tp"),
        P(spot),
        P(None, "tp", None),
        P(None, "tp", None),
        P(None, "tp", None, None),
        P(None, "tp", None, None),
        P(None, "tp", None),
        P(None, "tp", None),
        P(None, "tp", None, None),
        P(None, "tp", None, None),
        P(None, "tp"),
        P(None, "tp"),
        P(None, "tp"),
        P(spot, "tp"),
        P("tp"),
        P(SP, "tp"),
        P(SP, "tp"),
        P(None, None, "tp"),
        P("tp", SP),
    )
    return jax.shard_map(
        on_device, mesh=parted, in_specs=placed, out_specs=P(spot, "tp"), check_vma=False
    )
```

```python
import functools
import math

import jax
import jax.numpy as jnp
from jax import lax
from jax.experimental import pallas as pl
from jax.experimental.pallas import tpu as pltpu
from jax.sharding import Mesh
from jax.sharding import PartitionSpec as P

SHARE = 2
LANES = 128
SUB = 8
VMEM_BYTES = 24 * 2**20
EXTRA = 16

epsilon = 1e-06
SP = ("zp", "zi")
MEMBERS = ("gi", "zi", "tp")


def complex_times(left_real, left_quad, right_real, right_quad):
    return (
        left_real * right_real - left_quad * right_quad,
        left_real * right_quad + left_quad * right_real,
    )


def lanes_up(count):
    return -(-count // LANES) * LANES


def padded_last(array, width):
    return jnp.pad(array, [(0, 0)] * (array.ndim - 1) + [(0, width - array.shape[-1])])


def sent_to_all(array, axes):
    copies = jnp.broadcast_to(array, (lax.axis_size(axes), *array.shape))
    return lax.all_to_all(copies, axes, split_axis=0, concat_axis=0, tiled=True)


def pack_kernel(quads, which, value, gate, down, out):
    pair, rows, width = out.shape
    part = value.shape[1] // (pair * quads)
    for k in range(pair):
        pieces = []
        for w in (value, gate, down):
            own = None
            for q in range(quads):
                at = (q * pair + k) * part
                piece = w[:, at : at + part].astype(jnp.float32)
                own = piece if own is None else jnp.where(which[0] == q, piece, own)
            pieces.append(own)
        if width > 3 * part:
            pieces.append(jnp.zeros((rows, width - 3 * part), jnp.float32))
        out[k] = jnp.concatenate(pieces, axis=1).astype(out.dtype)


def weight_block(up_value, up_gate, down_weight):
    pair, quads = lax.axis_size("zi"), lax.axis_size("gi")
    rows, columns = up_value.shape
    part = columns // (pair * quads)
    which = lax.axis_index("gi").astype(jnp.int32).reshape(1)
    block = pl.pallas_call(
        functools.partial(pack_kernel, quads),
        name="pack",
        out_shape=jax.ShapeDtypeStruct((pair, rows, lanes_up(3 * part)), jnp.bfloat16),
        in_specs=in_memory(3),
        out_specs=in_memory(1)[1],
    )(which, up_value, up_gate, down_weight.T)
    block = lax.all_to_all(block, "zi", 0, 0, tiled=True)
    return block.reshape(pair * rows, -1), part


def cos_sin(turn, span):
    turns = (turn * (0.5 / math.pi)) * span
    half = (turns - jnp.floor(turns + 0.5)) * math.pi
    square = half * half
    sine, cosine = 1.0 / math.factorial(13), 1.0 / math.factorial(12)
    for k in range(11, 0, -2):
        sine = sine * square + (-1.0) ** (k // 2) / math.factorial(k)
    for k in range(10, -1, -2):
        cosine = cosine * square + (-1.0) ** (k // 2) / math.factorial(k)
    sine = sine * half
    return 1.0 - 2.0 * sine * sine, 2.0 * sine * cosine


def powers(rate, turn, span):
    shrink = jnp.exp(-rate * span)
    cosine, sine = cos_sin(turn, span)
    return shrink * cosine, shrink * sine


def in_lanes(wide, narrow, d):
    rows = [ref[d, k : k + 1, :] for ref in (wide, narrow) for k in range(ref.shape[1])]
    return jnp.concatenate(rows, axis=1)


def two_terms(x):
    high = x.astype(jnp.bfloat16)
    return high, (x - high.astype(jnp.float32)).astype(jnp.bfloat16)


def spread(ref, d, part, groups):
    states = ref.shape[2] // 2
    own = ref[d][:, part * states : (part + 1) * states]
    wide = jnp.concatenate([own] * groups, axis=1)
    row = lax.broadcasted_iota(jnp.int32, wide.shape, 0) // (wide.shape[0] // groups)
    lane = lax.broadcasted_iota(jnp.int32, wide.shape, 1) // states
    return two_terms(jnp.where(row == lane, wide, 0.0))


def shuffled(size, extent, row_axis):
    row = lax.broadcasted_iota(jnp.int32, (size, size), row_axis)
    position = lax.broadcasted_iota(jnp.int32, (size, size), 1 - row_axis)
    moved = (row % SUB) * (extent // SUB) + row // SUB
    return position == jnp.where(row < extent, moved, row)


def length_row(value):
    lane = lax.broadcasted_iota(jnp.int32, value.shape, 1)
    out = jnp.zeros(value.shape, jnp.float32)
    for k in range(3):
        addend = value.astype(jnp.bfloat16).astype(jnp.float32)
        out = jnp.where(lane == k, addend, out)
        value = value - addend
    return out


def local_kernel(
    mine, wide_in, narrow_in, spacing, stream, rw, tw, dw, rn, tn, dn,
    out, inputs, last, first, sr, si, pr, pi
):
    extent = spacing.shape[1]
    steps = extent // SUB
    place = shuffled(extent, extent, 0)
    span = jnp.sum(jnp.where(place, spacing[...], 0.0), axis=1, keepdims=True)
    both = jnp.concatenate([wide_in[...], narrow_in[...]], axis=0)
    rows = lax.dot_general(
        place.astype(jnp.float32).astype(jnp.bfloat16),
        both,
        (((1,), (1,)), ((), ())),
        preferred_element_type=jnp.float32,
    ).astype(jnp.bfloat16)
    inputs[...] = rows
    for edge, at in ((first, 0), (last, extent - 1)):
        near = at // (2 * SUB) * (2 * SUB)
        pieces = [
            x[near : near + 2 * SUB].astype(jnp.float32)[at - near : at - near + 1]
            for x in (rows, stream[...])
        ]
        pieces.append(length_row(jnp.broadcast_to(span[at : at + 1], (1, LANES))))
        pieces.append(jnp.zeros((SUB - 3, LANES), jnp.float32))
        edge[...] = jnp.concatenate(pieces, axis=0).astype(edge.dtype)
    channels = wide_in.shape[0]
    halves = ((rows[:, :channels], dw, rw.shape[1]), (rows[:, channels:], dn, rn.shape[1]))
    tiles = []
    for d in range(2):
        rate, turn = in_lanes(rw, rn, d), in_lanes(tw, tn, d)
        push = []
        for part in range(2):
            pieces = []
            for x, drive, groups in halves:
                high, low = spread(drive, d, part, groups)
                pieces.append(
                    jnp.dot(x, high, preferred_element_type=jnp.float32)
                    + jnp.dot(x, low, preferred_element_type=jnp.float32)
                )
            push.append(jnp.concatenate(pieces, axis=1))
        square = rate * rate + turn * turn
        back_real, back_quad = -rate / square, -turn / square
        decay_real, decay_quad = powers(rate, turn, span)
        coef_real, coef_quad = complex_times(decay_real - 1.0, decay_quad, back_real, back_quad)
        kick_real, kick_quad = complex_times(coef_real, coef_quad, push[0], push[1])
        order = range(steps) if d == 0 else range(steps - 1, -1, -1)
        state = None
        for i in order:
            at = slice(i * SUB, (i + 1) * SUB)
            decay = (decay_real[at], decay_quad[at])
            if state is None:
                state, power = (kick_real[at], kick_quad[at]), decay
            else:
                kept = complex_times(*decay, *state)
                state = (kept[0] + kick_real[at], kept[1] + kick_quad[at])
                power = complex_times(*decay, *power)
            sr[d, at, :] = state[0]
            si[d, at, :] = state[1]
            pr[d, at, :] = power[0]
            pi[d, at, :] = power[1]
        end = None
        for c in range(SUB) if d == 0 else range(SUB - 1, -1, -1):
            own = (state[0][c : c + 1], state[1][c : c + 1])
            if end is None:
                end = own
            else:
                kept = complex_times(power[0][c : c + 1], power[1][c : c + 1], *end)
                end = (kept[0] + own[0], kept[1] + own[1])
        count = end[0].shape[1] // LANES
        pieces = [e[:, k * LANES : (k + 1) * LANES] for e in end for k in range(count)]
        total = jnp.sum(spacing[...], axis=1, keepdims=True)
        pieces.append(length_row(jnp.broadcast_to(total, (1, LANES))))
        pieces.append(jnp.zeros((SUB - len(pieces), LANES), jnp.float32))
        tiles.append(jnp.concatenate(pieces, axis=0))
    for j in range(out.shape[0]):
        out[j] = jnp.where(j > mine[0], tiles[0], tiles[1]).astype(out.dtype)


def addends(x):
    first = lax.reduce_precision(x, 8, 7)
    second = lax.reduce_precision(x - first, 8, 7)
    return jnp.stack([first, second, x - first - second]).astype(jnp.bfloat16)


def beside_kernel(low, high, rw, tw, dw, rn, tn, dn, steps_out, rows_out):
    rows = jnp.concatenate([low[0:1], high[0:1]], axis=0).astype(jnp.float32)
    rows = jnp.concatenate([rows, jnp.zeros((EXTRA - 2, rows.shape[1]), jnp.float32)], axis=0)
    rows = rows.astype(jnp.bfloat16)
    rows_out[...] = rows
    channels = dw.shape[1]
    halves = ((rows[:, :channels], dw, rw.shape[1]), (rows[:, channels:], dn, rn.shape[1]))
    out = []
    for row, (d, side) in enumerate(((1, low), (0, high))):
        rate, turn = in_lanes(rw, rn, d), in_lanes(tw, tn, d)
        span = jnp.sum(side[2:3].astype(jnp.float32), axis=1, keepdims=True)
        push = []
        for part in range(2):
            pieces = []
            for x, drive, groups in halves:
                first, second = spread(drive, d, part, groups)
                pieces.append(
                    jnp.dot(x, first, preferred_element_type=jnp.float32)
                    + jnp.dot(x, second, preferred_element_type=jnp.float32)
                )
            push.append(jnp.concatenate(pieces, axis=1)[row : row + 1])
        square = rate * rate + turn * turn
        decay = powers(rate, turn, jnp.broadcast_to(span, rate.shape))
        coef = complex_times(decay[0] - 1.0, decay[1], -rate / square, -turn / square)
        out += [*decay, *complex_times(*coef, *push)]
    steps_out[...] = jnp.concatenate(out, axis=0)


def carried(mine, arrived, rates, turns, count):
    peers = arrived.shape[0]
    quads = 2 * count

    def tile(row):
        pieces = [row[:, k * LANES : (k + 1) * LANES] for k in range(count)] * 2
        pieces.append(jnp.zeros((SUB - quads, LANES), jnp.float32))
        return jnp.concatenate(pieces, axis=0)

    rates, turns = [tile(r) for r in rates], [tile(t) for t in turns]
    ends = [arrived[j].astype(jnp.float32) for j in range(peers)]
    spans = [jnp.sum(e[quads : quads + 1], axis=1, keepdims=True) for e in ends]
    spans = [jnp.broadcast_to(x, (1, LANES)) for x in spans]
    zero = jnp.zeros((1, LANES), jnp.float32)
    before, after = [zero] * peers, [zero] * peers
    for j in range(peers - 2, -1, -1):
        before[j] = jnp.where(j + 1 < mine, before[j + 1] + spans[j + 1], zero)
    for j in range(1, peers):
        after[j] = jnp.where(j - 1 > mine, after[j - 1] + spans[j - 1], zero)
    sums = [jnp.zeros((SUB, LANES), jnp.float32)] * 2
    for j in range(peers):
        early, late = j < mine, j > mine
        gap = jnp.where(early, before[j], after[j])
        weight = powers(
            jnp.where(early, rates[0], rates[1]), jnp.where(early, turns[0], turns[1]), gap
        )
        end = ends[j]
        crossed = jnp.concatenate([-end[count:quads], end[:count], end[quads:]], axis=0)
        term = weight[0] * end + weight[1] * crossed
        sums[0] = sums[0] + jnp.where(early, term, 0.0)
        sums[1] = sums[1] + jnp.where(late, term, 0.0)
    out = []
    for s in sums:
        row = [s[k : k + 1] for k in range(quads)]
        out.append((jnp.concatenate(row[:count], axis=1), jnp.concatenate(row[count:], axis=1)))
    return out


def reading_kernel(
    mine, arrived, rw, tw, dw, rn, tn, dn, skip, inputs, beside, more, sr, si, pr, pi, out
):
    extent = inputs.shape[0]
    steps = extent // SUB
    count = sr.shape[2] // LANES
    rates = [in_lanes(rw, rn, d) for d in range(2)]
    turns = [in_lanes(tw, tn, d) for d in range(2)]
    carries = carried(mine[0], arrived, rates, turns, count)
    channels = dw.shape[1]
    size = extent + EXTRA
    reading = [jnp.zeros((size, channels), jnp.float32) for _ in range(2)]
    for d in range(2):
        last = slice((steps - 1) * SUB, extent) if d == 0 else slice(0, SUB)
        state, power = (sr[d, last, :], si[d, last, :]), (pr[d, last, :], pi[d, last, :])
        carry, starts = carries[d], [None] * SUB
        for c in range(SUB) if d == 0 else range(SUB - 1, -1, -1):
            starts[c] = carry
            at = slice(c, c + 1)
            kept = complex_times(power[0][at], power[1][at], *carry)
            carry = (kept[0] + state[0][at], kept[1] + state[1][at])
        start = [jnp.concatenate([s[k] for s in starts], axis=0) for k in range(2)]
        start = [jnp.concatenate([s] * steps, axis=0) for s in start]
        extra = complex_times(pr[d], pi[d], *start)
        step = [more[k : k + 1, :] for k in range(4 * (1 - d), 4 * (1 - d) + 4)]
        beyond = complex_times(*step[:2], *carry)
        beyond = [beyond[k] + step[2 + k] for k in range(2)]
        pairs = zip(carries[d], beyond) if d == 0 else zip(beyond, carries[d])
        spare = jnp.zeros((EXTRA - 2, carry[0].shape[1]), jnp.float32)
        tail = [jnp.concatenate([*pair, spare], axis=0) for pair in pairs]
        at = 0
        for which, (read, groups) in enumerate(((dw, rw.shape[1]), (dn, rn.shape[1]))):
            upto = at + groups * read.shape[2] // 2
            for part, local in enumerate((sr, si)):
                value = local[d, :, at:upto] + extra[part][:, at:upto]
                value = jnp.concatenate([value, tail[part][:, at:upto]], axis=0)
                high, low = two_terms(value)
                read_high, read_low = spread(read, d, part, groups)
                for x, y in ((high, read_high), (low, read_high), (high, read_low)):
                    reading[which] = reading[which] + lax.dot_general(
                        x, y, (((1,), (1,)), ((), ())), preferred_element_type=jnp.float32
                    )
            at = upto
    rows = jnp.concatenate([inputs[...], beside[...]], axis=0).astype(jnp.float32)
    total = jnp.concatenate(reading, axis=1) + skip[...] * rows
    mixed = jax.nn.gelu(total).astype(jnp.bfloat16)
    back = shuffled(size, extent, 1).astype(jnp.float32).astype(jnp.bfloat16)
    rows = jnp.dot(back, mixed, preferred_element_type=jnp.float32).astype(jnp.bfloat16)
    for k in range(out.shape[0]):
        out[k] = rows


def norm_kernel(extent, slots, out):
    quads, pair, peers = slots.shape[:3]
    gains = [
        jnp.sum(slots[0, 0, k, extent + 2 : extent + 5, :].astype(jnp.float32), axis=0, keepdims=True)
        for k in range(peers)
    ]

    def scaled(pieces, q, rows):
        square = sum(jnp.sum(x * x, axis=1, keepdims=True) for x in pieces)
        scale = lax.rsqrt(square / (peers * LANES) + epsilon)
        for k in range(peers):
            value = pieces[k] * scale * gains[k]
            out[q, rows, k * LANES : (k + 1) * LANES] = value.astype(out.dtype)

    for q in range(quads):
        for m in range(pair):
            pieces = [slots[q, m, k, 0:extent, :].astype(jnp.float32) for k in range(peers)]
            scaled(pieces, q, slice(m * extent, (m + 1) * extent))
        pieces = []
        spare = jnp.zeros((EXTRA - 2, LANES), jnp.float32)
        for k in range(peers):
            low = slots[q, 0, k, extent : extent + 2, :].astype(jnp.float32)[0:1]
            high = slots[q, pair - 1, k, extent : extent + 2, :].astype(jnp.float32)[1:2]
            pieces.append(jnp.concatenate([low, high, spare], axis=0))
        scaled(pieces, q, slice(pair * extent, pair * extent + EXTRA))


def ffn_kernel(part, normed, weights, taps, out):
    quads, size, _ = normed.shape
    size = size - EXTRA
    width = taps.shape[1]
    peers = weights.shape[0] // LANES
    extent = out.shape[1]
    at = 2 * part // LANES * LANES
    row = lax.broadcasted_iota(jnp.int32, (size, width), 0)
    lane = lax.broadcasted_iota(jnp.int32, (size, width), 1)
    room = weights.shape[1] - at
    for q in range(quads):
        pre = jnp.dot(normed[q], weights[:, :width], preferred_element_type=jnp.float32)
        pre = pre.astype(jnp.bfloat16).astype(jnp.float32)
        main, low, high = pre[:size], pre[size : size + 1], pre[size + 1 : size + 2]
        before = jnp.where(row == 0, low, pltpu.roll(main, 1, 0))
        after = jnp.where(row == size - 1, high, pltpu.roll(main, size - 1, 0))
        conv = taps[0:1, :] * before + taps[1:2, :] * main + taps[2:3, :] * after
        gate = pltpu.roll(conv, width - part, 1)
        hidden = jnp.where(lane < part, jax.nn.silu(gate) * conv, 0.0)
        if room != width:
            spare = jnp.zeros((size, abs(room - width)), jnp.float32)
            hidden = jnp.concatenate([hidden, spare], axis=1) if room > width else hidden[:, :room]
        hidden = pltpu.roll(hidden, 2 * part - at, 1).astype(jnp.bfloat16)
        for k in range(peers):
            terms = lax.dot_general(
                hidden,
                weights[k * LANES : (k + 1) * LANES, at:],
                (((1,), (1,)), ((), ())),
                preferred_element_type=jnp.float32,
            ).astype(out.dtype)
            for m in range(size // extent):
                out[(q * (size // extent) + m) * peers + k] = terms[m * extent : (m + 1) * extent]


def in_memory(count):
    vmem = pl.BlockSpec(memory_space=pltpu.VMEM)
    return [pl.BlockSpec(memory_space=pltpu.SMEM)] + [vmem] * count


def mixer(input_wide, input_narrow, spacing, stream, wide, narrow, skip_gain):
    extent, channels = input_wide.shape
    rw, tw, dw, cw = wide
    rn, tn, dn, cn = narrow
    dw, cw, dn, cn = (m.reshape(2, channels, m.shape[3]) for m in (dw, cw, dn, cn))
    states = rw.shape[1] * rw.shape[2] + rn.shape[1] * rn.shape[2]
    mine = lax.axis_index(SP).astype(jnp.int32).reshape(1)
    f32 = functools.partial(jax.ShapeDtypeStruct, dtype=jnp.float32)
    table = f32((2, extent, states))
    cost = pl.CostEstimate(flops=20_000_000, bytes_accessed=2_000_000, transcendentals=100_000)
    edge = jax.ShapeDtypeStruct((SUB, LANES), jnp.bfloat16)
    out, inputs, last, first, *tables = pl.pallas_call(
        local_kernel,
        name="local_states",
        out_shape=(
            jax.ShapeDtypeStruct((lax.axis_size(SP), SUB, LANES), jnp.bfloat16),
            jax.ShapeDtypeStruct((extent, 2 * channels), jnp.bfloat16),
            edge,
            edge,
            table,
            table,
            table,
            table,
        ),
        in_specs=in_memory(10),
        out_specs=tuple(in_memory(8)[1:]),
        compiler_params=pltpu.CompilerParams(vmem_limit_bytes=VMEM_BYTES),
        cost_estimate=cost,
    )(mine, input_wide.T, input_narrow.T, spacing.reshape(1, -1), stream, rw, tw, dw, rn, tn, dn)
    with jax.named_scope("exchange"):
        arrived = lax.all_to_all(out, SP, split_axis=0, concat_axis=0, tiled=True)
    count = lax.axis_size(SP)
    with jax.named_scope("low"):
        low = lax.ppermute(last, SP, [(i, i + 1) for i in range(count - 1)])
    with jax.named_scope("high"):
        high = lax.ppermute(first, SP, [(i + 1, i) for i in range(count - 1)])
    more, beside = pl.pallas_call(
        beside_kernel,
        name="beside",
        out_shape=(f32((8, states)), jax.ShapeDtypeStruct((EXTRA, 2 * channels), jnp.bfloat16)),
        in_specs=in_memory(8)[1:],
        out_specs=tuple(in_memory(2)[1:]),
        compiler_params=pltpu.CompilerParams(vmem_limit_bytes=VMEM_BYTES),
        cost_estimate=cost,
    )(low, high, rw, tw, dw, rn, tn, dn)
    slots = pl.pallas_call(
        reading_kernel,
        name="readings",
        out_shape=jax.ShapeDtypeStruct(
            (lax.axis_size("tp"), extent + EXTRA, 2 * channels), jnp.bfloat16
        ),
        in_specs=in_memory(15),
        out_specs=in_memory(1)[1],
        compiler_params=pltpu.CompilerParams(vmem_limit_bytes=VMEM_BYTES),
        cost_estimate=cost,
    )(mine, arrived, rw, tw, cw, rn, tn, cn, skip_gain.reshape(1, -1), inputs, beside, more, *tables)
    return slots, low[1:2], high[1:2]


def on_device(
    input_wide,
    input_narrow,
    spacing,
    rate_wide,
    turn_wide,
    drive_wide,
    read_wide,
    narrow_decay_rate,
    turn_narrow,
    drive_narrow,
    read_narrow,
    skip_gain,
    out_value,
    out_gate,
    stream,
    norm_gain,
    up_value,
    up_gate,
    conv_taps,
    down_weight,
):
    pair, quads = lax.axis_size("zi"), lax.axis_size("gi")
    share = pair * quads
    extent = input_wide.shape[0]
    block, part = weight_block(up_value, up_gate, down_weight)
    block, input_wide, input_narrow, spacing = lax.optimization_barrier(
        (block, input_wide, input_narrow, spacing)
    )
    weights = lax.all_gather(block, "zp", axis=0, tiled=True)
    mixer_in, low, high = mixer(
        input_wide,
        input_narrow,
        spacing,
        stream,
        (rate_wide, turn_wide, drive_wide, read_wide),
        (narrow_decay_rate, turn_narrow, drive_narrow, read_narrow),
        skip_gain,
    )
    channels = input_wide.shape[1]
    slots = lax.all_to_all(mixer_in, "tp", split_axis=0, concat_axis=0, tiled=True)
    peers = slots.shape[0]
    rows = jnp.moveaxis(slots, 0, 1).reshape(extent + EXTRA, -1)

    def by_slot(weight):
        turned = jnp.moveaxis(weight.reshape(2, peers, channels, -1), 0, 1)
        return turned.reshape(weight.shape)

    value = jnp.dot(rows, by_slot(out_value), preferred_element_type=jnp.float32)
    gate = jnp.dot(rows, by_slot(out_gate), preferred_element_type=jnp.float32)
    mine, count = lax.axis_index(SP), lax.axis_size(SP)
    row = jnp.arange(extent + 2)[:, None]
    inside = ((row != extent) | (mine > 0)) & ((row != extent + 1) | (mine < count - 1))
    branch = (value * jax.nn.sigmoid(gate))[: extent + 2]
    middle = jnp.concatenate([stream, low, high], axis=0).astype(jnp.float32) + branch
    middle = jnp.where(inside, middle, 0.0).astype(jnp.bfloat16)
    sent = jnp.concatenate([middle, addends(norm_gain)], axis=0)
    middle = middle[:extent]
    slots = sent_to_all(sent, MEMBERS)
    slots = slots.reshape(quads, pair, -1, *sent.shape)
    size = pair * extent
    normed = pl.pallas_call(
        functools.partial(norm_kernel, extent),
        name="norm",
        out_shape=jax.ShapeDtypeStruct((quads, size + EXTRA, peers * LANES), jnp.bfloat16),
        in_specs=in_memory(1)[1:],
        out_specs=in_memory(1)[1],
        compiler_params=pltpu.CompilerParams(vmem_limit_bytes=VMEM_BYTES),
        cost_estimate=pl.CostEstimate(
            flops=3_000_000, bytes_accessed=2_000_000, transcendentals=1000
        ),
    )(slots)
    width = lanes_up(2 * part)
    taps = conv_taps.reshape(2, 3, share, -1)
    mine = lax.axis_index("gi") * pair + lax.axis_index("zi")
    taps = lax.dynamic_index_in_dim(taps, mine, 2, keepdims=False)
    taps = padded_last(jnp.moveaxis(taps, 0, 1).reshape(3, -1), width)
    terms = pl.pallas_call(
        functools.partial(ffn_kernel, part),
        name="ffn",
        out_shape=jax.ShapeDtypeStruct((share * peers, extent, LANES), jnp.bfloat16),
        in_specs=in_memory(3)[1:],
        out_specs=in_memory(1)[1],
        compiler_params=pltpu.CompilerParams(vmem_limit_bytes=VMEM_BYTES),
        cost_estimate=pl.CostEstimate(
            flops=600_000_000, bytes_accessed=4_000_000, transcendentals=100_000
        ),
    )(normed, weights, taps)
    arrived = lax.all_to_all(terms, MEMBERS, split_axis=0, concat_axis=0, tiled=True)
    ffn = jnp.sum(arrived.astype(jnp.float32), axis=0)
    return (middle.astype(jnp.float32) + ffn).astype(jnp.bfloat16)


def solution(mesh):
    grp, sp, tp = mesh.devices.shape
    quads = SHARE if grp % SHARE == 0 else 1
    parted = Mesh(
        mesh.devices.reshape(grp // quads, quads, sp // SHARE, SHARE, tp),
        ("gp", "gi", *SP, "tp"),
    )
    spot = ("gp", "gi", *SP)
    placed = (
        P(spot, "tp"),
        P(spot, "tp"),
        P(spot),
        P(None, "tp", None),
        P(None, "tp", None),
        P(None, "tp", None, None),
        P(None, "tp", None, None),
        P(None, "tp", None),
        P(None, "tp", None),
        P(None, "tp", None, None),
        P(None, "tp", None, None),
        P(None, "tp"),
        P(None, "tp"),
        P(None, "tp"),
        P(spot, "tp"),
        P("tp"),
        P(SP, "tp"),
        P(SP, "tp"),
        P(None, None, "tp"),
        P("tp", SP),
    )
    return jax.shard_map(
        on_device, mesh=parted, in_specs=placed, out_specs=P(spot, "tp"), check_vma=False
    )
```

```python
import functools
import math

import jax
import jax.numpy as jnp
from jax import lax
from jax.experimental import pallas as pl
from jax.experimental.pallas import tpu as pltpu
from jax.sharding import Mesh
from jax.sharding import PartitionSpec as P

SHARE = 2
LANES = 128
SUB = 8
VMEM_BYTES = 24 * 2**20
EXTRA = 16

epsilon = 1e-06
SP = ("zp", "zi")
MEMBERS = ("gi", "zi", "tp")


def complex_times(left_real, left_quad, right_real, right_quad):
    return (
        left_real * right_real - left_quad * right_quad,
        left_real * right_quad + left_quad * right_real,
    )


def lanes_up(count):
    return -(-count // LANES) * LANES


def padded_last(array, width):
    return jnp.pad(array, [(0, 0)] * (array.ndim - 1) + [(0, width - array.shape[-1])])


def sent_to_all(array, axes):
    copies = jnp.broadcast_to(array, (lax.axis_size(axes), *array.shape))
    return lax.all_to_all(copies, axes, split_axis=0, concat_axis=0, tiled=True)


def pack_kernel(quads, which, value, gate, down, out):
    pair, rows, width = out.shape
    part = value.shape[1] // (pair * quads)
    for k in range(pair):
        pieces = []
        for w in (value, gate, down):
            own = None
            for q in range(quads):
                at = (q * pair + k) * part
                piece = w[:, at : at + part].astype(jnp.float32)
                own = piece if own is None else jnp.where(which[0] == q, piece, own)
            pieces.append(own)
        if width > 3 * part:
            pieces.append(jnp.zeros((rows, width - 3 * part), jnp.float32))
        out[k] = jnp.concatenate(pieces, axis=1).astype(out.dtype)


def weight_block(up_value, up_gate, down_weight):
    pair, quads = lax.axis_size("zi"), lax.axis_size("gi")
    rows, columns = up_value.shape
    part = columns // (pair * quads)
    which = lax.axis_index("gi").astype(jnp.int32).reshape(1)
    block = pl.pallas_call(
        functools.partial(pack_kernel, quads),
        name="pack",
        out_shape=jax.ShapeDtypeStruct((pair, rows, lanes_up(3 * part)), jnp.bfloat16),
        in_specs=in_memory(3),
        out_specs=in_memory(1)[1],
    )(which, up_value, up_gate, down_weight.T)
    block = lax.all_to_all(block, "zi", 0, 0, tiled=True)
    return block.reshape(pair * rows, -1), part


def cos_sin(turn, span):
    turns = (turn * (0.5 / math.pi)) * span
    half = (turns - jnp.floor(turns + 0.5)) * math.pi
    square = half * half
    sine, cosine = 1.0 / math.factorial(13), 1.0 / math.factorial(12)
    for k in range(11, 0, -2):
        sine = sine * square + (-1.0) ** (k // 2) / math.factorial(k)
    for k in range(10, -1, -2):
        cosine = cosine * square + (-1.0) ** (k // 2) / math.factorial(k)
    sine = sine * half
    return 1.0 - 2.0 * sine * sine, 2.0 * sine * cosine


def powers(rate, turn, span):
    shrink = jnp.exp(-rate * span)
    cosine, sine = cos_sin(turn, span)
    return shrink * cosine, shrink * sine


def in_lanes(wide, narrow, d):
    rows = [ref[d, k : k + 1, :] for ref in (wide, narrow) for k in range(ref.shape[1])]
    return jnp.concatenate(rows, axis=1)


def two_terms(x):
    high = x.astype(jnp.bfloat16)
    return high, (x - high.astype(jnp.float32)).astype(jnp.bfloat16)


def spread(ref, d, part, groups):
    states = ref.shape[2] // 2
    own = ref[d][:, part * states : (part + 1) * states]
    wide = jnp.concatenate([own] * groups, axis=1)
    row = lax.broadcasted_iota(jnp.int32, wide.shape, 0) // (wide.shape[0] // groups)
    lane = lax.broadcasted_iota(jnp.int32, wide.shape, 1) // states
    return two_terms(jnp.where(row == lane, wide, 0.0))


def shuffled(size, extent, row_axis):
    row = lax.broadcasted_iota(jnp.int32, (size, size), row_axis)
    position = lax.broadcasted_iota(jnp.int32, (size, size), 1 - row_axis)
    moved = (row % SUB) * (extent // SUB) + row // SUB
    return position == jnp.where(row < extent, moved, row)


def length_row(value):
    lane = lax.broadcasted_iota(jnp.int32, value.shape, 1)
    out = jnp.zeros(value.shape, jnp.float32)
    for k in range(3):
        addend = value.astype(jnp.bfloat16).astype(jnp.float32)
        out = jnp.where(lane == k, addend, out)
        value = value - addend
    return out


def local_kernel(
    mine, wide_in, narrow_in, spacing, stream, rw, tw, dw, rn, tn, dn,
    out, inputs, last, first, sr, si, pr, pi
):
    extent = spacing.shape[1]
    steps = extent // SUB
    place = shuffled(extent, extent, 0)
    span = jnp.sum(jnp.where(place, spacing[...], 0.0), axis=1, keepdims=True)
    both = jnp.concatenate([wide_in[...], narrow_in[...]], axis=0)
    rows = lax.dot_general(
        place.astype(jnp.float32).astype(jnp.bfloat16),
        both,
        (((1,), (1,)), ((), ())),
        preferred_element_type=jnp.float32,
    ).astype(jnp.bfloat16)
    inputs[...] = rows
    for edge, at in ((first, 0), (last, extent - 1)):
        near = at // (2 * SUB) * (2 * SUB)
        pieces = [
            x[near : near + 2 * SUB].astype(jnp.float32)[at - near : at - near + 1]
            for x in (rows, stream[...])
        ]
        pieces.append(length_row(jnp.broadcast_to(span[at : at + 1], (1, LANES))))
        pieces.append(jnp.zeros((SUB - 3, LANES), jnp.float32))
        edge[...] = jnp.concatenate(pieces, axis=0).astype(edge.dtype)
    channels = wide_in.shape[0]
    halves = ((rows[:, :channels], dw, rw.shape[1]), (rows[:, channels:], dn, rn.shape[1]))
    tiles = []
    for d in range(2):
        rate, turn = in_lanes(rw, rn, d), in_lanes(tw, tn, d)
        push = []
        for part in range(2):
            pieces = []
            for x, drive, groups in halves:
                high, low = spread(drive, d, part, groups)
                pieces.append(
                    jnp.dot(x, high, preferred_element_type=jnp.float32)
                    + jnp.dot(x, low, preferred_element_type=jnp.float32)
                )
            push.append(jnp.concatenate(pieces, axis=1))
        square = rate * rate + turn * turn
        back_real, back_quad = -rate / square, -turn / square
        decay_real, decay_quad = powers(rate, turn, span)
        coef_real, coef_quad = complex_times(decay_real - 1.0, decay_quad, back_real, back_quad)
        kick_real, kick_quad = complex_times(coef_real, coef_quad, push[0], push[1])
        order = range(steps) if d == 0 else range(steps - 1, -1, -1)
        state = None
        for i in order:
            at = slice(i * SUB, (i + 1) * SUB)
            decay = (decay_real[at], decay_quad[at])
            if state is None:
                state, power = (kick_real[at], kick_quad[at]), decay
            else:
                kept = complex_times(*decay, *state)
                state = (kept[0] + kick_real[at], kept[1] + kick_quad[at])
                power = complex_times(*decay, *power)
            sr[d, at, :] = state[0]
            si[d, at, :] = state[1]
            pr[d, at, :] = power[0]
            pi[d, at, :] = power[1]
        end = None
        for c in range(SUB) if d == 0 else range(SUB - 1, -1, -1):
            own = (state[0][c : c + 1], state[1][c : c + 1])
            if end is None:
                end = own
            else:
                kept = complex_times(power[0][c : c + 1], power[1][c : c + 1], *end)
                end = (kept[0] + own[0], kept[1] + own[1])
        count = end[0].shape[1] // LANES
        pieces = [e[:, k * LANES : (k + 1) * LANES] for e in end for k in range(count)]
        total = jnp.sum(spacing[...], axis=1, keepdims=True)
        pieces.append(length_row(jnp.broadcast_to(total, (1, LANES))))
        pieces.append(jnp.zeros((SUB - len(pieces), LANES), jnp.float32))
        tiles.append(jnp.concatenate(pieces, axis=0))
    for j in range(out.shape[0]):
        out[j] = jnp.where(j > mine[0], tiles[0], tiles[1]).astype(out.dtype)


def addends(x):
    first = lax.reduce_precision(x, 8, 7)
    second = lax.reduce_precision(x - first, 8, 7)
    return jnp.stack([first, second, x - first - second]).astype(jnp.bfloat16)


def beside_kernel(low, high, rw, tw, dw, rn, tn, dn, steps_out, rows_out):
    rows = jnp.concatenate([low[0:1], high[0:1]], axis=0).astype(jnp.float32)
    rows = jnp.concatenate([rows, jnp.zeros((EXTRA - 2, rows.shape[1]), jnp.float32)], axis=0)
    rows = rows.astype(jnp.bfloat16)
    rows_out[...] = rows
    channels = dw.shape[1]
    halves = ((rows[:, :channels], dw, rw.shape[1]), (rows[:, channels:], dn, rn.shape[1]))
    out = []
    for row, (d, side) in enumerate(((1, low), (0, high))):
        rate, turn = in_lanes(rw, rn, d), in_lanes(tw, tn, d)
        span = jnp.sum(side[2:3].astype(jnp.float32), axis=1, keepdims=True)
        push = []
        for part in range(2):
            pieces = []
            for x, drive, groups in halves:
                first, second = spread(drive, d, part, groups)
                pieces.append(
                    jnp.dot(x, first, preferred_element_type=jnp.float32)
                    + jnp.dot(x, second, preferred_element_type=jnp.float32)
                )
            push.append(jnp.concatenate(pieces, axis=1)[row : row + 1])
        square = rate * rate + turn * turn
        decay = powers(rate, turn, jnp.broadcast_to(span, rate.shape))
        coef = complex_times(decay[0] - 1.0, decay[1], -rate / square, -turn / square)
        out += [*decay, *complex_times(*coef, *push)]
    steps_out[...] = jnp.concatenate(out, axis=0)


def carried(mine, arrived, rates, turns, count):
    peers = arrived.shape[0]
    quads = 2 * count

    def tile(row):
        pieces = [row[:, k * LANES : (k + 1) * LANES] for k in range(count)] * 2
        pieces.append(jnp.zeros((SUB - quads, LANES), jnp.float32))
        return jnp.concatenate(pieces, axis=0)

    rates, turns = [tile(r) for r in rates], [tile(t) for t in turns]
    ends = [arrived[j].astype(jnp.float32) for j in range(peers)]
    spans = [jnp.sum(e[quads : quads + 1], axis=1, keepdims=True) for e in ends]
    spans = [jnp.broadcast_to(x, (1, LANES)) for x in spans]
    zero = jnp.zeros((1, LANES), jnp.float32)
    before, after = [zero] * peers, [zero] * peers
    for j in range(peers - 2, -1, -1):
        before[j] = jnp.where(j + 1 < mine, before[j + 1] + spans[j + 1], zero)
    for j in range(1, peers):
        after[j] = jnp.where(j - 1 > mine, after[j - 1] + spans[j - 1], zero)
    sums = [jnp.zeros((SUB, LANES), jnp.float32)] * 2
    for j in range(peers):
        early, late = j < mine, j > mine
        gap = jnp.where(early, before[j], after[j])
        weight = powers(
            jnp.where(early, rates[0], rates[1]), jnp.where(early, turns[0], turns[1]), gap
        )
        end = ends[j]
        crossed = jnp.concatenate([-end[count:quads], end[:count], end[quads:]], axis=0)
        term = weight[0] * end + weight[1] * crossed
        sums[0] = sums[0] + jnp.where(early, term, 0.0)
        sums[1] = sums[1] + jnp.where(late, term, 0.0)
    out = []
    for s in sums:
        row = [s[k : k + 1] for k in range(quads)]
        out.append((jnp.concatenate(row[:count], axis=1), jnp.concatenate(row[count:], axis=1)))
    return out


def reading_kernel(
    mine, arrived, rw, tw, dw, rn, tn, dn, skip, inputs, beside, more, sr, si, pr, pi, out
):
    extent = inputs.shape[0]
    steps = extent // SUB
    count = sr.shape[2] // LANES
    rates = [in_lanes(rw, rn, d) for d in range(2)]
    turns = [in_lanes(tw, tn, d) for d in range(2)]
    carries = carried(mine[0], arrived, rates, turns, count)
    channels = dw.shape[1]
    size = extent + EXTRA
    reading = [jnp.zeros((size, channels), jnp.float32) for _ in range(2)]
    for d in range(2):
        last = slice((steps - 1) * SUB, extent) if d == 0 else slice(0, SUB)
        state, power = (sr[d, last, :], si[d, last, :]), (pr[d, last, :], pi[d, last, :])
        carry, starts = carries[d], [None] * SUB
        for c in range(SUB) if d == 0 else range(SUB - 1, -1, -1):
            starts[c] = carry
            at = slice(c, c + 1)
            kept = complex_times(power[0][at], power[1][at], *carry)
            carry = (kept[0] + state[0][at], kept[1] + state[1][at])
        start = [jnp.concatenate([s[k] for s in starts], axis=0) for k in range(2)]
        start = [jnp.concatenate([s] * steps, axis=0) for s in start]
        extra = complex_times(pr[d], pi[d], *start)
        step = [more[k : k + 1, :] for k in range(4 * (1 - d), 4 * (1 - d) + 4)]
        beyond = complex_times(*step[:2], *carry)
        beyond = [beyond[k] + step[2 + k] for k in range(2)]
        pairs = zip(carries[d], beyond) if d == 0 else zip(beyond, carries[d])
        spare = jnp.zeros((EXTRA - 2, carry[0].shape[1]), jnp.float32)
        tail = [jnp.concatenate([*pair, spare], axis=0) for pair in pairs]
        at = 0
        for which, (read, groups) in enumerate(((dw, rw.shape[1]), (dn, rn.shape[1]))):
            upto = at + groups * read.shape[2] // 2
            for part, local in enumerate((sr, si)):
                value = local[d, :, at:upto] + extra[part][:, at:upto]
                value = jnp.concatenate([value, tail[part][:, at:upto]], axis=0)
                high, low = two_terms(value)
                read_high, read_low = spread(read, d, part, groups)
                for x, y in ((high, read_high), (low, read_high), (high, read_low)):
                    reading[which] = reading[which] + lax.dot_general(
                        x, y, (((1,), (1,)), ((), ())), preferred_element_type=jnp.float32
                    )
            at = upto
    rows = jnp.concatenate([inputs[...], beside[...]], axis=0).astype(jnp.float32)
    total = jnp.concatenate(reading, axis=1) + skip[...] * rows
    mixed = jax.nn.gelu(total).astype(jnp.bfloat16)
    back = shuffled(size, extent, 1).astype(jnp.float32).astype(jnp.bfloat16)
    rows = jnp.dot(back, mixed, preferred_element_type=jnp.float32).astype(jnp.bfloat16)
    for k in range(out.shape[0]):
        out[k] = rows


def norm_kernel(extent, slots, out):
    quads, pair, peers = slots.shape[:3]
    gains = [
        jnp.sum(slots[0, 0, k, extent + 2 : extent + 5, :].astype(jnp.float32), axis=0, keepdims=True)
        for k in range(peers)
    ]

    def scaled(pieces, q, rows):
        square = sum(jnp.sum(x * x, axis=1, keepdims=True) for x in pieces)
        scale = lax.rsqrt(square / (peers * LANES) + epsilon)
        for k in range(peers):
            value = pieces[k] * scale * gains[k]
            out[q, rows, k * LANES : (k + 1) * LANES] = value.astype(out.dtype)

    for q in range(quads):
        for m in range(pair):
            pieces = [slots[q, m, k, 0:extent, :].astype(jnp.float32) for k in range(peers)]
            scaled(pieces, q, slice(m * extent, (m + 1) * extent))
        pieces = []
        spare = jnp.zeros((EXTRA - 2, LANES), jnp.float32)
        for k in range(peers):
            low = slots[q, 0, k, extent : extent + 2, :].astype(jnp.float32)[0:1]
            high = slots[q, pair - 1, k, extent : extent + 2, :].astype(jnp.float32)[1:2]
            pieces.append(jnp.concatenate([low, high, spare], axis=0))
        scaled(pieces, q, slice(pair * extent, pair * extent + EXTRA))


def ffn_kernel(part, normed, weights, taps, out):
    quads, size, _ = normed.shape
    size = size - EXTRA
    width = taps.shape[1]
    peers = weights.shape[0] // LANES
    extent = out.shape[1]
    at = 2 * part // LANES * LANES
    row = lax.broadcasted_iota(jnp.int32, (size, width), 0)
    lane = lax.broadcasted_iota(jnp.int32, (size, width), 1)
    room = weights.shape[1] - at
    for q in range(quads):
        pre = jnp.dot(normed[q], weights[:, :width], preferred_element_type=jnp.float32)
        pre = pre.astype(jnp.bfloat16).astype(jnp.float32)
        main, low, high = pre[:size], pre[size : size + 1], pre[size + 1 : size + 2]
        before = jnp.where(row == 0, low, pltpu.roll(main, 1, 0))
        after = jnp.where(row == size - 1, high, pltpu.roll(main, size - 1, 0))
        conv = taps[0:1, :] * before + taps[1:2, :] * main + taps[2:3, :] * after
        gate = pltpu.roll(conv, width - part, 1)
        hidden = jnp.where(lane < part, jax.nn.silu(gate) * conv, 0.0)
        if room != width:
            spare = jnp.zeros((size, abs(room - width)), jnp.float32)
            hidden = jnp.concatenate([hidden, spare], axis=1) if room > width else hidden[:, :room]
        hidden = pltpu.roll(hidden, 2 * part - at, 1).astype(jnp.bfloat16)
        for k in range(peers):
            terms = lax.dot_general(
                hidden,
                weights[k * LANES : (k + 1) * LANES, at:],
                (((1,), (1,)), ((), ())),
                preferred_element_type=jnp.float32,
            ).astype(out.dtype)
            for m in range(size // extent):
                out[(q * (size // extent) + m) * peers + k] = terms[m * extent : (m + 1) * extent]


def in_memory(count):
    vmem = pl.BlockSpec(memory_space=pltpu.VMEM)
    return [pl.BlockSpec(memory_space=pltpu.SMEM)] + [vmem] * count


def mixer(input_wide, input_narrow, spacing, stream, wide, narrow, skip_gain):
    extent, channels = input_wide.shape
    rw, tw, dw, cw = wide
    rn, tn, dn, cn = narrow
    dw, cw, dn, cn = (m.reshape(2, channels, m.shape[3]) for m in (dw, cw, dn, cn))
    states = rw.shape[1] * rw.shape[2] + rn.shape[1] * rn.shape[2]
    mine = lax.axis_index(SP).astype(jnp.int32).reshape(1)
    f32 = functools.partial(jax.ShapeDtypeStruct, dtype=jnp.float32)
    table = f32((2, extent, states))
    cost = pl.CostEstimate(flops=20_000_000, bytes_accessed=2_000_000, transcendentals=100_000)
    edge = jax.ShapeDtypeStruct((SUB, LANES), jnp.bfloat16)
    out, inputs, last, first, *tables = pl.pallas_call(
        local_kernel,
        name="local_states",
        out_shape=(
            jax.ShapeDtypeStruct((lax.axis_size(SP), SUB, LANES), jnp.bfloat16),
            jax.ShapeDtypeStruct((extent, 2 * channels), jnp.bfloat16),
            edge,
            edge,
            table,
            table,
            table,
            table,
        ),
        in_specs=in_memory(10),
        out_specs=tuple(in_memory(8)[1:]),
        cost_estimate=cost,
    )(mine, input_wide.T, input_narrow.T, spacing.reshape(1, -1), stream, rw, tw, dw, rn, tn, dn)
    with jax.named_scope("exchange"):
        arrived = lax.all_to_all(out, SP, split_axis=0, concat_axis=0, tiled=True)
    count = lax.axis_size(SP)
    with jax.named_scope("low"):
        low = lax.ppermute(last, SP, [(i, i + 1) for i in range(count - 1)])
    with jax.named_scope("high"):
        high = lax.ppermute(first, SP, [(i + 1, i) for i in range(count - 1)])
    more, beside = pl.pallas_call(
        beside_kernel,
        name="beside",
        out_shape=(f32((8, states)), jax.ShapeDtypeStruct((EXTRA, 2 * channels), jnp.bfloat16)),
        in_specs=in_memory(8)[1:],
        out_specs=tuple(in_memory(2)[1:]),
        cost_estimate=cost,
    )(low, high, rw, tw, dw, rn, tn, dn)
    slots = pl.pallas_call(
        reading_kernel,
        name="readings",
        out_shape=jax.ShapeDtypeStruct(
            (lax.axis_size("tp"), extent + EXTRA, 2 * channels), jnp.bfloat16
        ),
        in_specs=in_memory(15),
        out_specs=in_memory(1)[1],
        cost_estimate=cost,
    )(mine, arrived, rw, tw, cw, rn, tn, cn, skip_gain.reshape(1, -1), inputs, beside, more, *tables)
    return slots, low[1:2], high[1:2]


def on_device(
    input_wide,
    input_narrow,
    spacing,
    rate_wide,
    turn_wide,
    drive_wide,
    read_wide,
    narrow_decay_rate,
    turn_narrow,
    drive_narrow,
    read_narrow,
    skip_gain,
    out_value,
    out_gate,
    stream,
    norm_gain,
    up_value,
    up_gate,
    conv_taps,
    down_weight,
):
    pair, quads = lax.axis_size("zi"), lax.axis_size("gi")
    share = pair * quads
    extent = input_wide.shape[0]
    block, part = weight_block(up_value, up_gate, down_weight)
    block, input_wide, input_narrow, spacing = lax.optimization_barrier(
        (block, input_wide, input_narrow, spacing)
    )
    weights = lax.all_gather(block, "zp", axis=0, tiled=True)
    mixer_in, low, high = mixer(
        input_wide,
        input_narrow,
        spacing,
        stream,
        (rate_wide, turn_wide, drive_wide, read_wide),
        (narrow_decay_rate, turn_narrow, drive_narrow, read_narrow),
        skip_gain,
    )
    channels = input_wide.shape[1]
    slots = lax.all_to_all(mixer_in, "tp", split_axis=0, concat_axis=0, tiled=True)
    peers = slots.shape[0]
    rows = jnp.moveaxis(slots, 0, 1).reshape(extent + EXTRA, -1)

    def by_slot(weight):
        turned = jnp.moveaxis(weight.reshape(2, peers, channels, -1), 0, 1)
        return turned.reshape(weight.shape)

    value = jnp.dot(rows, by_slot(out_value), preferred_element_type=jnp.float32)
    gate = jnp.dot(rows, by_slot(out_gate), preferred_element_type=jnp.float32)
    mine, count = lax.axis_index(SP), lax.axis_size(SP)
    row = jnp.arange(extent + 2)[:, None]
    inside = ((row != extent) | (mine > 0)) & ((row != extent + 1) | (mine < count - 1))
    branch = (value * jax.nn.sigmoid(gate))[: extent + 2]
    middle = jnp.concatenate([stream, low, high], axis=0).astype(jnp.float32) + branch
    middle = jnp.where(inside, middle, 0.0).astype(jnp.bfloat16)
    sent = jnp.concatenate([middle, addends(norm_gain)], axis=0)
    middle = middle[:extent]
    slots = sent_to_all(sent, MEMBERS)
    slots = slots.reshape(quads, pair, -1, *sent.shape)
    size = pair * extent
    normed = pl.pallas_call(
        functools.partial(norm_kernel, extent),
        name="norm",
        out_shape=jax.ShapeDtypeStruct((quads, size + EXTRA, peers * LANES), jnp.bfloat16),
        in_specs=in_memory(1)[1:],
        out_specs=in_memory(1)[1],
        compiler_params=pltpu.CompilerParams(vmem_limit_bytes=VMEM_BYTES),
        cost_estimate=pl.CostEstimate(
            flops=3_000_000, bytes_accessed=2_000_000, transcendentals=1000
        ),
    )(slots)
    width = lanes_up(2 * part)
    taps = conv_taps.reshape(2, 3, share, -1)
    mine = lax.axis_index("gi") * pair + lax.axis_index("zi")
    taps = lax.dynamic_index_in_dim(taps, mine, 2, keepdims=False)
    taps = padded_last(jnp.moveaxis(taps, 0, 1).reshape(3, -1), width)
    terms = pl.pallas_call(
        functools.partial(ffn_kernel, part),
        name="ffn",
        out_shape=jax.ShapeDtypeStruct((share * peers, extent, LANES), jnp.bfloat16),
        in_specs=in_memory(3)[1:],
        out_specs=in_memory(1)[1],
        compiler_params=pltpu.CompilerParams(vmem_limit_bytes=VMEM_BYTES),
        cost_estimate=pl.CostEstimate(
            flops=600_000_000, bytes_accessed=4_000_000, transcendentals=100_000
        ),
    )(normed, weights, taps)
    arrived = lax.all_to_all(terms, MEMBERS, split_axis=0, concat_axis=0, tiled=True)
    ffn = jnp.sum(arrived.astype(jnp.float32), axis=0)
    return (middle.astype(jnp.float32) + ffn).astype(jnp.bfloat16)


def solution(mesh):
    grp, sp, tp = mesh.devices.shape
    quads = SHARE if grp % SHARE == 0 else 1
    parted = Mesh(
        mesh.devices.reshape(grp // quads, quads, sp // SHARE, SHARE, tp),
        ("gp", "gi", *SP, "tp"),
    )
    spot = ("gp", "gi", *SP)
    placed = (
        P(spot, "tp"),
        P(spot, "tp"),
        P(spot),
        P(None, "tp", None),
        P(None, "tp", None),
        P(None, "tp", None, None),
        P(None, "tp", None, None),
        P(None, "tp", None),
        P(None, "tp", None),
        P(None, "tp", None, None),
        P(None, "tp", None, None),
        P(None, "tp"),
        P(None, "tp"),
        P(None, "tp"),
        P(spot, "tp"),
        P("tp"),
        P(SP, "tp"),
        P(SP, "tp"),
        P(None, None, "tp"),
        P("tp", SP),
    )
    return jax.shard_map(
        on_device, mesh=parted, in_specs=placed, out_specs=P(spot, "tp"), check_vma=False
    )
```

```python
import functools
import math

import jax
import jax.numpy as jnp
from jax import lax
from jax.experimental import pallas as pl
from jax.experimental.pallas import tpu as pltpu
from jax.sharding import Mesh
from jax.sharding import PartitionSpec as P

SHARE = 2
LANES = 128
SUB = 8
VMEM_BYTES = 24 * 2**20
EXTRA = 16

epsilon = 1e-06
SP = ("zp", "zi")
MEMBERS = ("gi", "zi", "tp")


def complex_times(left_real, left_quad, right_real, right_quad):
    return (
        left_real * right_real - left_quad * right_quad,
        left_real * right_quad + left_quad * right_real,
    )


def lanes_up(count):
    return -(-count // LANES) * LANES


def padded_last(array, width):
    return jnp.pad(array, [(0, 0)] * (array.ndim - 1) + [(0, width - array.shape[-1])])


def sent_to_all(array, axes):
    copies = jnp.broadcast_to(array, (lax.axis_size(axes), *array.shape))
    return lax.all_to_all(copies, axes, split_axis=0, concat_axis=0, tiled=True)


def pack_kernel(quads, which, value, gate, down, out):
    pair, rows, width = out.shape
    part = value.shape[1] // (pair * quads)
    for k in range(pair):
        pieces = []
        for w in (value, gate, down):
            own = None
            for q in range(quads):
                at = (q * pair + k) * part
                piece = w[:, at : at + part].astype(jnp.float32)
                own = piece if own is None else jnp.where(which[0] == q, piece, own)
            pieces.append(own)
        if width > 3 * part:
            pieces.append(jnp.zeros((rows, width - 3 * part), jnp.float32))
        out[k] = jnp.concatenate(pieces, axis=1).astype(out.dtype)


def weight_block(up_value, up_gate, down_weight):
    pair, quads = lax.axis_size("zi"), lax.axis_size("gi")
    rows, columns = up_value.shape
    part = columns // (pair * quads)
    which = lax.axis_index("gi").astype(jnp.int32).reshape(1)
    block = pl.pallas_call(
        functools.partial(pack_kernel, quads),
        name="pack",
        out_shape=jax.ShapeDtypeStruct((pair, rows, lanes_up(3 * part)), jnp.bfloat16),
        in_specs=in_memory(3),
        out_specs=in_memory(1)[1],
    )(which, up_value, up_gate, down_weight.T)
    block = lax.all_to_all(block, "zi", 0, 0, tiled=True)
    return block.reshape(pair * rows, -1), part


def cos_sin(turn, span):
    turns = (turn * (0.5 / math.pi)) * span
    half = (turns - jnp.floor(turns + 0.5)) * math.pi
    square = half * half
    sine, cosine = 1.0 / math.factorial(13), 1.0 / math.factorial(12)
    for k in range(11, 0, -2):
        sine = sine * square + (-1.0) ** (k // 2) / math.factorial(k)
    for k in range(10, -1, -2):
        cosine = cosine * square + (-1.0) ** (k // 2) / math.factorial(k)
    sine = sine * half
    return 1.0 - 2.0 * sine * sine, 2.0 * sine * cosine


def powers(rate, turn, span):
    shrink = jnp.exp(-rate * span)
    cosine, sine = cos_sin(turn, span)
    return shrink * cosine, shrink * sine


def in_lanes(wide, narrow, d):
    rows = [ref[d, k : k + 1, :] for ref in (wide, narrow) for k in range(ref.shape[1])]
    return jnp.concatenate(rows, axis=1)


def two_terms(x):
    high = x.astype(jnp.bfloat16)
    return high, (x - high.astype(jnp.float32)).astype(jnp.bfloat16)


def spread(ref, d, part, groups):
    states = ref.shape[2] // 2
    own = ref[d][:, part * states : (part + 1) * states]
    wide = jnp.concatenate([own] * groups, axis=1)
    row = lax.broadcasted_iota(jnp.int32, wide.shape, 0) // (wide.shape[0] // groups)
    lane = lax.broadcasted_iota(jnp.int32, wide.shape, 1) // states
    return two_terms(jnp.where(row == lane, wide, 0.0))


def shuffled(size, extent, row_axis):
    row = lax.broadcasted_iota(jnp.int32, (size, size), row_axis)
    position = lax.broadcasted_iota(jnp.int32, (size, size), 1 - row_axis)
    moved = (row % SUB) * (extent // SUB) + row // SUB
    return position == jnp.where(row < extent, moved, row)


def length_row(value):
    lane = lax.broadcasted_iota(jnp.int32, value.shape, 1)
    out = jnp.zeros(value.shape, jnp.float32)
    for k in range(3):
        addend = value.astype(jnp.bfloat16).astype(jnp.float32)
        out = jnp.where(lane == k, addend, out)
        value = value - addend
    return out


def local_kernel(
    mine, wide_in, narrow_in, spacing, stream, rw, tw, dw, rn, tn, dn,
    out, inputs, last, first, sr, si, pr, pi
):
    extent = spacing.shape[1]
    steps = extent // SUB
    place = shuffled(extent, extent, 0)
    span = jnp.sum(jnp.where(place, spacing[...], 0.0), axis=1, keepdims=True)
    both = jnp.concatenate([wide_in[...], narrow_in[...]], axis=0)
    rows = lax.dot_general(
        place.astype(jnp.float32).astype(jnp.bfloat16),
        both,
        (((1,), (1,)), ((), ())),
        preferred_element_type=jnp.float32,
    ).astype(jnp.bfloat16)
    inputs[...] = rows
    for edge, at in ((first, 0), (last, extent - 1)):
        near = at // (2 * SUB) * (2 * SUB)
        pieces = [
            x[near : near + 2 * SUB].astype(jnp.float32)[at - near : at - near + 1]
            for x in (rows, stream[...])
        ]
        pieces.append(length_row(jnp.broadcast_to(span[at : at + 1], (1, LANES))))
        pieces.append(jnp.zeros((SUB - 3, LANES), jnp.float32))
        edge[...] = jnp.concatenate(pieces, axis=0).astype(edge.dtype)
    channels = wide_in.shape[0]
    halves = ((rows[:, :channels], dw, rw.shape[1]), (rows[:, channels:], dn, rn.shape[1]))
    tiles = []
    for d in range(2):
        rate, turn = in_lanes(rw, rn, d), in_lanes(tw, tn, d)
        push = []
        for part in range(2):
            pieces = []
            for x, drive, groups in halves:
                high, low = spread(drive, d, part, groups)
                pieces.append(
                    jnp.dot(x, high, preferred_element_type=jnp.float32)
                    + jnp.dot(x, low, preferred_element_type=jnp.float32)
                )
            push.append(jnp.concatenate(pieces, axis=1))
        square = rate * rate + turn * turn
        back_real, back_quad = -rate / square, -turn / square
        decay_real, decay_quad = powers(rate, turn, span)
        coef_real, coef_quad = complex_times(decay_real - 1.0, decay_quad, back_real, back_quad)
        kick_real, kick_quad = complex_times(coef_real, coef_quad, push[0], push[1])
        order = range(steps) if d == 0 else range(steps - 1, -1, -1)
        state = None
        for i in order:
            at = slice(i * SUB, (i + 1) * SUB)
            decay = (decay_real[at], decay_quad[at])
            if state is None:
                state, power = (kick_real[at], kick_quad[at]), decay
            else:
                kept = complex_times(*decay, *state)
                state = (kept[0] + kick_real[at], kept[1] + kick_quad[at])
                power = complex_times(*decay, *power)
            sr[d, at, :] = state[0]
            si[d, at, :] = state[1]
            pr[d, at, :] = power[0]
            pi[d, at, :] = power[1]
        end = None
        for c in range(SUB) if d == 0 else range(SUB - 1, -1, -1):
            own = (state[0][c : c + 1], state[1][c : c + 1])
            if end is None:
                end = own
            else:
                kept = complex_times(power[0][c : c + 1], power[1][c : c + 1], *end)
                end = (kept[0] + own[0], kept[1] + own[1])
        count = end[0].shape[1] // LANES
        pieces = [e[:, k * LANES : (k + 1) * LANES] for e in end for k in range(count)]
        total = jnp.sum(spacing[...], axis=1, keepdims=True)
        pieces.append(length_row(jnp.broadcast_to(total, (1, LANES))))
        pieces.append(jnp.zeros((SUB - len(pieces), LANES), jnp.float32))
        tiles.append(jnp.concatenate(pieces, axis=0))
    for j in range(out.shape[0]):
        out[j] = jnp.where(j > mine[0], tiles[0], tiles[1]).astype(out.dtype)


def addends(x):
    first = lax.reduce_precision(x, 8, 7)
    second = lax.reduce_precision(x - first, 8, 7)
    return jnp.stack([first, second, x - first - second]).astype(jnp.bfloat16)


def beside_kernel(low, high, rw, tw, dw, rn, tn, dn, inputs, *refs):
    rows = jnp.concatenate([low[0:1], high[0:1]], axis=0).astype(jnp.float32)
    rows = jnp.concatenate([rows, jnp.zeros((EXTRA - 2, rows.shape[1]), jnp.float32)], axis=0)
    rows = rows.astype(jnp.bfloat16)
    steps_out, rows_out, *handed = refs[len(refs) // 2 - 1 :]
    rows_out[: inputs.shape[0]] = inputs[...]
    rows_out[inputs.shape[0] :] = rows
    for source, place in zip(refs, handed):
        place[...] = source[...]
    channels = dw.shape[1]
    halves = ((rows[:, :channels], dw, rw.shape[1]), (rows[:, channels:], dn, rn.shape[1]))
    out = []
    for row, (d, side) in enumerate(((1, low), (0, high))):
        rate, turn = in_lanes(rw, rn, d), in_lanes(tw, tn, d)
        span = jnp.sum(side[2:3].astype(jnp.float32), axis=1, keepdims=True)
        push = []
        for part in range(2):
            pieces = []
            for x, drive, groups in halves:
                first, second = spread(drive, d, part, groups)
                pieces.append(
                    jnp.dot(x, first, preferred_element_type=jnp.float32)
                    + jnp.dot(x, second, preferred_element_type=jnp.float32)
                )
            push.append(jnp.concatenate(pieces, axis=1)[row : row + 1])
        square = rate * rate + turn * turn
        decay = powers(rate, turn, jnp.broadcast_to(span, rate.shape))
        coef = complex_times(decay[0] - 1.0, decay[1], -rate / square, -turn / square)
        out += [*decay, *complex_times(*coef, *push)]
    out += [in_lanes(*pair, d) for pair in ((rw, rn), (tw, tn)) for d in range(2)]
    out.append(jnp.zeros((2 * SUB - len(out), out[0].shape[1]), jnp.float32))
    steps_out[...] = jnp.concatenate(out, axis=0)


def carried(mine, arrived, rates, turns, count):
    peers = arrived.shape[0]
    quads = 2 * count

    def tile(row):
        pieces = [row[:, k * LANES : (k + 1) * LANES] for k in range(count)] * 2
        pieces.append(jnp.zeros((SUB - quads, LANES), jnp.float32))
        return jnp.concatenate(pieces, axis=0)

    rates, turns = [tile(r) for r in rates], [tile(t) for t in turns]
    ends = [arrived[j].astype(jnp.float32) for j in range(peers)]
    spans = [jnp.sum(e[quads : quads + 1], axis=1, keepdims=True) for e in ends]
    spans = [jnp.broadcast_to(x, (1, LANES)) for x in spans]
    zero = jnp.zeros((1, LANES), jnp.float32)
    before, after = [zero] * peers, [zero] * peers
    for j in range(peers - 2, -1, -1):
        before[j] = jnp.where(j + 1 < mine, before[j + 1] + spans[j + 1], zero)
    for j in range(1, peers):
        after[j] = jnp.where(j - 1 > mine, after[j - 1] + spans[j - 1], zero)
    sums = [jnp.zeros((SUB, LANES), jnp.float32)] * 2
    for j in range(peers):
        early, late = j < mine, j > mine
        gap = jnp.where(early, before[j], after[j])
        weight = powers(
            jnp.where(early, rates[0], rates[1]), jnp.where(early, turns[0], turns[1]), gap
        )
        end = ends[j]
        crossed = jnp.concatenate([-end[count:quads], end[:count], end[quads:]], axis=0)
        term = weight[0] * end + weight[1] * crossed
        sums[0] = sums[0] + jnp.where(early, term, 0.0)
        sums[1] = sums[1] + jnp.where(late, term, 0.0)
    out = []
    for s in sums:
        row = [s[k : k + 1] for k in range(quads)]
        out.append((jnp.concatenate(row[:count], axis=1), jnp.concatenate(row[count:], axis=1)))
    return out


def reading_kernel(
    groups_of, mine, arrived, dw, dn, skip, inputs, more, sr, si, pr, pi, out
):
    extent = inputs.shape[0] - EXTRA
    steps = extent // SUB
    count = sr.shape[2] // LANES
    rates = [more[k : k + 1, :] for k in (8, 9)]
    turns = [more[k : k + 1, :] for k in (10, 11)]
    carries = carried(mine[0], arrived, rates, turns, count)
    channels = dw.shape[1]
    size = extent + EXTRA
    reading = [jnp.zeros((size, channels), jnp.float32) for _ in range(2)]
    for d in range(2):
        last = slice((steps - 1) * SUB, extent) if d == 0 else slice(0, SUB)
        state, power = (sr[d, last, :], si[d, last, :]), (pr[d, last, :], pi[d, last, :])
        carry, starts = carries[d], [None] * SUB
        for c in range(SUB) if d == 0 else range(SUB - 1, -1, -1):
            starts[c] = carry
            at = slice(c, c + 1)
            kept = complex_times(power[0][at], power[1][at], *carry)
            carry = (kept[0] + state[0][at], kept[1] + state[1][at])
        start = [jnp.concatenate([s[k] for s in starts], axis=0) for k in range(2)]
        start = [jnp.concatenate([s] * steps, axis=0) for s in start]
        extra = complex_times(pr[d], pi[d], *start)
        step = [more[k : k + 1, :] for k in range(4 * (1 - d), 4 * (1 - d) + 4)]
        beyond = complex_times(*step[:2], *carry)
        beyond = [beyond[k] + step[2 + k] for k in range(2)]
        pairs = zip(carries[d], beyond) if d == 0 else zip(beyond, carries[d])
        spare = jnp.zeros((EXTRA - 2, carry[0].shape[1]), jnp.float32)
        tail = [jnp.concatenate([*pair, spare], axis=0) for pair in pairs]
        at = 0
        for which, (read, groups) in enumerate(zip((dw, dn), groups_of)):
            upto = at + groups * read.shape[2] // 2
            for part, local in enumerate((sr, si)):
                value = local[d, :, at:upto] + extra[part][:, at:upto]
                value = jnp.concatenate([value, tail[part][:, at:upto]], axis=0)
                high, low = two_terms(value)
                read_high, read_low = spread(read, d, part, groups)
                for x, y in ((high, read_high), (low, read_high), (high, read_low)):
                    reading[which] = reading[which] + lax.dot_general(
                        x, y, (((1,), (1,)), ((), ())), preferred_element_type=jnp.float32
                    )
            at = upto
    rows = inputs[...].astype(jnp.float32)
    total = jnp.concatenate(reading, axis=1) + skip[...] * rows
    mixed = jax.nn.gelu(total).astype(jnp.bfloat16)
    back = shuffled(size, extent, 1).astype(jnp.float32).astype(jnp.bfloat16)
    rows = jnp.dot(back, mixed, preferred_element_type=jnp.float32).astype(jnp.bfloat16)
    for k in range(out.shape[0]):
        out[k] = rows


def norm_kernel(extent, slots, out):
    quads, pair, peers = slots.shape[:3]
    gains = [
        jnp.sum(slots[0, 0, k, extent + 2 : extent + 5, :].astype(jnp.float32), axis=0, keepdims=True)
        for k in range(peers)
    ]

    def scaled(pieces, q, rows):
        square = sum(jnp.sum(x * x, axis=1, keepdims=True) for x in pieces)
        scale = lax.rsqrt(square / (peers * LANES) + epsilon)
        for k in range(peers):
            value = pieces[k] * scale * gains[k]
            out[q, rows, k * LANES : (k + 1) * LANES] = value.astype(out.dtype)

    for q in range(quads):
        for m in range(pair):
            pieces = [slots[q, m, k, 0:extent, :].astype(jnp.float32) for k in range(peers)]
            scaled(pieces, q, slice(m * extent, (m + 1) * extent))
        pieces = []
        spare = jnp.zeros((EXTRA - 2, LANES), jnp.float32)
        for k in range(peers):
            low = slots[q, 0, k, extent : extent + 2, :].astype(jnp.float32)[0:1]
            high = slots[q, pair - 1, k, extent : extent + 2, :].astype(jnp.float32)[1:2]
            pieces.append(jnp.concatenate([low, high, spare], axis=0))
        scaled(pieces, q, slice(pair * extent, pair * extent + EXTRA))


def ffn_kernel(part, normed, weights, taps, out):
    quads, size, _ = normed.shape
    size = size - EXTRA
    width = taps.shape[1]
    peers = weights.shape[0] // LANES
    extent = out.shape[1]
    at = 2 * part // LANES * LANES
    row = lax.broadcasted_iota(jnp.int32, (size, width), 0)
    lane = lax.broadcasted_iota(jnp.int32, (size, width), 1)
    room = weights.shape[1] - at
    for q in range(quads):
        pre = jnp.dot(normed[q], weights[:, :width], preferred_element_type=jnp.float32)
        pre = pre.astype(jnp.bfloat16).astype(jnp.float32)
        main, low, high = pre[:size], pre[size : size + 1], pre[size + 1 : size + 2]
        before = jnp.where(row == 0, low, pltpu.roll(main, 1, 0))
        after = jnp.where(row == size - 1, high, pltpu.roll(main, size - 1, 0))
        conv = taps[0:1, :] * before + taps[1:2, :] * main + taps[2:3, :] * after
        gate = pltpu.roll(conv, width - part, 1)
        hidden = jnp.where(lane < part, jax.nn.silu(gate) * conv, 0.0)
        if room != width:
            spare = jnp.zeros((size, abs(room - width)), jnp.float32)
            hidden = jnp.concatenate([hidden, spare], axis=1) if room > width else hidden[:, :room]
        hidden = pltpu.roll(hidden, 2 * part - at, 1).astype(jnp.bfloat16)
        for k in range(peers):
            terms = lax.dot_general(
                hidden,
                weights[k * LANES : (k + 1) * LANES, at:],
                (((1,), (1,)), ((), ())),
                preferred_element_type=jnp.float32,
            ).astype(out.dtype)
            for m in range(size // extent):
                out[(q * (size // extent) + m) * peers + k] = terms[m * extent : (m + 1) * extent]


def in_memory(count):
    vmem = pl.BlockSpec(memory_space=pltpu.VMEM)
    return [pl.BlockSpec(memory_space=pltpu.SMEM)] + [vmem] * count


def mixer(input_wide, input_narrow, spacing, stream, wide, narrow, skip_gain):
    extent, channels = input_wide.shape
    rw, tw, dw, cw = wide
    rn, tn, dn, cn = narrow
    dw, cw, dn, cn = (m.reshape(2, channels, m.shape[3]) for m in (dw, cw, dn, cn))
    states = rw.shape[1] * rw.shape[2] + rn.shape[1] * rn.shape[2]
    mine = lax.axis_index(SP).astype(jnp.int32).reshape(1)
    f32 = functools.partial(jax.ShapeDtypeStruct, dtype=jnp.float32)
    table = f32((2, extent, states))
    cost = pl.CostEstimate(flops=20_000_000, bytes_accessed=2_000_000, transcendentals=100_000)
    edge = jax.ShapeDtypeStruct((SUB, LANES), jnp.bfloat16)
    out, inputs, last, first, *tables = pl.pallas_call(
        local_kernel,
        name="local_states",
        out_shape=(
            jax.ShapeDtypeStruct((lax.axis_size(SP), SUB, LANES), jnp.bfloat16),
            jax.ShapeDtypeStruct((extent, 2 * channels), jnp.bfloat16),
            edge,
            edge,
            table,
            table,
            table,
            table,
        ),
        in_specs=in_memory(10),
        out_specs=tuple(in_memory(8)[1:]),
        cost_estimate=cost,
    )(mine, input_wide.T, input_narrow.T, spacing.reshape(1, -1), stream, rw, tw, dw, rn, tn, dn)
    with jax.named_scope("exchange"):
        arrived = lax.all_to_all(out, SP, split_axis=0, concat_axis=0, tiled=True)
    count = lax.axis_size(SP)
    with jax.named_scope("low"):
        low = lax.ppermute(last, SP, [(i, i + 1) for i in range(count - 1)])
    with jax.named_scope("high"):
        high = lax.ppermute(first, SP, [(i + 1, i) for i in range(count - 1)])
    more, inputs, *tables = pl.pallas_call(
        beside_kernel,
        name="beside",
        out_shape=(
            f32((2 * SUB, states)),
            jax.ShapeDtypeStruct((extent + EXTRA, 2 * channels), jnp.bfloat16),
            table,
            table,
            table,
            table,
        ),
        in_specs=in_memory(13)[1:],
        out_specs=tuple(in_memory(6)[1:]),
        compiler_params=pltpu.CompilerParams(vmem_limit_bytes=VMEM_BYTES),
        cost_estimate=cost,
    )(low, high, rw, tw, dw, rn, tn, dn, inputs, *tables)
    slots = pl.pallas_call(
        functools.partial(reading_kernel, (rw.shape[1], rn.shape[1])),
        name="readings",
        out_shape=jax.ShapeDtypeStruct(
            (lax.axis_size("tp"), extent + EXTRA, 2 * channels), jnp.bfloat16
        ),
        in_specs=in_memory(10),
        out_specs=in_memory(1)[1],
        compiler_params=pltpu.CompilerParams(vmem_limit_bytes=VMEM_BYTES),
        cost_estimate=cost,
    )(mine, arrived, cw, cn, skip_gain.reshape(1, -1), inputs, more, *tables)
    return slots, low[1:2], high[1:2]


def on_device(
    input_wide,
    input_narrow,
    spacing,
    rate_wide,
    turn_wide,
    drive_wide,
    read_wide,
    narrow_decay_rate,
    turn_narrow,
    drive_narrow,
    read_narrow,
    skip_gain,
    out_value,
    out_gate,
    stream,
    norm_gain,
    up_value,
    up_gate,
    conv_taps,
    down_weight,
):
    pair, quads = lax.axis_size("zi"), lax.axis_size("gi")
    share = pair * quads
    extent = input_wide.shape[0]
    block, part = weight_block(up_value, up_gate, down_weight)
    block, input_wide, input_narrow, spacing = lax.optimization_barrier(
        (block, input_wide, input_narrow, spacing)
    )
    weights = lax.all_gather(block, "zp", axis=0, tiled=True)
    mixer_in, low, high = mixer(
        input_wide,
        input_narrow,
        spacing,
        stream,
        (rate_wide, turn_wide, drive_wide, read_wide),
        (narrow_decay_rate, turn_narrow, drive_narrow, read_narrow),
        skip_gain,
    )
    channels = input_wide.shape[1]
    slots = lax.all_to_all(mixer_in, "tp", split_axis=0, concat_axis=0, tiled=True)
    peers = slots.shape[0]
    rows = jnp.moveaxis(slots, 0, 1).reshape(extent + EXTRA, -1)

    def by_slot(weight):
        turned = jnp.moveaxis(weight.reshape(2, peers, channels, -1), 0, 1)
        return turned.reshape(weight.shape)

    value = jnp.dot(rows, by_slot(out_value), preferred_element_type=jnp.float32)
    gate = jnp.dot(rows, by_slot(out_gate), preferred_element_type=jnp.float32)
    mine, count = lax.axis_index(SP), lax.axis_size(SP)
    row = jnp.arange(extent + 2)[:, None]
    inside = ((row != extent) | (mine > 0)) & ((row != extent + 1) | (mine < count - 1))
    branch = (value * jax.nn.sigmoid(gate))[: extent + 2]
    middle = jnp.concatenate([stream, low, high], axis=0).astype(jnp.float32) + branch
    middle = jnp.where(inside, middle, 0.0).astype(jnp.bfloat16)
    sent = jnp.concatenate([middle, addends(norm_gain)], axis=0)
    middle = middle[:extent]
    slots = sent_to_all(sent, MEMBERS)
    slots = slots.reshape(quads, pair, -1, *sent.shape)
    size = pair * extent
    normed = pl.pallas_call(
        functools.partial(norm_kernel, extent),
        name="norm",
        out_shape=jax.ShapeDtypeStruct((quads, size + EXTRA, peers * LANES), jnp.bfloat16),
        in_specs=in_memory(1)[1:],
        out_specs=in_memory(1)[1],
        compiler_params=pltpu.CompilerParams(vmem_limit_bytes=VMEM_BYTES),
        cost_estimate=pl.CostEstimate(
            flops=3_000_000, bytes_accessed=2_000_000, transcendentals=1000
        ),
    )(slots)
    width = lanes_up(2 * part)
    taps = conv_taps.reshape(2, 3, share, -1)
    mine = lax.axis_index("gi") * pair + lax.axis_index("zi")
    taps = lax.dynamic_index_in_dim(taps, mine, 2, keepdims=False)
    taps = padded_last(jnp.moveaxis(taps, 0, 1).reshape(3, -1), width)
    terms = pl.pallas_call(
        functools.partial(ffn_kernel, part),
        name="ffn",
        out_shape=jax.ShapeDtypeStruct((share * peers, extent, LANES), jnp.bfloat16),
        in_specs=in_memory(3)[1:],
        out_specs=in_memory(1)[1],
        compiler_params=pltpu.CompilerParams(vmem_limit_bytes=VMEM_BYTES),
        cost_estimate=pl.CostEstimate(
            flops=600_000_000, bytes_accessed=4_000_000, transcendentals=100_000
        ),
    )(normed, weights, taps)
    arrived = lax.all_to_all(terms, MEMBERS, split_axis=0, concat_axis=0, tiled=True)
    ffn = jnp.sum(arrived.astype(jnp.float32), axis=0)
    return (middle.astype(jnp.float32) + ffn).astype(jnp.bfloat16)


def solution(mesh):
    grp, sp, tp = mesh.devices.shape
    quads = SHARE if grp % SHARE == 0 else 1
    parted = Mesh(
        mesh.devices.reshape(grp // quads, quads, sp // SHARE, SHARE, tp),
        ("gp", "gi", *SP, "tp"),
    )
    spot = ("gp", "gi", *SP)
    placed = (
        P(spot, "tp"),
        P(spot, "tp"),
        P(spot),
        P(None, "tp", None),
        P(None, "tp", None),
        P(None, "tp", None, None),
        P(None, "tp", None, None),
        P(None, "tp", None),
        P(None, "tp", None),
        P(None, "tp", None, None),
        P(None, "tp", None, None),
        P(None, "tp"),
        P(None, "tp"),
        P(None, "tp"),
        P(spot, "tp"),
        P("tp"),
        P(SP, "tp"),
        P(SP, "tp"),
        P(None, None, "tp"),
        P("tp", SP),
    )
    return jax.shard_map(
        on_device, mesh=parted, in_specs=placed, out_specs=P(spot, "tp"), check_vma=False
    )
```

```python
import functools
import math

import jax
import jax.numpy as jnp
from jax import lax
from jax.experimental import pallas as pl
from jax.experimental.pallas import tpu as pltpu
from jax.sharding import Mesh
from jax.sharding import PartitionSpec as P

SHARE = 2
LANES = 128
SUB = 8
VMEM_BYTES = 24 * 2**20
FFN_BYTES = 53_500_000
EXTRA = 16

epsilon = 1e-06
SP = ("zp", "zi")
MEMBERS = ("gi", "zi", "tp")


def complex_times(left_real, left_quad, right_real, right_quad):
    return (
        left_real * right_real - left_quad * right_quad,
        left_real * right_quad + left_quad * right_real,
    )


def lanes_up(count):
    return -(-count // LANES) * LANES


def padded_last(array, width):
    return jnp.pad(array, [(0, 0)] * (array.ndim - 1) + [(0, width - array.shape[-1])])


def sent_to_all(array, axes):
    copies = jnp.broadcast_to(array, (lax.axis_size(axes), *array.shape))
    return lax.all_to_all(copies, axes, split_axis=0, concat_axis=0, tiled=True)


def pack_kernel(quads, which, value, gate, down, out):
    pair, rows, width = out.shape
    part = value.shape[1] // (pair * quads)
    for k in range(pair):
        pieces = []
        for w in (value, gate, down):
            own = None
            for q in range(quads):
                at = (q * pair + k) * part
                piece = w[:, at : at + part].astype(jnp.float32)
                own = piece if own is None else jnp.where(which[0] == q, piece, own)
            pieces.append(own)
        if width > 3 * part:
            pieces.append(jnp.zeros((rows, width - 3 * part), jnp.float32))
        out[k] = jnp.concatenate(pieces, axis=1).astype(out.dtype)


def weight_block(up_value, up_gate, down_weight):
    pair, quads = lax.axis_size("zi"), lax.axis_size("gi")
    rows, columns = up_value.shape
    part = columns // (pair * quads)
    which = lax.axis_index("gi").astype(jnp.int32).reshape(1)
    block = pl.pallas_call(
        functools.partial(pack_kernel, quads),
        name="pack",
        out_shape=jax.ShapeDtypeStruct((pair, rows, lanes_up(3 * part)), jnp.bfloat16),
        in_specs=in_memory(3),
        out_specs=in_memory(1)[1],
    )(which, up_value, up_gate, down_weight.T)
    block = lax.all_to_all(block, "zi", 0, 0, tiled=True)
    return block.reshape(pair * rows, -1), part


def cos_sin(turn, span):
    turns = (turn * (0.5 / math.pi)) * span
    half = (turns - jnp.floor(turns + 0.5)) * math.pi
    square = half * half
    sine, cosine = 1.0 / math.factorial(13), 1.0 / math.factorial(12)
    for k in range(11, 0, -2):
        sine = sine * square + (-1.0) ** (k // 2) / math.factorial(k)
    for k in range(10, -1, -2):
        cosine = cosine * square + (-1.0) ** (k // 2) / math.factorial(k)
    sine = sine * half
    return 1.0 - 2.0 * sine * sine, 2.0 * sine * cosine


def powers(rate, turn, span):
    shrink = jnp.exp(-rate * span)
    cosine, sine = cos_sin(turn, span)
    return shrink * cosine, shrink * sine


def in_lanes(wide, narrow, d):
    rows = [ref[d, k : k + 1, :] for ref in (wide, narrow) for k in range(ref.shape[1])]
    return jnp.concatenate(rows, axis=1)


def two_terms(x):
    high = x.astype(jnp.bfloat16)
    return high, (x - high.astype(jnp.float32)).astype(jnp.bfloat16)


def spread(ref, d, part, groups):
    states = ref.shape[2] // 2
    own = ref[d][:, part * states : (part + 1) * states]
    wide = jnp.concatenate([own] * groups, axis=1)
    row = lax.broadcasted_iota(jnp.int32, wide.shape, 0) // (wide.shape[0] // groups)
    lane = lax.broadcasted_iota(jnp.int32, wide.shape, 1) // states
    return two_terms(jnp.where(row == lane, wide, 0.0))


def shuffled(size, extent, row_axis):
    row = lax.broadcasted_iota(jnp.int32, (size, size), row_axis)
    position = lax.broadcasted_iota(jnp.int32, (size, size), 1 - row_axis)
    moved = (row % SUB) * (extent // SUB) + row // SUB
    return position == jnp.where(row < extent, moved, row)


def length_row(value):
    lane = lax.broadcasted_iota(jnp.int32, value.shape, 1)
    out = jnp.zeros(value.shape, jnp.float32)
    for k in range(3):
        addend = value.astype(jnp.bfloat16).astype(jnp.float32)
        out = jnp.where(lane == k, addend, out)
        value = value - addend
    return out


def local_kernel(
    mine, wide_in, narrow_in, spacing, stream, rw, tw, dw, rn, tn, dn,
    out, inputs, last, first, sr, si, pr, pi
):
    extent = spacing.shape[1]
    steps = extent // SUB
    place = shuffled(extent, extent, 0)
    span = jnp.sum(jnp.where(place, spacing[...], 0.0), axis=1, keepdims=True)
    both = jnp.concatenate([wide_in[...], narrow_in[...]], axis=0)
    rows = lax.dot_general(
        place.astype(jnp.float32).astype(jnp.bfloat16),
        both,
        (((1,), (1,)), ((), ())),
        preferred_element_type=jnp.float32,
    ).astype(jnp.bfloat16)
    inputs[...] = rows
    for edge, at in ((first, 0), (last, extent - 1)):
        near = at // (2 * SUB) * (2 * SUB)
        pieces = [
            x[near : near + 2 * SUB].astype(jnp.float32)[at - near : at - near + 1]
            for x in (rows, stream[...])
        ]
        pieces.append(length_row(jnp.broadcast_to(span[at : at + 1], (1, LANES))))
        pieces.append(jnp.zeros((SUB - 3, LANES), jnp.float32))
        edge[...] = jnp.concatenate(pieces, axis=0).astype(edge.dtype)
    channels = wide_in.shape[0]
    halves = ((rows[:, :channels], dw, rw.shape[1]), (rows[:, channels:], dn, rn.shape[1]))
    tiles = []
    for d in range(2):
        rate, turn = in_lanes(rw, rn, d), in_lanes(tw, tn, d)
        push = []
        for part in range(2):
            pieces = []
            for x, drive, groups in halves:
                high, low = spread(drive, d, part, groups)
                pieces.append(
                    jnp.dot(x, high, preferred_element_type=jnp.float32)
                    + jnp.dot(x, low, preferred_element_type=jnp.float32)
                )
            push.append(jnp.concatenate(pieces, axis=1))
        square = rate * rate + turn * turn
        back_real, back_quad = -rate / square, -turn / square
        decay_real, decay_quad = powers(rate, turn, span)
        coef_real, coef_quad = complex_times(decay_real - 1.0, decay_quad, back_real, back_quad)
        kick_real, kick_quad = complex_times(coef_real, coef_quad, push[0], push[1])
        order = range(steps) if d == 0 else range(steps - 1, -1, -1)
        state = None
        for i in order:
            at = slice(i * SUB, (i + 1) * SUB)
            decay = (decay_real[at], decay_quad[at])
            if state is None:
                state, power = (kick_real[at], kick_quad[at]), decay
            else:
                kept = complex_times(*decay, *state)
                state = (kept[0] + kick_real[at], kept[1] + kick_quad[at])
                power = complex_times(*decay, *power)
            sr[d, at, :] = state[0]
            si[d, at, :] = state[1]
            pr[d, at, :] = power[0]
            pi[d, at, :] = power[1]
        end = None
        for c in range(SUB) if d == 0 else range(SUB - 1, -1, -1):
            own = (state[0][c : c + 1], state[1][c : c + 1])
            if end is None:
                end = own
            else:
                kept = complex_times(power[0][c : c + 1], power[1][c : c + 1], *end)
                end = (kept[0] + own[0], kept[1] + own[1])
        count = end[0].shape[1] // LANES
        pieces = [e[:, k * LANES : (k + 1) * LANES] for e in end for k in range(count)]
        total = jnp.sum(spacing[...], axis=1, keepdims=True)
        pieces.append(length_row(jnp.broadcast_to(total, (1, LANES))))
        pieces.append(jnp.zeros((SUB - len(pieces), LANES), jnp.float32))
        tiles.append(jnp.concatenate(pieces, axis=0))
    for j in range(out.shape[0]):
        out[j] = jnp.where(j > mine[0], tiles[0], tiles[1]).astype(out.dtype)


def addends(x):
    first = lax.reduce_precision(x, 8, 7)
    second = lax.reduce_precision(x - first, 8, 7)
    return jnp.stack([first, second, x - first - second]).astype(jnp.bfloat16)


def beside_kernel(low, high, rw, tw, dw, rn, tn, dn, inputs, *refs):
    rows = jnp.concatenate([low[0:1], high[0:1]], axis=0).astype(jnp.float32)
    rows = jnp.concatenate([rows, jnp.zeros((EXTRA - 2, rows.shape[1]), jnp.float32)], axis=0)
    rows = rows.astype(jnp.bfloat16)
    steps_out, rows_out, *handed = refs[len(refs) // 2 - 1 :]
    rows_out[: inputs.shape[0]] = inputs[...]
    rows_out[inputs.shape[0] :] = rows
    for source, place in zip(refs, handed):
        place[...] = source[...]
    channels = dw.shape[1]
    halves = ((rows[:, :channels], dw, rw.shape[1]), (rows[:, channels:], dn, rn.shape[1]))
    out = []
    for row, (d, side) in enumerate(((1, low), (0, high))):
        rate, turn = in_lanes(rw, rn, d), in_lanes(tw, tn, d)
        span = jnp.sum(side[2:3].astype(jnp.float32), axis=1, keepdims=True)
        push = []
        for part in range(2):
            pieces = []
            for x, drive, groups in halves:
                first, second = spread(drive, d, part, groups)
                pieces.append(
                    jnp.dot(x, first, preferred_element_type=jnp.float32)
                    + jnp.dot(x, second, preferred_element_type=jnp.float32)
                )
            push.append(jnp.concatenate(pieces, axis=1)[row : row + 1])
        square = rate * rate + turn * turn
        decay = powers(rate, turn, jnp.broadcast_to(span, rate.shape))
        coef = complex_times(decay[0] - 1.0, decay[1], -rate / square, -turn / square)
        out += [*decay, *complex_times(*coef, *push)]
    out += [in_lanes(*pair, d) for pair in ((rw, rn), (tw, tn)) for d in range(2)]
    out.append(jnp.zeros((2 * SUB - len(out), out[0].shape[1]), jnp.float32))
    steps_out[...] = jnp.concatenate(out, axis=0)


def carried(mine, arrived, rates, turns, count):
    peers = arrived.shape[0]
    quads = 2 * count

    def tile(row):
        pieces = [row[:, k * LANES : (k + 1) * LANES] for k in range(count)] * 2
        pieces.append(jnp.zeros((SUB - quads, LANES), jnp.float32))
        return jnp.concatenate(pieces, axis=0)

    rates, turns = [tile(r) for r in rates], [tile(t) for t in turns]
    ends = [arrived[j].astype(jnp.float32) for j in range(peers)]
    spans = [jnp.sum(e[quads : quads + 1], axis=1, keepdims=True) for e in ends]
    spans = [jnp.broadcast_to(x, (1, LANES)) for x in spans]
    zero = jnp.zeros((1, LANES), jnp.float32)
    before, after = [zero] * peers, [zero] * peers
    for j in range(peers - 2, -1, -1):
        before[j] = jnp.where(j + 1 < mine, before[j + 1] + spans[j + 1], zero)
    for j in range(1, peers):
        after[j] = jnp.where(j - 1 > mine, after[j - 1] + spans[j - 1], zero)
    sums = [jnp.zeros((SUB, LANES), jnp.float32)] * 2
    for j in range(peers):
        early, late = j < mine, j > mine
        gap = jnp.where(early, before[j], after[j])
        weight = powers(
            jnp.where(early, rates[0], rates[1]), jnp.where(early, turns[0], turns[1]), gap
        )
        end = ends[j]
        crossed = jnp.concatenate([-end[count:quads], end[:count], end[quads:]], axis=0)
        term = weight[0] * end + weight[1] * crossed
        sums[0] = sums[0] + jnp.where(early, term, 0.0)
        sums[1] = sums[1] + jnp.where(late, term, 0.0)
    out = []
    for s in sums:
        row = [s[k : k + 1] for k in range(quads)]
        out.append((jnp.concatenate(row[:count], axis=1), jnp.concatenate(row[count:], axis=1)))
    return out


def reading_kernel(
    groups_of, mine, arrived, dw, dn, skip, inputs, more, sr, si, pr, pi, out
):
    extent = inputs.shape[0] - EXTRA
    steps = extent // SUB
    count = sr.shape[2] // LANES
    rates = [more[k : k + 1, :] for k in (8, 9)]
    turns = [more[k : k + 1, :] for k in (10, 11)]
    carries = carried(mine[0], arrived, rates, turns, count)
    channels = dw.shape[1]
    size = extent + EXTRA
    reading = [jnp.zeros((size, channels), jnp.float32) for _ in range(2)]
    for d in range(2):
        last = slice((steps - 1) * SUB, extent) if d == 0 else slice(0, SUB)
        state, power = (sr[d, last, :], si[d, last, :]), (pr[d, last, :], pi[d, last, :])
        carry, starts = carries[d], [None] * SUB
        for c in range(SUB) if d == 0 else range(SUB - 1, -1, -1):
            starts[c] = carry
            at = slice(c, c + 1)
            kept = complex_times(power[0][at], power[1][at], *carry)
            carry = (kept[0] + state[0][at], kept[1] + state[1][at])
        start = [jnp.concatenate([s[k] for s in starts], axis=0) for k in range(2)]
        start = [jnp.concatenate([s] * steps, axis=0) for s in start]
        extra = complex_times(pr[d], pi[d], *start)
        step = [more[k : k + 1, :] for k in range(4 * (1 - d), 4 * (1 - d) + 4)]
        beyond = complex_times(*step[:2], *carry)
        beyond = [beyond[k] + step[2 + k] for k in range(2)]
        pairs = zip(carries[d], beyond) if d == 0 else zip(beyond, carries[d])
        spare = jnp.zeros((EXTRA - 2, carry[0].shape[1]), jnp.float32)
        tail = [jnp.concatenate([*pair, spare], axis=0) for pair in pairs]
        at = 0
        for which, (read, groups) in enumerate(zip((dw, dn), groups_of)):
            upto = at + groups * read.shape[2] // 2
            for part, local in enumerate((sr, si)):
                value = local[d, :, at:upto] + extra[part][:, at:upto]
                value = jnp.concatenate([value, tail[part][:, at:upto]], axis=0)
                high, low = two_terms(value)
                read_high, read_low = spread(read, d, part, groups)
                for x, y in ((high, read_high), (low, read_high), (high, read_low)):
                    reading[which] = reading[which] + lax.dot_general(
                        x, y, (((1,), (1,)), ((), ())), preferred_element_type=jnp.float32
                    )
            at = upto
    rows = inputs[...].astype(jnp.float32)
    total = jnp.concatenate(reading, axis=1) + skip[...] * rows
    mixed = jax.nn.gelu(total).astype(jnp.bfloat16)
    back = shuffled(size, extent, 1).astype(jnp.float32).astype(jnp.bfloat16)
    rows = jnp.dot(back, mixed, preferred_element_type=jnp.float32).astype(jnp.bfloat16)
    for k in range(out.shape[0]):
        out[k] = rows


def norm_kernel(extent, slots, out):
    quads, pair, peers = slots.shape[:3]
    gains = [
        jnp.sum(slots[0, 0, k, extent + 2 : extent + 5, :].astype(jnp.float32), axis=0, keepdims=True)
        for k in range(peers)
    ]

    def scaled(pieces, q, rows):
        square = sum(jnp.sum(x * x, axis=1, keepdims=True) for x in pieces)
        scale = lax.rsqrt(square / (peers * LANES) + epsilon)
        for k in range(peers):
            value = pieces[k] * scale * gains[k]
            out[q, rows, k * LANES : (k + 1) * LANES] = value.astype(out.dtype)

    for q in range(quads):
        for m in range(pair):
            pieces = [slots[q, m, k, 0:extent, :].astype(jnp.float32) for k in range(peers)]
            scaled(pieces, q, slice(m * extent, (m + 1) * extent))
        pieces = []
        spare = jnp.zeros((EXTRA - 2, LANES), jnp.float32)
        for k in range(peers):
            low = slots[q, 0, k, extent : extent + 2, :].astype(jnp.float32)[0:1]
            high = slots[q, pair - 1, k, extent : extent + 2, :].astype(jnp.float32)[1:2]
            pieces.append(jnp.concatenate([low, high, spare], axis=0))
        scaled(pieces, q, slice(pair * extent, pair * extent + EXTRA))


def ffn_kernel(part, normed, source, taps, out, weights, sems):
    quads, size, _ = normed.shape
    edge = taps.shape[1]
    copies = [
        pltpu.make_async_copy(source.at[:, cut], weights.at[:, cut], sems.at[n])
        for n, cut in enumerate((pl.ds(0, edge), pl.ds(edge, source.shape[1] - edge)))
    ]
    for copy in copies:
        copy.start()
    copies[0].wait()
    size = size - EXTRA
    width = taps.shape[1]
    peers = weights.shape[0] // LANES
    extent = out.shape[1]
    at = 2 * part // LANES * LANES
    row = lax.broadcasted_iota(jnp.int32, (size, width), 0)
    lane = lax.broadcasted_iota(jnp.int32, (size, width), 1)
    room = weights.shape[1] - at
    for q in range(quads):
        pre = jnp.dot(normed[q], weights[:, :width], preferred_element_type=jnp.float32)
        pre = pre.astype(jnp.bfloat16).astype(jnp.float32)
        main, low, high = pre[:size], pre[size : size + 1], pre[size + 1 : size + 2]
        before = jnp.where(row == 0, low, pltpu.roll(main, 1, 0))
        after = jnp.where(row == size - 1, high, pltpu.roll(main, size - 1, 0))
        conv = taps[0:1, :] * before + taps[1:2, :] * main + taps[2:3, :] * after
        gate = pltpu.roll(conv, width - part, 1)
        hidden = jnp.where(lane < part, jax.nn.silu(gate) * conv, 0.0)
        if room != width:
            spare = jnp.zeros((size, abs(room - width)), jnp.float32)
            hidden = jnp.concatenate([hidden, spare], axis=1) if room > width else hidden[:, :room]
        hidden = pltpu.roll(hidden, 2 * part - at, 1).astype(jnp.bfloat16)
        if q == 0:
            copies[1].wait()
        for k in range(peers):
            terms = lax.dot_general(
                hidden,
                weights[k * LANES : (k + 1) * LANES, at:],
                (((1,), (1,)), ((), ())),
                preferred_element_type=jnp.float32,
            ).astype(out.dtype)
            for m in range(size // extent):
                out[(q * (size // extent) + m) * peers + k] = terms[m * extent : (m + 1) * extent]


def in_memory(count):
    vmem = pl.BlockSpec(memory_space=pltpu.VMEM)
    return [pl.BlockSpec(memory_space=pltpu.SMEM)] + [vmem] * count


def mixer(input_wide, input_narrow, spacing, stream, wide, narrow, skip_gain):
    extent, channels = input_wide.shape
    rw, tw, dw, cw = wide
    rn, tn, dn, cn = narrow
    dw, cw, dn, cn = (m.reshape(2, channels, m.shape[3]) for m in (dw, cw, dn, cn))
    states = rw.shape[1] * rw.shape[2] + rn.shape[1] * rn.shape[2]
    mine = lax.axis_index(SP).astype(jnp.int32).reshape(1)
    f32 = functools.partial(jax.ShapeDtypeStruct, dtype=jnp.float32)
    table = f32((2, extent, states))
    cost = pl.CostEstimate(flops=20_000_000, bytes_accessed=2_000_000, transcendentals=100_000)
    edge = jax.ShapeDtypeStruct((SUB, LANES), jnp.bfloat16)
    out, inputs, last, first, *tables = pl.pallas_call(
        local_kernel,
        name="local_states",
        out_shape=(
            jax.ShapeDtypeStruct((lax.axis_size(SP), SUB, LANES), jnp.bfloat16),
            jax.ShapeDtypeStruct((extent, 2 * channels), jnp.bfloat16),
            edge,
            edge,
            table,
            table,
            table,
            table,
        ),
        in_specs=in_memory(10),
        out_specs=tuple(in_memory(8)[1:]),
        cost_estimate=cost,
    )(mine, input_wide.T, input_narrow.T, spacing.reshape(1, -1), stream, rw, tw, dw, rn, tn, dn)
    with jax.named_scope("exchange"):
        arrived = lax.all_to_all(out, SP, split_axis=0, concat_axis=0, tiled=True)
    count = lax.axis_size(SP)
    with jax.named_scope("low"):
        low = lax.ppermute(last, SP, [(i, i + 1) for i in range(count - 1)])
    with jax.named_scope("high"):
        high = lax.ppermute(first, SP, [(i + 1, i) for i in range(count - 1)])
    more, inputs, *tables = pl.pallas_call(
        beside_kernel,
        name="beside",
        out_shape=(
            f32((2 * SUB, states)),
            jax.ShapeDtypeStruct((extent + EXTRA, 2 * channels), jnp.bfloat16),
            table,
            table,
            table,
            table,
        ),
        in_specs=in_memory(13)[1:],
        out_specs=tuple(in_memory(6)[1:]),
        compiler_params=pltpu.CompilerParams(vmem_limit_bytes=VMEM_BYTES),
        cost_estimate=cost,
    )(low, high, rw, tw, dw, rn, tn, dn, inputs, *tables)
    slots = pl.pallas_call(
        functools.partial(reading_kernel, (rw.shape[1], rn.shape[1])),
        name="readings",
        out_shape=jax.ShapeDtypeStruct(
            (lax.axis_size("tp"), extent + EXTRA, 2 * channels), jnp.bfloat16
        ),
        in_specs=in_memory(10),
        out_specs=in_memory(1)[1],
        compiler_params=pltpu.CompilerParams(vmem_limit_bytes=VMEM_BYTES),
        cost_estimate=cost,
    )(mine, arrived, cw, cn, skip_gain.reshape(1, -1), inputs, more, *tables)
    return slots, low[1:2], high[1:2]


def on_device(
    input_wide,
    input_narrow,
    spacing,
    rate_wide,
    turn_wide,
    drive_wide,
    read_wide,
    narrow_decay_rate,
    turn_narrow,
    drive_narrow,
    read_narrow,
    skip_gain,
    out_value,
    out_gate,
    stream,
    norm_gain,
    up_value,
    up_gate,
    conv_taps,
    down_weight,
):
    pair, quads = lax.axis_size("zi"), lax.axis_size("gi")
    share = pair * quads
    extent = input_wide.shape[0]
    block, part = weight_block(up_value, up_gate, down_weight)
    block, input_wide, input_narrow, spacing = lax.optimization_barrier(
        (block, input_wide, input_narrow, spacing)
    )
    weights = lax.all_gather(block, "zp", axis=0, tiled=True)
    mixer_in, low, high = mixer(
        input_wide,
        input_narrow,
        spacing,
        stream,
        (rate_wide, turn_wide, drive_wide, read_wide),
        (narrow_decay_rate, turn_narrow, drive_narrow, read_narrow),
        skip_gain,
    )
    channels = input_wide.shape[1]
    slots = lax.all_to_all(mixer_in, "tp", split_axis=0, concat_axis=0, tiled=True)
    peers = slots.shape[0]
    rows = jnp.moveaxis(slots, 0, 1).reshape(extent + EXTRA, -1)

    def by_slot(weight):
        turned = jnp.moveaxis(weight.reshape(2, peers, channels, -1), 0, 1)
        return turned.reshape(weight.shape)

    value = jnp.dot(rows, by_slot(out_value), preferred_element_type=jnp.float32)
    gate = jnp.dot(rows, by_slot(out_gate), preferred_element_type=jnp.float32)
    mine, count = lax.axis_index(SP), lax.axis_size(SP)
    row = jnp.arange(extent + 2)[:, None]
    inside = ((row != extent) | (mine > 0)) & ((row != extent + 1) | (mine < count - 1))
    branch = (value * jax.nn.sigmoid(gate))[: extent + 2]
    middle = jnp.concatenate([stream, low, high], axis=0).astype(jnp.float32) + branch
    middle = jnp.where(inside, middle, 0.0).astype(jnp.bfloat16)
    sent = jnp.concatenate([middle, addends(norm_gain)], axis=0)
    middle = middle[:extent]
    slots = sent_to_all(sent, MEMBERS)
    slots = slots.reshape(quads, pair, -1, *sent.shape)
    size = pair * extent
    normed = pl.pallas_call(
        functools.partial(norm_kernel, extent),
        name="norm",
        out_shape=jax.ShapeDtypeStruct((quads, size + EXTRA, peers * LANES), jnp.bfloat16),
        in_specs=in_memory(1)[1:],
        out_specs=in_memory(1)[1],
        compiler_params=pltpu.CompilerParams(vmem_limit_bytes=VMEM_BYTES),
        cost_estimate=pl.CostEstimate(
            flops=3_000_000, bytes_accessed=2_000_000, transcendentals=1000
        ),
    )(slots)
    width = lanes_up(2 * part)
    taps = conv_taps.reshape(2, 3, share, -1)
    mine = lax.axis_index("gi") * pair + lax.axis_index("zi")
    taps = lax.dynamic_index_in_dim(taps, mine, 2, keepdims=False)
    taps = padded_last(jnp.moveaxis(taps, 0, 1).reshape(3, -1), width)
    terms = pl.pallas_call(
        functools.partial(ffn_kernel, part),
        name="ffn",
        out_shape=jax.ShapeDtypeStruct((share * peers, extent, LANES), jnp.bfloat16),
        in_specs=[
            pl.BlockSpec(memory_space=space) for space in (pltpu.VMEM, pl.ANY, pltpu.VMEM)
        ],
        out_specs=in_memory(1)[1],
        scratch_shapes=[
            pltpu.VMEM(weights.shape, weights.dtype),
            pltpu.SemaphoreType.DMA((2,)),
        ],
        compiler_params=pltpu.CompilerParams(vmem_limit_bytes=FFN_BYTES),
        cost_estimate=pl.CostEstimate(
            flops=600_000_000, bytes_accessed=4_000_000, transcendentals=100_000
        ),
    )(normed, weights, taps)
    arrived = lax.all_to_all(terms, MEMBERS, split_axis=0, concat_axis=0, tiled=True)
    ffn = jnp.sum(arrived.astype(jnp.float32), axis=0)
    return (middle.astype(jnp.float32) + ffn).astype(jnp.bfloat16)


def solution(mesh):
    grp, sp, tp = mesh.devices.shape
    quads = SHARE if grp % SHARE == 0 else 1
    parted = Mesh(
        mesh.devices.reshape(grp // quads, quads, sp // SHARE, SHARE, tp),
        ("gp", "gi", *SP, "tp"),
    )
    spot = ("gp", "gi", *SP)
    placed = (
        P(spot, "tp"),
        P(spot, "tp"),
        P(spot),
        P(None, "tp", None),
        P(None, "tp", None),
        P(None, "tp", None, None),
        P(None, "tp", None, None),
        P(None, "tp", None),
        P(None, "tp", None),
        P(None, "tp", None, None),
        P(None, "tp", None, None),
        P(None, "tp"),
        P(None, "tp"),
        P(None, "tp"),
        P(spot, "tp"),
        P("tp"),
        P(SP, "tp"),
        P(SP, "tp"),
        P(None, None, "tp"),
        P("tp", SP),
    )
    return jax.shard_map(
        on_device, mesh=parted, in_specs=placed, out_specs=P(spot, "tp"), check_vma=False
    )
```
